32 devices in a mesh: sp: 8 (over z, y), tp: 4 (over x, core).
Axes of the slice: x: 2, y: 2, z: 4, core: 2. Of those that a mesh axis runs over, the one named last changes fastest.
Arguments:
- conv_input: bfloat16 [2048, 2048], P('sp', 'tp'), may hold values from -6 to 6
- gate_branch: bfloat16 [2048, 2048], P('sp', 'tp'), may hold values from -6 to 6
- conv_taps: float32 [4, 2048], P(None, 'tp'), may hold values from -3 to 3
- narrow_maps: bfloat16 [2, 8, 128, 128], P(None, 'tp'), may hold values from -0.5 to 0.5
- wide_maps: bfloat16 [2, 4, 256, 256], P(None, 'tp'), may hold values from -0.375 to 0.375
- decay_param: float32 [2048], P('tp'), may hold values from 4.5 to 20
- decay_shift: float32 [2048, 2048], P('sp', 'tp'), may hold values from -0.75 to 0
- mixer_out: bfloat16 [2048, 2048], P('tp'), may hold values from -0.125 to 0.125
- stream: bfloat16 [2048, 2048], P(('sp', 'tp')), may hold values from -6 to 6
- norm_gain: float32 [2048], replicated, may hold values from 0.1 to 1.9
- routes: int32 [2048, 4], P('sp'), may hold values from 0 to 7, all different within a row; in each aligned block of 64 rows (0 to 63, 64 to 127, ...) at most 64 rows name the same one
- route_weights: float32 [2048, 4], P('sp'), may hold values from 0.05 to 0.5
- expert_gate: bfloat16 [8, 2048, 2048], P('sp', None, 'tp'), may hold values from -1 to 1
- expert_up: bfloat16 [8, 2048, 2048], P('sp', None, 'tp'), may hold values from -1 to 1
- expert_down: bfloat16 [8, 2048, 2048], P('sp', 'tp'), may hold values from -0.015625 to 0.015625
Outputs:
- layer_out: bfloat16 [2048, 2048], P(('sp', 'tp'))
The draws below stay inside these ranges and needn't reach their ends.
Inputs may be any that keep to these rules, and one draw needn't show every extreme that they name: `routes`: each row names 4 different experts. In each aligned block of 64 rows no expert is named more than 64 times, and in every draw some expert is named exactly 64 times in some block.
All inputs are finite; a program needn't handle non-finite values.
Results may differ from the reference program's by a relative error of at most 0.015.
Values may be sent and summed in bfloat16 or wider, within the bound.
A program may use at most 128 MiB of HBM per device.

```python
import math
import jax
import jax.numpy as jnp
import numpy as np
from jax import lax

D = 2048
HN = 128
HW = 256
WIDE_HEADS = 4
NARROW_HEADS = 8
RECURRENT_WIDTH = 2048
CONV = 4
FF = 2048
FF_PIECE = 512
TOP = 4
EXPERTS = 8
TOK_DEV = 256
TOK_LOCAL = 64
SEQUENCE_TOKENS = 2048
CAP = 64
N_TP = 4


def head_of_channel():
    channel = jnp.arange(RECURRENT_WIDTH, dtype=jnp.int32)
    segment = channel // (2 * HN + HW)
    within = channel % (2 * HN + HW)
    narrow_head = 2 * segment + within // HN
    return jnp.where(within < 2 * HN, narrow_head, 2 * WIDE_HEADS + segment)


def draw_decay_param(key, part):
    random_key_series = jax.random.split(jax.random.fold_in(key, 21), 3)
    fast_odds = 8
    fast_head = jax.random.randint(random_key_series[0], (3 * WIDE_HEADS,), 0, 16) < fast_odds
    fast_rate = jnp.exp(jax.random.uniform(random_key_series[1], (RECURRENT_WIDTH,), jnp.float32, math.log(1.0 / 50.0), math.log(1.0 / 30.0)))
    slow_rate = jnp.exp(jax.random.uniform(random_key_series[2], (RECURRENT_WIDTH,), jnp.float32, math.log(0.05), math.log(0.4))) / SEQUENCE_TOKENS
    step_rate = jnp.where(fast_head[head_of_channel()], fast_rate, slow_rate)
    return (-jnp.log(jnp.expm1(0.25 * step_rate))).astype(jnp.float32)


def draw_decay_shift(key, part):
    random_key_series = jax.random.split(jax.random.fold_in(key, 31), 3)
    block_count = SEQUENCE_TOKENS // TOK_DEV
    block_rate = jnp.exp(jax.random.uniform(random_key_series[0], (block_count, 1, RECURRENT_WIDTH), jnp.float32, math.log(0.1), math.log(1.0))) / SEQUENCE_TOKENS
    stable_level = -jnp.broadcast_to(block_rate, (block_count, TOK_DEV, RECURRENT_WIDTH)).reshape(SEQUENCE_TOKENS, RECURRENT_WIDTH)
    spike_position = jax.random.randint(random_key_series[1], (2,), 0, SEQUENCE_TOKENS)
    spike_hit = jnp.any(jnp.arange(SEQUENCE_TOKENS)[:, None] == spike_position[None, :], axis=1).astype(jnp.float32)
    spike_magnitude = jax.random.uniform(random_key_series[2], (1, RECURRENT_WIDTH), jnp.float32, math.log(0.5), math.log(0.8))
    return (stable_level + spike_hit[:, None] * spike_magnitude).astype(jnp.float32)


def expert_matrix(key, salt_value):
    key_pair = jax.random.split(jax.random.fold_in(key, salt_value), 2)
    column_scale = jnp.exp(jax.random.uniform(key_pair[0], (EXPERTS, FF), jnp.float32, math.log(0.5), math.log(12.0)))

    def one_expert(inputs):
        expert_index, scale_row = inputs
        expert_key = jax.random.fold_in(key_pair[1], expert_index)
        entries = jax.random.normal(expert_key, (D, FF), jnp.float32)
        return jnp.clip(entries * scale_row[None, :] * D ** (-0.5), -1.0, 1.0).astype(jnp.bfloat16)
    return lax.map(one_expert, (jnp.arange(EXPERTS), column_scale))


def draw_expert_gate(key, part):
    return expert_matrix(key, 41)


def draw_expert_up(key, part):
    return expert_matrix(key, 42)


def shard_levels(key, dims, cuts, least, high):
    loudness, own = 1.0, jax.random.fold_in(key, 6)
    for dim, blocks in cuts:
        heights = jnp.exp(jax.random.uniform(jax.random.fold_in(own, dim), (blocks,), jnp.float32, least / len(cuts), high / len(cuts)))
        loudness = loudness * jnp.repeat(heights, dims[dim] // blocks).reshape([-1 if axis == dim else 1 for axis in range(len(dims))])
    return loudness


def assign_block(key, own, number, rows, amount, top, limit, lean):
    sequence = jax.random.permutation(key, amount)
    packed, common = load_shares(amount, rows * top, limit, lean, True), load_shares(amount, rows * top, limit, lean, False)
    places = jnp.arange(amount)

    def named(sizes, turn):
        used = int((sizes > 0).sum())
        fixed = max(1, used // 4)
        moved = fixed + (places - fixed + turn * (used - fixed)) % max(1, amount - fixed)
        return jnp.zeros((amount,), jnp.int32).at[sequence[jnp.where(places < fixed, places, moved)]].set(jnp.asarray(sizes, jnp.int32))

    sizes = jnp.where(number % 4 == 0, named(packed, number // 4), named(common, number - number // 4 - 1))
    mixed = jax.random.permutation(jax.random.fold_in(own, 3), amount)
    source_of, sink = mixed[0:amount // 2 * 2:2], mixed[1:amount // 2 * 2:2]
    margin = jnp.minimum(sizes[source_of] - 1, limit - sizes[sink]) // 2
    margin = jnp.where((source_of == sequence[0]) | (sink == sequence[0]) | (sizes[sink] == 0), 0, jnp.maximum(margin, 0))
    moved = jax.random.randint(jax.random.fold_in(own, 4), (amount // 2,), 0, 1 << 20) % (margin + 1)
    sizes = sizes.at[source_of].add(-moved).at[sink].add(moved)
    labels = jnp.searchsorted(jnp.cumsum(sizes), jnp.arange(rows * top), side="right").astype(jnp.int32)
    grid = labels.reshape(top, rows).T
    grid = grid[jax.random.permutation(jax.random.fold_in(own, 1), rows)]
    turn = jax.random.randint(jax.random.fold_in(own, 2), (rows, 1), 0, top)
    return jnp.take_along_axis(grid, (jnp.arange(top)[None, :] + turn) % top, axis=1)


def load_shares(amount, total, most, lean, full):
    weights = [(1 << 20) // math.isqrt(rank ** lean) + 1 for rank in range(1, amount + 1)]
    largest = most if full else min(most, max(-(-total // amount), total * weights[0] // sum(weights)))
    least = 1 if total - largest >= amount - 1 else 0
    holding, rest = [largest] + [least] * (amount - 1), total - largest - least * (amount - 1)
    while rest > 0:
        movable = [i for i in range(1, amount) if holding[i] < largest] or [i for i in range(1, amount) if holding[i] < most]
        whole, budget = sum([weights[i] for i in movable]), rest
        for i in movable:
            extra = min(most - holding[i], max(1, budget * weights[i] // whole), rest)
            holding[i] = holding[i] + extra
            rest = rest - extra
    return np.array(holding)


def bell_draw(stream_key, shape, spread, reach, cuts=(), kind=jnp.bfloat16):
    drawn = spread * jax.random.normal(stream_key, shape, jnp.float32)
    if cuts:
        drawn = drawn * shard_levels(stream_key, shape, cuts, -0.22, 0.18)
    return jnp.clip(drawn, -reach, reach).astype(kind)


def setup_inputs(seed: int = 0) -> dict:
    key_list = jax.random.split(jax.random.key(seed), 16)
    conv_input = bell_draw(key_list[0], (SEQUENCE_TOKENS, RECURRENT_WIDTH), 1.0, 6.0, ((0, 8), (1, 4)))
    gate_branch = bell_draw(key_list[1], (SEQUENCE_TOKENS, RECURRENT_WIDTH), 1.0, 6.0, ((0, 8), (1, 4)))
    conv_taps = bell_draw(key_list[2], (CONV, RECURRENT_WIDTH), 0.5, 3.0, ((1, 4),), jnp.float32)
    narrow_maps = bell_draw(key_list[3], (2, NARROW_HEADS, HN, HN), HN ** -0.5, 0.5, ((1, 4),))
    wide_maps = bell_draw(key_list[4], (2, WIDE_HEADS, HW, HW), HW ** -0.5, 0.375, ((1, 4),))
    decay_param = draw_decay_param(jax.random.fold_in(key_list[15], 71), 0)
    decay_shift = draw_decay_shift(jax.random.fold_in(key_list[15], 71), 0)
    mixer_out = bell_draw(key_list[7], (RECURRENT_WIDTH, D), RECURRENT_WIDTH ** -0.5, 0.125, ((0, 4),))
    stream = bell_draw(key_list[8], (SEQUENCE_TOKENS, D), 1.0, 6.0, ((0, 32),))
    norm_gain = jnp.clip(1.0 + 0.18 * jax.random.normal(key_list[9], (D,), jnp.float32), 0.1, 1.9)
    routes_keys = jax.random.split(jax.random.fold_in(key_list[10], 1), SEQUENCE_TOKENS // TOK_LOCAL)
    routes_turns = jax.random.permutation(jax.random.fold_in(key_list[10], 3), SEQUENCE_TOKENS // TOK_LOCAL)
    routes = jax.vmap(lambda own, number: assign_block(jax.random.fold_in(key_list[10], 2), own, number, TOK_LOCAL, EXPERTS, TOP, CAP, 2))(routes_keys, routes_turns).reshape((SEQUENCE_TOKENS, TOP))
    route_weights = jnp.clip(0.05 + 0.45 * jax.random.uniform(key_list[11], (SEQUENCE_TOKENS, TOP), jnp.float32) ** shard_levels(key_list[11], (SEQUENCE_TOKENS, TOP), ((0, 8),), -0.2, 0.2), 0.05, 0.5)
    expert_gate = draw_expert_gate(jax.random.fold_in(key_list[15], 71), 0)
    expert_up = draw_expert_up(jax.random.fold_in(key_list[15], 71), 0)
    expert_down = bell_draw(key_list[14], (EXPERTS, FF, D), (FF * 64) ** -0.5, 0.015625, ((0, 8), (1, 4)))
    return dict(conv_input=conv_input, gate_branch=gate_branch, conv_taps=conv_taps, narrow_maps=narrow_maps, wide_maps=wide_maps, decay_param=decay_param, decay_shift=decay_shift, mixer_out=mixer_out, stream=stream, norm_gain=norm_gain, routes=routes, route_weights=route_weights, expert_gate=expert_gate, expert_up=expert_up, expert_down=expert_down)


NORM_EPSILON = 1e-06
CLAMP_LIMIT = 7.0
GATE_SLOPE = 1.702
DECAY_SCALE = 8.0

def combine_steps(earlier, later):
    return (earlier[0] * later[0], later[0] * earlier[1] + later[1])

def head_maps(convolved, narrow_maps, wide_maps):
    seq_rows = convolved.shape[0]
    segments = convolved.reshape(seq_rows, WIDE_HEADS, 2 * HN + HW).astype(jnp.float32)
    narrow = segments[:, :, :2 * HN].reshape(seq_rows, 2 * WIDE_HEADS, HN)
    wide_part = segments[:, :, 2 * HN:]
    narrow_pre = jnp.einsum('rhi,mhio->mrho', narrow, narrow_maps.astype(jnp.float32))
    wide_pre = jnp.einsum('rhi,mhio->mrho', wide_part, wide_maps.astype(jnp.float32))
    narrow_pre = narrow_pre.reshape(2, seq_rows, WIDE_HEADS, 2 * HN)
    return jnp.concatenate([narrow_pre, wide_pre], axis=3).reshape(2, seq_rows, RECURRENT_WIDTH)

def clamp_units(gate_pre, up_pre):
    clamped = jnp.minimum(gate_pre, CLAMP_LIMIT)
    upper = jnp.clip(up_pre, -CLAMP_LIMIT, CLAMP_LIMIT)
    return (upper + 1.0) * clamped * jax.nn.sigmoid(GATE_SLOPE * clamped)

def reference(conv_input, gate_branch, conv_taps, narrow_maps, wide_maps, decay_param, decay_shift, mixer_out, stream, norm_gain, routes, route_weights, expert_gate, expert_up, expert_down):
    padded = jnp.pad(conv_input.astype(jnp.float32), ((CONV - 1, 0), (0, 0)))
    convolved = jnp.zeros((SEQUENCE_TOKENS, RECURRENT_WIDTH), jnp.float32)
    for offset in range(CONV):
        convolved = convolved + padded[offset:offset + SEQUENCE_TOKENS] * conv_taps[offset]
    convolved = convolved.astype(jnp.bfloat16)
    gate_pre = head_maps(convolved, narrow_maps, wide_maps)
    log_decay = -DECAY_SCALE * jax.nn.sigmoid(gate_pre[0]) * jax.nn.softplus(-decay_param) + decay_shift
    driving = jnp.sqrt(-jnp.expm1(2.0 * log_decay)) * jax.nn.sigmoid(gate_pre[1]) * convolved.astype(jnp.float32)
    _, recurrent = lax.associative_scan(combine_steps, (jnp.exp(log_decay), driving), axis=0)
    gated_rows = (recurrent * jax.nn.gelu(gate_branch.astype(jnp.float32))).astype(jnp.bfloat16)
    mixer_sum = jnp.dot(gated_rows, mixer_out, preferred_element_type=jnp.float32)
    hidden = (stream.astype(jnp.float32) + mixer_sum).astype(jnp.bfloat16)
    hidden_f = hidden.astype(jnp.float32)
    normed = (hidden_f * lax.rsqrt(lax.optimization_barrier(jnp.mean(hidden_f * hidden_f, axis=-1, keepdims=True)) + NORM_EPSILON) * norm_gain).astype(jnp.bfloat16)
    blocks = SEQUENCE_TOKENS // TOK_LOCAL
    flat_routes = routes.reshape(blocks, TOK_LOCAL * TOP)
    onehot = (flat_routes[:, :, None] == jnp.arange(EXPERTS, dtype=jnp.int32)[None, None, :]).astype(jnp.int32)
    slot_rank = lax.optimization_barrier(jnp.sum(jnp.cumsum(onehot, axis=1) * onehot, axis=2)) - 1
    block_index = jnp.arange(blocks, dtype=jnp.int32)[:, None]
    slot_index = flat_routes * (blocks * CAP) + block_index * CAP + slot_rank
    token_index = block_index * TOK_LOCAL + jnp.arange(TOK_LOCAL * TOP, dtype=jnp.int32)[None, :] // TOP
    slot_token = jnp.zeros((EXPERTS * blocks * CAP,), jnp.int32).at[slot_index.reshape(-1)].set(token_index.reshape(-1).astype(jnp.int32))
    slot_weight = jnp.zeros((EXPERTS * blocks * CAP,), route_weights.dtype).at[slot_index.reshape(-1)].set(route_weights.reshape(-1))
    slot_token = slot_token.reshape(EXPERTS, blocks * CAP)
    slot_weight = slot_weight.reshape(EXPERTS, blocks * CAP)

    def one_expert(combined, inputs):
        tokens_here, weights_here, gate_here, up_here, down_here = inputs
        picked = normed[tokens_here]
        gate_val = jnp.dot(picked, gate_here, preferred_element_type=jnp.float32)
        up_val = jnp.dot(picked, up_here, preferred_element_type=jnp.float32)
        activation = clamp_units(gate_val, up_val).astype(jnp.bfloat16)
        summed = jnp.zeros((picked.shape[0], D), jnp.float32)
        for piece_index in range(N_TP):
            first = piece_index * FF_PIECE
            partial_value = jnp.dot(activation[:, first:first + FF_PIECE], down_here[first:first + FF_PIECE], preferred_element_type=jnp.float32).astype(jnp.bfloat16)
            partial_value = lax.optimization_barrier(partial_value)
            summed = summed + partial_value.astype(jnp.float32)
        expert_out = lax.optimization_barrier(summed.astype(jnp.bfloat16)).astype(jnp.float32)
        combined = combined.at[tokens_here].add(weights_here[:, None] * expert_out)
        return (combined, None)
    combined, _ = lax.scan(one_expert, jnp.zeros((SEQUENCE_TOKENS, D), jnp.float32), (slot_token, slot_weight, expert_gate, expert_up, expert_down))
    return (hidden_f + combined).astype(jnp.bfloat16)
```

```python
import functools
import types

import jax
import jax.numpy as jnp
from jax import lax
from jax.experimental import pallas as pl
from jax.experimental.pallas import tpu as pltpu
from jax.sharding import PartitionSpec as P

NORM_EPSILON = 1e-06
CLAMP_LIMIT = 7.0
GATE_SLOPE = 1.702
DECAY_SCALE = 8.0


def shifted(block, axis, distance):
    devices = range(lax.axis_size(axis))
    route = [(i - distance, i) for i in devices if i - distance in devices]
    return lax.ppermute(block, axis, route)


def clamp_units(gate_pre, up_pre):
    clamped = jnp.minimum(gate_pre, CLAMP_LIMIT)
    upper = jnp.clip(up_pre, -CLAMP_LIMIT, CLAMP_LIMIT)
    return (upper + 1.0) * clamped * jax.nn.sigmoid(GATE_SLOPE * clamped)


def slot_ranks(flat_routes, expert_total):
    onehot = (
        flat_routes[:, :, None] == jnp.arange(expert_total, dtype=jnp.int32)[None, None, :]
    ).astype(jnp.int32)
    return jnp.sum(jnp.cumsum(onehot, axis=1) * onehot, axis=2) - 1


def take_rows(source_rows, slot_source):
    filled = slot_source >= 0
    picked = source_rows[jnp.maximum(slot_source, 0)]
    return jnp.where(filled[:, None], picked, jnp.zeros_like(picked))


def expert_work(arrived, expert_gate, expert_up, expert_down):
    local_experts = expert_gate.shape[0]
    buffer_shape = arrived.shape
    grouped = arrived.reshape(
        buffer_shape[0] // local_experts,
        local_experts,
        buffer_shape[1] * buffer_shape[2],
        buffer_shape[3],
    )
    gate_pre = jnp.einsum(
        "sxcd,xdf->sxcf", grouped, expert_gate, preferred_element_type=jnp.float32
    )
    up_pre = jnp.einsum("sxcd,xdf->sxcf", grouped, expert_up, preferred_element_type=jnp.float32)
    activation = clamp_units(gate_pre, up_pre).astype(jnp.bfloat16)
    partial_value = jnp.einsum(
        "sxcf,xfd->sxcd", activation, expert_down, preferred_element_type=jnp.float32
    )
    return partial_value.reshape(buffer_shape)


LANES = 128
SUBLANES = 8
DX, DY, DC = 1, 2, 4
SERIES_LIMIT = 0.05
GELU_SCALE = 0.7978845608028654
GELU_CUBIC = 0.044715


def mix_kernel(
    head_ref, conv_ref, taps_ref, narrow_ref, wide_ref, soft_ref, shift_ref,
    factor_ref, state_ref, padded, log_keep, drive_keep,
):
    rows, channels = conv_ref.shape
    taps = taps_ref.shape[0]
    padded[0:SUBLANES, :] = head_ref[...]
    padded[SUBLANES:, :] = conv_ref[...].astype(jnp.float32)
    total = jnp.zeros((rows, channels), jnp.float32)
    for k in range(taps):
        total = total + padded[pl.ds(SUBLANES - taps + 1 + k, rows), :] * taps_ref[k : k + 1, :]
    convolved = total.astype(jnp.bfloat16)
    narrow_size, wide_size = narrow_ref.shape[2], wide_ref.shape[2]
    spans = []
    for j in range(wide_ref.shape[1]):
        base = j * (2 * narrow_size + wide_size)
        spans.append((base, narrow_size, narrow_ref, 2 * j))
        spans.append((base + narrow_size, narrow_size, narrow_ref, 2 * j + 1))
        spans.append((base + 2 * narrow_size, wide_size, wide_ref, j))
    for start, size, maps, head in spans:
        piece = convolved[:, start : start + size]
        decay_pre = jnp.dot(piece, maps[0, head], preferred_element_type=jnp.float32)
        input_pre = jnp.dot(piece, maps[1, head], preferred_element_type=jnp.float32)
        cols = slice(start, start + size)
        log_decay = (
            -DECAY_SCALE * jax.nn.sigmoid(decay_pre) * soft_ref[:, cols] + shift_ref[:, cols]
        )
        decay = jnp.exp(log_decay)
        y = 2.0 * log_decay
        series = -y * (1.0 + y * (0.5 + y * (1.0 / 6.0 + y * (1.0 / 24.0 + y * (1.0 / 120.0)))))
        lost = jnp.where(y > -SERIES_LIMIT, series, 1.0 - decay * decay)
        log_keep[:, cols] = decay
        drive_keep[:, cols] = (
            jnp.sqrt(lost) * jax.nn.sigmoid(input_pre) * piece.astype(jnp.float32)
        )
    row_id = lax.broadcasted_iota(jnp.int32, (SUBLANES, channels), 0)

    def tile(i, carry):
        product, state = carry
        at = pl.ds(pl.multiple_of(i * SUBLANES, SUBLANES), SUBLANES)
        a, b = log_keep[at, :], drive_keep[at, :]
        step = 1
        while step < SUBLANES:
            inside = row_id >= step
            a_before = jnp.where(inside, pltpu.roll(a, step, 0), 1.0)
            b_before = jnp.where(inside, pltpu.roll(b, step, 0), 0.0)
            b = a * b_before + b
            a = a * a_before
            step *= 2
        b = b + a * state
        a = a * product
        factor_ref[at, :] = a
        state_ref[at, :] = b
        last = slice(SUBLANES - 1, SUBLANES)
        return (a[last, :], b[last, :])

    lax.fori_loop(
        0,
        rows // SUBLANES,
        tile,
        (jnp.ones((1, channels), jnp.float32), jnp.zeros((1, channels), jnp.float32)),
    )


def mix_local(head, conv_input, conv_taps, narrow_maps, wide_maps, soft, decay_shift):
    shape = conv_input.shape
    flat = jax.ShapeDtypeStruct(shape, jnp.float32)
    return pl.pallas_call(
        mix_kernel,
        out_shape=(flat, flat),
        in_specs=[pl.BlockSpec(memory_space=pltpu.VMEM)] * 7,
        out_specs=(pl.BlockSpec(memory_space=pltpu.VMEM),) * 2,
        scratch_shapes=[
            pltpu.VMEM((shape[0] + SUBLANES, shape[1]), jnp.float32),
            pltpu.VMEM(shape, jnp.float32),
            pltpu.VMEM(shape, jnp.float32),
        ],
        compiler_params=pltpu.CompilerParams(vmem_limit_bytes=32 * 1024 * 1024),
    )(head, conv_input, conv_taps, narrow_maps, wide_maps, soft, decay_shift)


def nearest(z, p, depth):
    short = jnp.minimum(z, depth - 1 - z)
    near = p <= 2 * short
    distance = jnp.where(near, (p + 1) // 2, p - short)
    left = jnp.where(near, p % 2, jnp.where(z > depth - 1 - z, 1, 0))
    return jnp.where(p == 0, 0, jnp.where(left == 1, distance, depth - distance))


def layer_kernel(count, names, *refs):
    v = types.SimpleNamespace(**dict(zip(names, refs)))
    rows, channels = v.conv.shape
    kept, width = v.stream.shape
    depth = count // 2
    half = kept // 2
    single, kind = (jnp.float32, jnp.bfloat16)
    sp, tp = (lax.axis_index("sp"), lax.axis_index("tp"))
    z, y = (sp // 2, sp % 2)
    x, c = (tp // 2, tp % 2)
    mesh_id = pl.DeviceIdType.MESH
    peer_c = {"sp": sp, "tp": x * 2 + 1 - c}
    peer_x = {"sp": sp, "tp": (1 - x) * 2 + c}
    peer_y = {"sp": z * 2 + 1 - y, "tp": tp}

    def plane(k):
        return {"sp": ((z + k) % depth) * 2 + y, "tp": tp}

    def later(k):
        return {"sp": (sp + k) % count, "tp": tp}

    def copy(src, dst, send, recv, peer):
        return pltpu.make_async_remote_copy(
            src_ref=src, dst_ref=dst, send_sem=send, recv_sem=recv,
            device_id=peer, device_id_type=mesh_id,
        )

    barrier = pltpu.get_barrier_semaphore()
    peers = [peer_x, peer_c] + [later(k) for k in range(1, count)]
    for peer in peers:
        pl.semaphore_signal(barrier, inc=1, device_id=peer, device_id_type=mesh_id)
    load_names = (
        "conv", "taps", "narrow", "wide", "decay", "shift", "gate", "routes", "shares", "stream",
        "gain", "mixer", "gate_w", "up_w", "down_w",
    )
    loads = {}
    for n, name in enumerate(load_names):
        source = getattr(v, name + "_hbm")
        source = source.at[0] if name.endswith("_w") else source
        loads[name] = pltpu.make_async_copy(source, getattr(v, name), v.load_sem.at[n])
        loads[name].start()

    loads["conv"].wait()
    pl.semaphore_wait(barrier, len(peers))
    halo_rows = v.halo.shape[0]
    halo_copy = copy(
        v.conv.at[pl.ds(rows - halo_rows, halo_rows)], v.halo, v.halo_send, v.halo_recv, later(1)
    )
    halo_copy.start()

    loads["routes"].wait()
    loads["shares"].wait()
    lines = v.weigh_out.shape[1]
    line = lax.broadcasted_iota(jnp.int32, (lines, rows), 0)
    for e in range(count):
        share = jnp.zeros((1, rows), single)
        for n in range(v.routes.shape[0]):
            share = share + jnp.where(
                v.routes[n : n + 1, :] == e, v.shares[n : n + 1, :], 0.0
            )
        v.weigh_out[e] = jnp.where(line == sp, share, 0.0)
    weigh_copies = [
        copy(
            v.weigh_out.at[(sp + k) % count], v.weigh_in.at[k], v.weigh_send.at[k],
            v.weigh_recv.at[k], later(k),
        )
        for k in range(1, count)
    ]
    for one in weigh_copies:
        one.start()

    loads["decay"].wait()
    t = jnp.exp(-v.decay[...])
    v.soft[...] = t * (1.0 - t * (0.5 - t * (1.0 / 3.0 - t * (0.25 - t * (0.2 - t * (1.0 / 6.0))))))
    loads["gate"].wait()
    g = v.gate[...].astype(single)
    v.gelu[...] = 0.5 * g * (1.0 + jnp.tanh(GELU_SCALE * (g + GELU_CUBIC * g * g * g)))
    for name in ("taps", "narrow", "wide", "shift"):
        loads[name].wait()

    halo_copy.wait()
    before = v.halo[...].astype(single)[halo_rows - SUBLANES :]
    v.head[...] = jnp.where(sp > 0, before, jnp.zeros_like(before))
    mix_kernel(
        v.head, v.conv, v.taps, v.narrow, v.wide, v.soft, v.shift,
        v.factor, v.state, v.padded, v.log_keep, v.drive_keep,
    )
    groups = channels // LANES
    for n in range(groups):
        cols = slice(n * LANES, (n + 1) * LANES)
        v.ends[0, n : n + 1, :] = v.factor[rows - 1 : rows, cols]
        v.ends[0, groups + n : groups + n + 1, :] = v.state[rows - 1 : rows, cols]
    end_copies = [
        copy(v.ends.at[0], v.ends.at[k], v.end_send.at[k], v.end_recv.at[k], later(k))
        for k in range(1, count)
    ]
    for one in end_copies:
        one.start()

    table = v.weigh_out[sp]
    for k in range(1, count):
        weigh_copies[k - 1].wait_recv()
        table = table + v.weigh_in[k]
    filled = jnp.concatenate([table, jnp.zeros((LANES - lines, rows), single)], axis=0)
    v.weigh[...] = jnp.transpose(filled)
    for name in ("mixer", "stream", "gain"):
        loads[name].wait()

    carry = jnp.zeros((groups, LANES), single)
    for k in range(count - 1, 0, -1):
        end_copies[k - 1].wait_recv()
        longer = v.ends[k, 0:groups, :] * carry + v.ends[k, groups : 2 * groups, :]
        carry = jnp.where(sp >= k, longer, carry)
    carry = jnp.concatenate([carry[n : n + 1, :] for n in range(groups)], axis=1)
    order = [(1 - x, 1 - c), (x, 1 - c), (1 - x, c), (x, c)]
    for n, (chip, core) in enumerate(order):
        at = pl.ds(pl.multiple_of((chip * 2 + core) * kept, kept), kept)
        recurrent = v.state[at, :] + v.factor[at, :] * carry
        v.gated[n * kept : (n + 1) * kept, :] = (recurrent * v.gelu[at, :]).astype(kind)

    pieces = v.pair_send.shape[0]
    piece = width // pieces

    def pair(n):
        cols = pl.ds(n * piece, piece)
        return copy(
            v.give.at[:, :, cols], v.got.at[:, :, cols], v.pair_send.at[n], v.pair_recv.at[n],
            peer_c,
        )

    for n in range(pieces):
        cols = slice(n * piece, (n + 1) * piece)
        value = jnp.dot(v.gated[...], v.mixer[:, cols], preferred_element_type=single)
        v.give[:, :, cols] = value[: 2 * kept].astype(kind).reshape(2, kept, piece)
        v.keep[:, :, cols] = value[2 * kept :].reshape(2, kept, piece)
        pair(n).start()
    for n in range(pieces):
        pair(n).wait_recv()

    def part_of(h):
        return pl.ds(h * half, half)

    def cross(h):
        return copy(
            v.over.at[part_of(h)], v.came.at[part_of(h)], v.cross_send.at[h], v.cross_recv.at[h],
            peer_x,
        )

    for h in range(2):
        at = slice(h * half, (h + 1) * half)
        v.over[at, :] = (v.keep[0, at, :] + v.got[0, at, :].astype(single)).astype(kind)
        cross(h).start()

    xs, part = (v.xs, v.part)

    def ax(k, h):
        return copy(
            xs.at[k, 0, part_of(h)], xs.at[k, DX, part_of(h)], v.ax_send.at[k, h],
            v.ax_recv.at[k, h], peer_x,
        )

    def ay(k, h):
        return copy(
            xs.at[k, 0, part_of(h)], xs.at[k, DY, part_of(h)], v.ay_send.at[k, h],
            v.ay_recv.at[k, h], peer_y,
        )

    def fy(k):
        return copy(
            xs.at[k, DX, part_of(0)], xs.at[k, DX + DY, part_of(0)], v.af_send.at[k, 0],
            v.af_recv.at[k, 0], peer_y,
        )

    def fx(k):
        return copy(
            xs.at[k, DY, part_of(1)], xs.at[k, DX + DY, part_of(1)], v.af_send.at[k, 1],
            v.af_recv.at[k, 1], peer_x,
        )

    def ac(k, s):
        return copy(
            xs.at[k, s], xs.at[k, DC + s], v.ac_send.at[k, s], v.ac_recv.at[k, s], peer_c
        )

    def upward(i, h):
        return copy(
            xs.at[i - 1, 0, part_of(h)], xs.at[i, 0, part_of(h)], v.up_send.at[i, h],
            v.az_recv.at[i, h], plane(1),
        )

    def downward(i, h):
        return copy(
            xs.at[(depth - i + 1) % depth, 0, part_of(h)], xs.at[depth - i, 0, part_of(h)],
            v.dn_send.at[i, h], v.az_recv.at[depth - i, h], plane(depth - 1),
        )

    def landed(k, h):
        return copy(
            xs.at[0, 0, part_of(h)], xs.at[k, 0, part_of(h)], v.up_send.at[k, h],
            v.az_recv.at[k, h], plane(1),
        )

    for h in range(2):
        at = slice(h * half, (h + 1) * half)
        cross(h).wait_recv()
        total = v.keep[1, at, :] + v.got[1, at, :].astype(single) + v.came[at, :].astype(single)
        hidden = (v.stream[at, :].astype(single) + total).astype(kind)
        v.hidden[at, :] = hidden
        wide = hidden.astype(single)
        mean = jnp.mean(wide * wide, axis=-1, keepdims=True)
        normed = wide * lax.rsqrt(mean + NORM_EPSILON) * v.gain[...]
        xs[0, 0, at, :] = normed.astype(kind)
        ax(0, h).start()
        ay(0, h).start()

        @pl.when(z < depth - 1)
        def _():
            upward(1, h).start()

        @pl.when(z > 0)
        def _():
            downward(1, h).start()

    ac(0, 0).start()
    for name in ("gate_w", "up_w", "down_w"):
        loads[name].wait()

    def rc(k):
        return copy(
            part.at[k, pl.ds(DC, DC)], v.from_core.at[k], v.rc_send.at[k], v.rc_recv.at[k], peer_c
        )

    def rs(k, n):
        sems = (v.rs_send.at[k, n], v.rs_recv.at[k, n])
        if n == 0:
            return copy(part.at[k, DX + DY, part_of(0)], v.from_y.at[k, 1], *sems, peer_y)
        if n == 1:
            return copy(part.at[k, DX + DY, part_of(1)], v.from_x.at[k, 1], *sems, peer_x)
        if n == 2:
            return copy(part.at[k, DY, part_of(0)], v.from_y.at[k, 0], *sems, peer_y)
        if n == 3:
            return copy(part.at[k, DX, part_of(1)], v.from_x.at[k, 0], *sems, peer_x)
        if n == 4:
            return copy(part.at[k, DX, part_of(0)], v.last_x.at[k], *sems, peer_x)
        return copy(part.at[k, DY, part_of(1)], v.last_y.at[k], *sems, peer_y)

    def zr(k):
        return copy(
            part.at[k, 0], v.from_z.at[k], v.rz_send.at[k], v.rz_recv.at[k], plane(depth - k)
        )

    lane = lax.broadcasted_iota(jnp.int32, (kept, LANES), 1)

    def share_of(k, j):
        plane_from = (z + depth - k) % depth
        columns = []
        for s in range(DC):
            y_from = 1 - y if s & DY else y
            x_from = 1 - x if s & DX else x
            c_from = 1 - c if j else c
            at = pl.ds(pl.multiple_of((x_from * 2 + c_from) * kept, kept), kept)
            mine = lane == plane_from * 2 + y_from
            columns.append(
                jnp.sum(jnp.where(mine, v.weigh[at, :], 0.0), axis=1, keepdims=True)
            )
        return jnp.concatenate(columns, axis=0)

    def activated(k, j):
        rows_in = xs[k, j * DC : (j + 1) * DC].reshape(DC * kept, width)
        g = jnp.dot(rows_in, v.gate_w[...], preferred_element_type=single)
        u = jnp.dot(rows_in, v.up_w[...], preferred_element_type=single)
        return (clamp_units(g, u) * share_of(k, j)).astype(kind)

    def theirs(k):
        act = activated(k, 1)
        for n in range(pieces):
            cols = slice(n * piece, (n + 1) * piece)
            down = jnp.dot(act, v.down_w[:, cols], preferred_element_type=single)
            part[k, DC : 2 * DC, :, cols] = down.astype(kind).reshape(DC, kept, piece)
        rc(k).start()

    def ours(k):
        act = activated(k, 0)
        rc(k).wait_recv()
        for n in range(pieces):
            cols = slice(n * piece, (n + 1) * piece)
            down = jnp.dot(act, v.down_w[:, cols], preferred_element_type=single)
            down = down.reshape(DC, kept, piece) + v.from_core[k, :, :, cols].astype(single)
            part[k, 0:DC, :, cols] = down.astype(kind)

    def spread_first(k):
        ax(k, 0).wait_recv()
        fy(k).start()
        ay(k, 1).wait_recv()
        fx(k).start()

    def spread_rest(k):
        ax(k, 1).wait_recv()
        ac(k, DX).start()
        ay(k, 0).wait_recv()
        ac(k, DY).start()

    def spread_last(k):
        af_y, af_x = (fy(k), fx(k))
        af_y.wait_recv()
        af_x.wait_recv()
        ac(k, DX + DY).start()

    def enter(k):
        for h in range(2):
            landed(k, h).wait_recv()

        @pl.when((k <= z) & (z < depth - 1))
        def _():
            for h in range(2):
                upward(k + 1, h).start()

        @pl.when((k > z) & (z > 0))
        def _():
            for h in range(2):
                downward(depth - k + 1, h).start()

        ax(k, 0).start()
        ay(k, 1).start()
        ax(k, 1).start()
        ay(k, 0).start()
        ac(k, 0).start()

    def reduce_first(k):
        for n in range(4):
            rs(k, n).start()

    def reduce_next(k):
        rs(k, 0).wait_recv()
        now = part[k, DX, 0:half].astype(single) + v.from_y[k, 1].astype(single)
        part[k, DX, 0:half] = now.astype(kind)
        rs(k, 4).start()
        rs(k, 1).wait_recv()
        now = part[k, DY, half:kept].astype(single) + v.from_x[k, 1].astype(single)
        part[k, DY, half:kept] = now.astype(kind)
        rs(k, 5).start()

    def reduced(k):
        for n in (2, 3, 4, 5):
            rs(k, n).wait_recv()
        upper = part[k, 0, 0:half].astype(single) + v.from_y[k, 0].astype(single)
        lower = part[k, 0, half:kept].astype(single) + v.from_x[k, 0].astype(single)
        return (upper + v.last_x[k].astype(single), lower + v.last_y[k].astype(single))

    def reduce_last(k):
        upper, lower = reduced(k)
        part[k, 0, 0:half] = upper.astype(kind)
        part[k, 0, half:kept] = lower.astype(kind)
        zr(k).start()

    def step(q, none):
        k = nearest(z, q % depth, depth)
        k_next = nearest(z, (q + 1) % depth, depth)
        k_done = nearest(z, (q + depth - 1) % depth, depth)
        k_older = nearest(z, (q + depth - 2) % depth, depth)
        live, late = (q < depth, q > 0)

        @pl.when(live)
        def _():
            spread_first(k)

        @pl.when(late)
        def _():
            for s in range(DC):
                ac(k_done, s).wait_recv()
            theirs(k_done)

        @pl.when(q + 1 < depth)
        def _():
            enter(k_next)

        @pl.when(live)
        def _():
            spread_rest(k)

        @pl.when(q > 3)
        def _():
            reduce_next(k_older)

        @pl.when(late)
        def _():
            ours(k_done)

        @pl.when(q > 2)
        def _():
            reduce_first(k_done)

        @pl.when(live)
        def _():
            spread_last(k)

        return none

    lax.fori_loop(0, depth + 1, step, 0)
    k_1, k_near, k_far = [nearest(z, p, depth) for p in (1, depth - 2, depth - 1)]
    reduce_last(k_near)
    reduce_next(k_far)
    reduce_first(k_1)
    reduce_last(k_far)
    reduce_next(k_1)
    reduce_first(0)
    reduce_last(k_1)
    reduce_next(0)
    upper, lower = reduced(0)
    upper = upper + v.hidden[0:half, :].astype(single)
    lower = lower + v.hidden[half:kept, :].astype(single)
    for k in range(1, depth):
        zr(k).wait_recv()
        upper = upper + v.from_z[k, 0:half].astype(single)
        lower = lower + v.from_z[k, half:kept].astype(single)
    v.out[0:half, :] = upper.astype(v.out.dtype)
    v.out[half:kept, :] = lower.astype(v.out.dtype)

    for one in weigh_copies + end_copies:
        one.wait_send()
    for n in range(pieces):
        pair(n).wait_send()
    for h in range(2):
        cross(h).wait_send()

    def drain(k, none):
        for h in range(2):
            ax(k, h).wait_send()
            ay(k, h).wait_send()
        fy(k).wait_send()
        fx(k).wait_send()
        for s in range(DC):
            ac(k, s).wait_send()
        rc(k).wait_send()
        for n in range(6):
            rs(k, n).wait_send()
        return none

    lax.fori_loop(0, depth, drain, 0)

    def drain_planes(i, none):
        zr(i).wait_send()

        @pl.when((i - 1 <= z) & (z < depth - 1))
        def _():
            for h in range(2):
                upward(i, h).wait_send()

        @pl.when((z + i <= depth) & (z > 0))
        def _():
            for h in range(2):
                downward(i, h).wait_send()

        return none

    lax.fori_loop(1, depth, drain_planes, 0)


def layer(
    conv_input, gate_branch, conv_taps, narrow_maps, wide_maps, decay, decay_shift, mixer_out,
    stream, gain, routes, shares, expert_gate, expert_up, expert_down,
):
    count = lax.axis_size("sp")
    depth = count // 2
    rows, channels = conv_input.shape
    kept, width = stream.shape
    half = kept // 2
    pieces = 4
    lines = -(-count // SUBLANES) * SUBLANES
    single, kind = (jnp.float32, jnp.bfloat16)
    dma = pltpu.SemaphoreType.DMA
    inputs = dict(
        conv=conv_input, gate=gate_branch, taps=conv_taps, narrow=narrow_maps, wide=wide_maps,
        decay=decay, shift=decay_shift, mixer=mixer_out, stream=stream, gain=gain, routes=routes,
        shares=shares, gate_w=expert_gate, up_w=expert_up, down_w=expert_down,
    )
    scratch = {
        name: pltpu.VMEM(one.shape[1:] if name.endswith("_w") else one.shape, one.dtype)
        for name, one in inputs.items()
    }
    flat = pltpu.VMEM((rows, channels), single)
    scratch.update(
        soft=pltpu.VMEM(decay.shape, single),
        gelu=flat,
        head=pltpu.VMEM((SUBLANES, channels), single),
        halo=pltpu.VMEM((2 * SUBLANES, channels), kind),
        factor=flat,
        state=flat,
        padded=pltpu.VMEM((rows + SUBLANES, channels), single),
        log_keep=flat,
        drive_keep=flat,
        ends=pltpu.VMEM((count, 2 * channels // LANES, LANES), single),
        weigh_out=pltpu.VMEM((count, lines, rows), single),
        weigh_in=pltpu.VMEM((count, lines, rows), single),
        weigh=pltpu.VMEM((rows, LANES), single),
        gated=pltpu.VMEM((rows, channels), kind),
        give=pltpu.VMEM((2, kept, width), kind),
        got=pltpu.VMEM((2, kept, width), kind),
        keep=pltpu.VMEM((2, kept, width), single),
        over=pltpu.VMEM((kept, width), kind),
        came=pltpu.VMEM((kept, width), kind),
        hidden=pltpu.VMEM((kept, width), kind),
        xs=pltpu.VMEM((depth, 2 * DC, kept, width), kind),
        part=pltpu.VMEM((depth, 2 * DC, kept, width), kind),
        from_core=pltpu.VMEM((depth, DC, kept, width), kind),
        from_y=pltpu.VMEM((depth, 2, half, width), kind),
        from_x=pltpu.VMEM((depth, 2, half, width), kind),
        last_x=pltpu.VMEM((depth, half, width), kind),
        last_y=pltpu.VMEM((depth, half, width), kind),
        from_z=pltpu.VMEM((depth, kept, width), kind),
        load_sem=dma((len(inputs),)),
        halo_send=dma,
        halo_recv=dma,
    )
    for name, shape in dict(
        weigh=(count,), end=(count,), pair=(pieces,), cross=(2,), ax=(depth, 2), ay=(depth, 2),
        af=(depth, 2), ac=(depth, DC), rc=(depth,), rs=(depth, 6), rz=(depth,),
    ).items():
        scratch[name + "_send"] = dma(shape)
        scratch[name + "_recv"] = dma(shape)
    for name in ("up_send", "dn_send", "az_recv"):
        scratch[name] = dma((depth, 2))
    names = [name + "_hbm" for name in inputs] + ["out"] + list(scratch)
    return pl.pallas_call(
        functools.partial(layer_kernel, count, names),
        out_shape=jax.ShapeDtypeStruct((kept, width), kind),
        in_specs=[pl.BlockSpec(memory_space=pl.ANY)] * len(inputs),
        out_specs=pl.BlockSpec(memory_space=pltpu.VMEM),
        scratch_shapes=list(scratch.values()),
        compiler_params=pltpu.CompilerParams(
            collective_id=1, has_side_effects=True, vmem_limit_bytes=60 * 1024 * 1024
        ),
    )(*inputs.values())


def shards(
    conv_input,
    gate_branch,
    conv_taps,
    narrow_maps,
    wide_maps,
    decay_param,
    decay_shift,
    mixer_out,
    stream,
    norm_gain,
    routes,
    route_weights,
    expert_gate,
    expert_up,
    expert_down,
):
    seq_rows, channels = conv_input.shape
    tap_count = conv_taps.shape[0]
    tp_count = lax.axis_size("tp")
    tok_local = seq_rows // tp_count
    top_count = routes.shape[1]
    expert_total = expert_gate.shape[0] * lax.axis_size("sp")
    capacity = max(2, 2 * tok_local * top_count // expert_total)
    whole_rows = capacity >= tok_local and expert_gate.shape[0] == 1
    if whole_rows and tp_count == 4 and lax.axis_size("sp") == 8:
        return layer(
            conv_input, gate_branch, conv_taps, narrow_maps, wide_maps, decay_param[None, :],
            decay_shift, mixer_out, stream, norm_gain[None, :], routes.T, route_weights.T,
            expert_gate, expert_up, expert_down,
        )
    own_index = lax.axis_index("tp")
    own_rows = lax.dynamic_slice_in_dim(routes, own_index * tok_local, tok_local, 0)
    own_weights = lax.dynamic_slice_in_dim(route_weights, own_index * tok_local, tok_local, 0)
    soft = jax.nn.softplus(-decay_param)[None, :]
    earlier = shifted(conv_input[seq_rows - tap_count + 1 :], "sp", 1)
    head = jnp.zeros((SUBLANES, channels), jnp.float32)
    head = head.at[SUBLANES - tap_count + 1 :].set(earlier.astype(jnp.float32))
    factors, local_state = mix_local(
        head, conv_input, conv_taps, narrow_maps, wide_maps, soft, decay_shift
    )
    ends = lax.all_gather(jnp.stack([factors[-1], local_state[-1]]), "sp")
    mine = lax.axis_index("sp")
    state = jnp.zeros((channels,), jnp.float32)
    for position in range(lax.axis_size("sp") - 1):
        longer = ends[position, 0] * state + ends[position, 1]
        state = jnp.where(position < mine, longer, state)
    carried = (None, state)
    recurrent = local_state + factors * carried[1]
    gated_rows = (recurrent * jax.nn.gelu(gate_branch.astype(jnp.float32))).astype(jnp.bfloat16)
    mixer_sum = lax.psum_scatter(
        jnp.dot(gated_rows, mixer_out, preferred_element_type=jnp.float32).astype(jnp.bfloat16),
        "tp",
        scatter_dimension=0,
        tiled=True,
    ).astype(jnp.float32)
    hidden_f = stream.astype(jnp.float32) + mixer_sum
    hidden = hidden_f.astype(jnp.bfloat16)
    hidden_f = hidden.astype(jnp.float32)
    normed = (
        hidden_f
        * lax.rsqrt(jnp.mean(hidden_f * hidden_f, axis=-1, keepdims=True) + NORM_EPSILON)
        * norm_gain
    ).astype(jnp.bfloat16)
    model_width = normed.shape[1]
    assignments = tok_local * top_count
    own_routes = own_rows.reshape(assignments)
    own_ranks = slot_ranks(own_routes[None, :], expert_total)[0]
    source = jnp.arange(assignments, dtype=jnp.int32) // top_count
    slot_source = (
        jnp.full((expert_total * capacity,), -1, jnp.int32)
        .at[own_routes * capacity + own_ranks]
        .set(source)
    )
    outgoing = take_rows(normed, slot_source).reshape(expert_total, 1, capacity, model_width)
    partial_value = expert_work(
        lax.all_gather(
            lax.all_to_all(outgoing, "sp", split_axis=0, concat_axis=0, tiled=True),
            "tp",
            axis=1,
            tiled=True,
        ),
        expert_gate,
        expert_up,
        expert_down,
    )
    summed = lax.psum_scatter(
        partial_value.astype(jnp.bfloat16), "tp", scatter_dimension=1, tiled=True
    )
    returned = lax.all_to_all(summed, "sp", split_axis=0, concat_axis=0, tiled=True)
    own_slots = own_routes * capacity + own_ranks
    picked = returned.reshape(expert_total * capacity, model_width)[own_slots]
    combined = jnp.sum(
        picked.reshape(tok_local, top_count, model_width).astype(jnp.float32)
        * own_weights[:, :, None],
        axis=1,
    )
    return (hidden_f + combined).astype(jnp.bfloat16)


def solution(mesh):
    placed = (
        P("sp", "tp"),
        P("sp", "tp"),
        P(None, "tp"),
        P(None, "tp", None, None),
        P(None, "tp", None, None),
        P("tp"),
        P("sp", "tp"),
        P("tp", None),
        P(("sp", "tp"), None),
        P(),
        P("sp", None),
        P("sp", None),
        P("sp", None, "tp"),
        P("sp", None, "tp"),
        P("sp", "tp", None),
    )
    return jax.shard_map(
        shards, mesh=mesh, in_specs=placed, out_specs=P(("sp", "tp"), None), check_vma=False
    )
```

```python
import functools
import types

import jax
import jax.numpy as jnp
from jax import lax
from jax.experimental import pallas as pl
from jax.experimental.pallas import tpu as pltpu
from jax.sharding import PartitionSpec as P

NORM_EPSILON = 1e-06
CLAMP_LIMIT = 7.0
GATE_SLOPE = 1.702
DECAY_SCALE = 8.0


def shifted(block, axis, distance):
    devices = range(lax.axis_size(axis))
    route = [(i - distance, i) for i in devices if i - distance in devices]
    return lax.ppermute(block, axis, route)


def clamp_units(gate_pre, up_pre):
    clamped = jnp.minimum(gate_pre, CLAMP_LIMIT)
    upper = jnp.clip(up_pre, -CLAMP_LIMIT, CLAMP_LIMIT)
    return (upper + 1.0) * clamped * jax.nn.sigmoid(GATE_SLOPE * clamped)


def slot_ranks(flat_routes, expert_total):
    onehot = (
        flat_routes[:, :, None] == jnp.arange(expert_total, dtype=jnp.int32)[None, None, :]
    ).astype(jnp.int32)
    return jnp.sum(jnp.cumsum(onehot, axis=1) * onehot, axis=2) - 1


def take_rows(source_rows, slot_source):
    filled = slot_source >= 0
    picked = source_rows[jnp.maximum(slot_source, 0)]
    return jnp.where(filled[:, None], picked, jnp.zeros_like(picked))


def expert_work(arrived, expert_gate, expert_up, expert_down):
    local_experts = expert_gate.shape[0]
    buffer_shape = arrived.shape
    grouped = arrived.reshape(
        buffer_shape[0] // local_experts,
        local_experts,
        buffer_shape[1] * buffer_shape[2],
        buffer_shape[3],
    )
    gate_pre = jnp.einsum(
        "sxcd,xdf->sxcf", grouped, expert_gate, preferred_element_type=jnp.float32
    )
    up_pre = jnp.einsum("sxcd,xdf->sxcf", grouped, expert_up, preferred_element_type=jnp.float32)
    activation = clamp_units(gate_pre, up_pre).astype(jnp.bfloat16)
    partial_value = jnp.einsum(
        "sxcf,xfd->sxcd", activation, expert_down, preferred_element_type=jnp.float32
    )
    return partial_value.reshape(buffer_shape)


LANES = 128
SUBLANES = 8
DX, DY, DC = 1, 2, 4
SERIES_LIMIT = 0.05
GELU_SCALE = 0.7978845608028654
GELU_CUBIC = 0.044715


def mix_kernel(
    head_ref, conv_ref, taps_ref, narrow_ref, wide_ref, soft_ref, shift_ref,
    factor_ref, state_ref, padded, log_keep, drive_keep,
):
    rows, channels = conv_ref.shape
    taps = taps_ref.shape[0]
    padded[0:SUBLANES, :] = head_ref[...]
    padded[SUBLANES:, :] = conv_ref[...].astype(jnp.float32)
    total = jnp.zeros((rows, channels), jnp.float32)
    for k in range(taps):
        total = total + padded[pl.ds(SUBLANES - taps + 1 + k, rows), :] * taps_ref[k : k + 1, :]
    convolved = total.astype(jnp.bfloat16)
    narrow_size, wide_size = narrow_ref.shape[2], wide_ref.shape[2]
    spans = []
    for j in range(wide_ref.shape[1]):
        base = j * (2 * narrow_size + wide_size)
        spans.append((base, narrow_size, narrow_ref, 2 * j))
        spans.append((base + narrow_size, narrow_size, narrow_ref, 2 * j + 1))
        spans.append((base + 2 * narrow_size, wide_size, wide_ref, j))
    for start, size, maps, head in spans:
        piece = convolved[:, start : start + size]
        decay_pre = jnp.dot(piece, maps[0, head], preferred_element_type=jnp.float32)
        input_pre = jnp.dot(piece, maps[1, head], preferred_element_type=jnp.float32)
        cols = slice(start, start + size)
        log_decay = (
            -DECAY_SCALE * jax.nn.sigmoid(decay_pre) * soft_ref[:, cols] + shift_ref[:, cols]
        )
        decay = jnp.exp(log_decay)
        y = 2.0 * log_decay
        series = -y * (1.0 + y * (0.5 + y * (1.0 / 6.0 + y * (1.0 / 24.0 + y * (1.0 / 120.0)))))
        lost = jnp.where(y > -SERIES_LIMIT, series, 1.0 - decay * decay)
        log_keep[:, cols] = decay
        drive_keep[:, cols] = (
            jnp.sqrt(lost) * jax.nn.sigmoid(input_pre) * piece.astype(jnp.float32)
        )
    row_id = lax.broadcasted_iota(jnp.int32, (SUBLANES, channels), 0)

    def tile(i, carry):
        product, state = carry
        at = pl.ds(pl.multiple_of(i * SUBLANES, SUBLANES), SUBLANES)
        a, b = log_keep[at, :], drive_keep[at, :]
        step = 1
        while step < SUBLANES:
            inside = row_id >= step
            a_before = jnp.where(inside, pltpu.roll(a, step, 0), 1.0)
            b_before = jnp.where(inside, pltpu.roll(b, step, 0), 0.0)
            b = a * b_before + b
            a = a * a_before
            step *= 2
        b = b + a * state
        a = a * product
        factor_ref[at, :] = a
        state_ref[at, :] = b
        last = slice(SUBLANES - 1, SUBLANES)
        return (a[last, :], b[last, :])

    lax.fori_loop(
        0,
        rows // SUBLANES,
        tile,
        (jnp.ones((1, channels), jnp.float32), jnp.zeros((1, channels), jnp.float32)),
    )


def mix_local(head, conv_input, conv_taps, narrow_maps, wide_maps, soft, decay_shift):
    shape = conv_input.shape
    flat = jax.ShapeDtypeStruct(shape, jnp.float32)
    return pl.pallas_call(
        mix_kernel,
        out_shape=(flat, flat),
        in_specs=[pl.BlockSpec(memory_space=pltpu.VMEM)] * 7,
        out_specs=(pl.BlockSpec(memory_space=pltpu.VMEM),) * 2,
        scratch_shapes=[
            pltpu.VMEM((shape[0] + SUBLANES, shape[1]), jnp.float32),
            pltpu.VMEM(shape, jnp.float32),
            pltpu.VMEM(shape, jnp.float32),
        ],
        compiler_params=pltpu.CompilerParams(vmem_limit_bytes=32 * 1024 * 1024),
    )(head, conv_input, conv_taps, narrow_maps, wide_maps, soft, decay_shift)


def nearest(z, p, depth):
    short = jnp.minimum(z, depth - 1 - z)
    near = p <= 2 * short
    distance = jnp.where(near, (p + 1) // 2, p - short)
    left = jnp.where(near, p % 2, jnp.where(z > depth - 1 - z, 1, 0))
    return jnp.where(p == 0, 0, jnp.where(left == 1, distance, depth - distance))


def layer_kernel(count, names, *refs):
    v = types.SimpleNamespace(**dict(zip(names, refs)))
    rows, channels = v.conv.shape
    kept, width = v.stream.shape
    depth = count // 2
    half = kept // 2
    single, kind = (jnp.float32, jnp.bfloat16)
    sp, tp = (lax.axis_index("sp"), lax.axis_index("tp"))
    z, y = (sp // 2, sp % 2)
    x, c = (tp // 2, tp % 2)
    mesh_id = pl.DeviceIdType.MESH
    peer_c = {"sp": sp, "tp": x * 2 + 1 - c}
    peer_x = {"sp": sp, "tp": (1 - x) * 2 + c}
    peer_y = {"sp": z * 2 + 1 - y, "tp": tp}

    def plane(k):
        return {"sp": ((z + k) % depth) * 2 + y, "tp": tp}

    def later(k):
        return {"sp": (sp + k) % count, "tp": tp}

    def copy(src, dst, send, recv, peer):
        return pltpu.make_async_remote_copy(
            src_ref=src, dst_ref=dst, send_sem=send, recv_sem=recv,
            device_id=peer, device_id_type=mesh_id,
        )

    def all_of(ref, sem):
        return copy(ref, ref, sem, sem, peer_c)

    barrier = pltpu.get_barrier_semaphore()
    peers = [peer_x, peer_c] + [later(k) for k in range(1, count)]
    for peer in peers:
        pl.semaphore_signal(barrier, inc=1, device_id=peer, device_id_type=mesh_id)
    load_names = (
        "conv", "taps", "narrow", "wide", "decay", "shift", "gate", "routes", "shares", "stream",
        "gain", "mixer", "gate_w", "up_w", "down_w",
    )
    loads = {}
    for n, name in enumerate(load_names):
        source = getattr(v, name + "_hbm")
        source = source.at[0] if name.endswith("_w") else source
        loads[name] = pltpu.make_async_copy(source, getattr(v, name), v.load_sem.at[n])
        loads[name].start()

    loads["conv"].wait()
    pl.semaphore_wait(barrier, len(peers))
    halo_rows = v.halo.shape[0]
    halo_copy = copy(
        v.conv.at[pl.ds(rows - halo_rows, halo_rows)], v.halo, v.halo_send, v.halo_recv, later(1)
    )
    halo_copy.start()

    loads["routes"].wait()
    loads["shares"].wait()
    lines = v.weigh_out.shape[1]
    line = lax.broadcasted_iota(jnp.int32, (lines, rows), 0)
    for e in range(count):
        share = jnp.zeros((1, rows), single)
        for n in range(v.routes.shape[0]):
            share = share + jnp.where(
                v.routes[n : n + 1, :] == e, v.shares[n : n + 1, :], 0.0
            )
        v.weigh_out[e] = jnp.where(line == sp, share, 0.0)
    weigh_copies = [
        copy(
            v.weigh_out.at[(sp + k) % count], v.weigh_in.at[k], v.weigh_send, v.weigh_recv,
            later(k),
        )
        for k in range(1, count)
    ]
    for one in weigh_copies:
        one.start()

    loads["decay"].wait()
    t = jnp.exp(-v.decay[...])
    v.soft[...] = t * (1.0 - t * (0.5 - t * (1.0 / 3.0 - t * (0.25 - t * (0.2 - t * (1.0 / 6.0))))))
    loads["gate"].wait()
    g = v.gate[...].astype(single)
    v.gelu[...] = 0.5 * g * (1.0 + jnp.tanh(GELU_SCALE * (g + GELU_CUBIC * g * g * g)))
    for name in ("taps", "narrow", "wide", "shift"):
        loads[name].wait()

    halo_copy.wait()
    before = v.halo[...].astype(single)[halo_rows - SUBLANES :]
    v.head[...] = jnp.where(sp > 0, before, jnp.zeros_like(before))
    mix_kernel(
        v.head, v.conv, v.taps, v.narrow, v.wide, v.soft, v.shift,
        v.factor, v.state, v.padded, v.log_keep, v.drive_keep,
    )
    groups = channels // LANES
    for n in range(groups):
        cols = slice(n * LANES, (n + 1) * LANES)
        v.ends[0, n : n + 1, :] = v.factor[rows - 1 : rows, cols]
        v.ends[0, groups + n : groups + n + 1, :] = v.state[rows - 1 : rows, cols]
    end_copies = [
        copy(v.ends.at[0], v.ends.at[k], v.end_send, v.end_recv, later(k))
        for k in range(1, count)
    ]
    for one in end_copies:
        one.start()

    others = pl.ds(1, count - 1)
    all_of(v.weigh_in.at[others], v.weigh_recv).wait_recv()
    table = v.weigh_out[sp]
    for k in range(1, count):
        table = table + v.weigh_in[k]
    filled = jnp.concatenate([table, jnp.zeros((LANES - lines, rows), single)], axis=0)
    v.weigh[...] = jnp.transpose(filled)
    for name in ("mixer", "stream", "gain"):
        loads[name].wait()

    all_of(v.ends.at[others], v.end_recv).wait_recv()
    carry = jnp.zeros((groups, LANES), single)
    for k in range(count - 1, 0, -1):
        longer = v.ends[k, 0:groups, :] * carry + v.ends[k, groups : 2 * groups, :]
        carry = jnp.where(sp >= k, longer, carry)
    carry = jnp.concatenate([carry[n : n + 1, :] for n in range(groups)], axis=1)
    order = [(1 - x, 1 - c), (x, 1 - c), (1 - x, c), (x, c)]
    for n, (chip, core) in enumerate(order):
        at = pl.ds(pl.multiple_of((chip * 2 + core) * kept, kept), kept)
        recurrent = v.state[at, :] + v.factor[at, :] * carry
        v.gated[n * kept : (n + 1) * kept, :] = (recurrent * v.gelu[at, :]).astype(kind)

    pieces = 4
    piece = width // pieces

    def pair(n):
        cols = pl.ds(n * piece, piece)
        return copy(
            v.give.at[:, :, cols], v.got.at[:, :, cols], v.pair_send, v.pair_recv, peer_c
        )

    for n in range(pieces):
        cols = slice(n * piece, (n + 1) * piece)
        value = jnp.dot(v.gated[...], v.mixer[:, cols], preferred_element_type=single)
        v.give[:, :, cols] = value[: 2 * kept].astype(kind).reshape(2, kept, piece)
        v.keep[:, :, cols] = value[2 * kept :].reshape(2, kept, piece)
        pair(n).start()
    all_of(v.got, v.pair_recv).wait_recv()

    def part_of(h):
        return pl.ds(h * half, half)

    def cross(h):
        return copy(
            v.over.at[part_of(h)], v.came.at[part_of(h)], v.cross_send, v.cross_recv.at[h],
            peer_x,
        )

    for h in range(2):
        at = slice(h * half, (h + 1) * half)
        v.over[at, :] = (v.keep[0, at, :] + v.got[0, at, :].astype(single)).astype(kind)
        cross(h).start()

    xs, part = (v.xs, v.part)

    def ax(k, h):
        return copy(
            xs.at[k, 0, part_of(h)], xs.at[k, DX, part_of(h)], v.ax_send,
            v.ax_recv.at[k, h], peer_x,
        )

    def ay(k, h):
        return copy(
            xs.at[k, 0, part_of(h)], xs.at[k, DY, part_of(h)], v.ay_send,
            v.ay_recv.at[k, h], peer_y,
        )

    def fy(k):
        return copy(
            xs.at[k, DX, part_of(0)], xs.at[k, DX + DY, part_of(0)], v.af_send,
            v.af_recv.at[k], peer_y,
        )

    def fx(k):
        return copy(
            xs.at[k, DY, part_of(1)], xs.at[k, DX + DY, part_of(1)], v.af_send,
            v.af_recv.at[k], peer_x,
        )

    def ac(k, s):
        return copy(
            xs.at[k, s], xs.at[k, DC + s], v.ac_send, v.ac_recv.at[k], peer_c
        )

    whole = pl.ds(0, kept)

    def upward(i, at):
        return copy(
            xs.at[i - 1, 0, at], xs.at[i, 0, at], v.up_send.at[i], v.az_recv.at[i], plane(1)
        )

    def downward(i, at):
        return copy(
            xs.at[(depth - i + 1) % depth, 0, at], xs.at[depth - i, 0, at], v.dn_send.at[i],
            v.az_recv.at[depth - i], plane(depth - 1),
        )

    def landed(k):
        return all_of(xs.at[k, 0], v.az_recv.at[k])

    for h in range(2):
        at = slice(h * half, (h + 1) * half)
        cross(h).wait_recv()
        total = v.keep[1, at, :] + v.got[1, at, :].astype(single) + v.came[at, :].astype(single)
        hidden = (v.stream[at, :].astype(single) + total).astype(kind)
        v.hidden[at, :] = hidden
        wide = hidden.astype(single)
        mean = jnp.mean(wide * wide, axis=-1, keepdims=True)
        normed = wide * lax.rsqrt(mean + NORM_EPSILON) * v.gain[...]
        xs[0, 0, at, :] = normed.astype(kind)
        ax(0, h).start()
        ay(0, h).start()

        @pl.when(z < depth - 1)
        def _():
            upward(1, part_of(h)).start()

        @pl.when(z > 0)
        def _():
            downward(1, part_of(h)).start()

    ac(0, 0).start()
    for name in ("gate_w", "up_w", "down_w"):
        loads[name].wait()

    def rc(k):
        return copy(
            part.at[k, pl.ds(DC, DC)], v.from_core.at[k], v.rc_send, v.rc_recv.at[k], peer_c
        )

    def rs(k, n):
        sems = (v.rs_send, v.rs_recv.at[k, min(n, 2)])
        if n == 0:
            return copy(part.at[k, DX + DY, part_of(0)], v.first.at[k, 0], *sems, peer_y)
        if n == 1:
            return copy(part.at[k, DX + DY, part_of(1)], v.first.at[k, 1], *sems, peer_x)
        if n == 2:
            return copy(part.at[k, DY, part_of(0)], v.rest.at[k, 0], *sems, peer_y)
        if n == 3:
            return copy(part.at[k, DX, part_of(1)], v.rest.at[k, 1], *sems, peer_x)
        if n == 4:
            return copy(part.at[k, DX, part_of(0)], v.rest.at[k, 2], *sems, peer_x)
        return copy(part.at[k, DY, part_of(1)], v.rest.at[k, 3], *sems, peer_y)

    def zr(k):
        return copy(
            part.at[k, 0], v.from_z.at[k], v.rz_send, v.rz_recv, plane(depth - k)
        )

    lane = lax.broadcasted_iota(jnp.int32, (kept, LANES), 1)

    def share_of(k, j):
        plane_from = (z + depth - k) % depth
        columns = []
        for s in range(DC):
            y_from = 1 - y if s & DY else y
            x_from = 1 - x if s & DX else x
            c_from = 1 - c if j else c
            at = pl.ds(pl.multiple_of((x_from * 2 + c_from) * kept, kept), kept)
            mine = lane == plane_from * 2 + y_from
            columns.append(
                jnp.sum(jnp.where(mine, v.weigh[at, :], 0.0), axis=1, keepdims=True)
            )
        return jnp.concatenate(columns, axis=0)

    def activated(k, j):
        rows_in = xs[k, j * DC : (j + 1) * DC].reshape(DC * kept, width)
        g = jnp.dot(rows_in, v.gate_w[...], preferred_element_type=single)
        u = jnp.dot(rows_in, v.up_w[...], preferred_element_type=single)
        return (clamp_units(g, u) * share_of(k, j)).astype(kind)

    def theirs(k):
        act = activated(k, 1)
        for n in range(pieces):
            cols = slice(n * piece, (n + 1) * piece)
            down = jnp.dot(act, v.down_w[:, cols], preferred_element_type=single)
            part[k, DC : 2 * DC, :, cols] = down.astype(kind).reshape(DC, kept, piece)
        rc(k).start()

    def ours(k):
        act = activated(k, 0)
        rc(k).wait_recv()
        for n in range(pieces):
            cols = slice(n * piece, (n + 1) * piece)
            down = jnp.dot(act, v.down_w[:, cols], preferred_element_type=single)
            down = down.reshape(DC, kept, piece) + v.from_core[k, :, :, cols].astype(single)
            part[k, 0:DC, :, cols] = down.astype(kind)

    def spread_first(k):
        ax(k, 0).wait_recv()
        fy(k).start()
        ay(k, 1).wait_recv()
        fx(k).start()

    def spread_rest(k):
        ax(k, 1).wait_recv()
        ac(k, DX).start()
        ay(k, 0).wait_recv()
        ac(k, DY).start()

    def spread_last(k):
        all_of(xs.at[k, DX + DY], v.af_recv.at[k]).wait_recv()
        ac(k, DX + DY).start()

    def relay(i):
        @pl.when(i <= z)
        def _():
            landed(i).wait_recv()

            @pl.when(z < depth - 1)
            def _():
                upward(i + 1, whole).start()

        @pl.when(z + i < depth)
        def _():
            landed(depth - i).wait_recv()

            @pl.when(z > 0)
            def _():
                downward(i + 1, whole).start()

    def enter(k):
        ax(k, 0).start()
        ay(k, 1).start()
        ax(k, 1).start()
        ay(k, 0).start()
        ac(k, 0).start()

    def reduce_first(k):
        for n in range(4):
            rs(k, n).start()

    def reduce_next(k):
        rs(k, 0).wait_recv()
        now = part[k, DX, 0:half].astype(single) + v.first[k, 0].astype(single)
        part[k, DX, 0:half] = now.astype(kind)
        rs(k, 4).start()
        rs(k, 1).wait_recv()
        now = part[k, DY, half:kept].astype(single) + v.first[k, 1].astype(single)
        part[k, DY, half:kept] = now.astype(kind)
        rs(k, 5).start()

    def reduced(k):
        all_of(v.rest.at[k], v.rs_recv.at[k, 2]).wait_recv()
        upper = part[k, 0, 0:half].astype(single) + v.rest[k, 0].astype(single)
        lower = part[k, 0, half:kept].astype(single) + v.rest[k, 1].astype(single)
        return (upper + v.rest[k, 2].astype(single), lower + v.rest[k, 3].astype(single))

    def reduce_last(k):
        upper, lower = reduced(k)
        part[k, 0, 0:half] = upper.astype(kind)
        part[k, 0, half:kept] = lower.astype(kind)
        zr(k).start()

    def step(q, none):
        k = nearest(z, q % depth, depth)
        k_next = nearest(z, (q + 1) % depth, depth)
        k_done = nearest(z, (q + depth - 1) % depth, depth)
        k_older = nearest(z, (q + depth - 2) % depth, depth)
        live, late = (q < depth, q > 0)

        @pl.when(live)
        def _():
            spread_first(k)

        @pl.when(late)
        def _():
            all_of(xs.at[k_done, pl.ds(DC, DC)], v.ac_recv.at[k_done]).wait_recv()
            theirs(k_done)

        @pl.when(q + 1 < depth)
        def _():
            relay(q + 1)
            enter(k_next)

        @pl.when(live)
        def _():
            spread_rest(k)

        @pl.when(q > 3)
        def _():
            reduce_next(k_older)

        @pl.when(late)
        def _():
            ours(k_done)

        @pl.when(q > 2)
        def _():
            reduce_first(k_done)

        @pl.when(live)
        def _():
            spread_last(k)

        return none

    lax.fori_loop(0, depth + 1, step, 0)
    k_1, k_near, k_far = [nearest(z, p, depth) for p in (1, depth - 2, depth - 1)]
    reduce_last(k_near)
    reduce_next(k_far)
    reduce_first(k_1)
    reduce_last(k_far)
    reduce_next(k_1)
    reduce_first(0)
    reduce_last(k_1)
    reduce_next(0)
    upper, lower = reduced(0)
    upper = upper + v.hidden[0:half, :].astype(single)
    lower = lower + v.hidden[half:kept, :].astype(single)
    beyond = pl.ds(1, depth - 1)
    all_of(v.from_z.at[beyond], v.rz_recv).wait_recv()
    for k in range(1, depth):
        upper = upper + v.from_z[k, 0:half].astype(single)
        lower = lower + v.from_z[k, half:kept].astype(single)
    results = []
    for h, value in enumerate((upper, lower)):
        v.result[h * half : (h + 1) * half, :] = value.astype(v.result.dtype)
        results.append(
            pltpu.make_async_copy(
                v.result.at[part_of(h)], v.out.at[part_of(h)], v.result_sem.at[h]
            )
        )
        results[h].start()

    every = pl.ds(0, depth)
    quarter = xs.at[every, pl.ds(0, 1)]
    for ref, sem in (
        (v.weigh_in.at[others], v.weigh_send), (v.ends.at[others], v.end_send),
        (v.give, v.pair_send), (v.over, v.cross_send), (quarter, v.ax_send),
        (quarter, v.ay_send), (quarter, v.af_send), (xs.at[every, pl.ds(0, DC)], v.ac_send),
        (part.at[every, pl.ds(DC, DC)], v.rc_send), (part.at[every, pl.ds(0, 3)], v.rs_send),
        (v.from_z.at[beyond], v.rz_send),
    ):
        all_of(ref, sem).wait_send()
    for i in range(1, depth):

        @pl.when((i - 1 <= z) & (z < depth - 1))
        def _():
            upward(i, whole).wait_send()

        @pl.when((z + i <= depth) & (z > 0))
        def _():
            downward(i, whole).wait_send()

    for one in results:
        one.wait()


def layer(
    conv_input, gate_branch, conv_taps, narrow_maps, wide_maps, decay, decay_shift, mixer_out,
    stream, gain, routes, shares, expert_gate, expert_up, expert_down,
):
    count = lax.axis_size("sp")
    depth = count // 2
    rows, channels = conv_input.shape
    kept, width = stream.shape
    half = kept // 2
    pieces = 4
    lines = -(-count // SUBLANES) * SUBLANES
    single, kind = (jnp.float32, jnp.bfloat16)
    dma = pltpu.SemaphoreType.DMA
    inputs = dict(
        conv=conv_input, gate=gate_branch, taps=conv_taps, narrow=narrow_maps, wide=wide_maps,
        decay=decay, shift=decay_shift, mixer=mixer_out, stream=stream, gain=gain, routes=routes,
        shares=shares, gate_w=expert_gate, up_w=expert_up, down_w=expert_down,
    )
    scratch = {
        name: pltpu.VMEM(one.shape[1:] if name.endswith("_w") else one.shape, one.dtype)
        for name, one in inputs.items()
    }
    flat = pltpu.VMEM((rows, channels), single)
    scratch.update(
        soft=pltpu.VMEM(decay.shape, single),
        gelu=flat,
        head=pltpu.VMEM((SUBLANES, channels), single),
        halo=pltpu.VMEM((2 * SUBLANES, channels), kind),
        factor=flat,
        state=flat,
        padded=pltpu.VMEM((rows + SUBLANES, channels), single),
        log_keep=flat,
        drive_keep=flat,
        ends=pltpu.VMEM((count, 2 * channels // LANES, LANES), single),
        weigh_out=pltpu.VMEM((count, lines, rows), single),
        weigh_in=pltpu.VMEM((count, lines, rows), single),
        weigh=pltpu.VMEM((rows, LANES), single),
        gated=pltpu.VMEM((rows, channels), kind),
        give=pltpu.VMEM((2, kept, width), kind),
        got=pltpu.VMEM((2, kept, width), kind),
        keep=pltpu.VMEM((2, kept, width), single),
        over=pltpu.VMEM((kept, width), kind),
        came=pltpu.VMEM((kept, width), kind),
        hidden=pltpu.VMEM((kept, width), kind),
        xs=pltpu.VMEM((depth, 2 * DC, kept, width), kind),
        part=pltpu.VMEM((depth, 2 * DC, kept, width), kind),
        from_core=pltpu.VMEM((depth, DC, kept, width), kind),
        first=pltpu.VMEM((depth, 2, half, width), kind),
        rest=pltpu.VMEM((depth, 4, half, width), kind),
        from_z=pltpu.VMEM((depth, kept, width), kind),
        result=pltpu.VMEM((kept, width), kind),
        load_sem=dma((len(inputs),)),
        result_sem=dma((2,)),
        halo_send=dma,
        halo_recv=dma,
    )
    sent = ("weigh", "end", "pair", "cross", "ax", "ay", "af", "ac", "rc", "rs", "rz")
    scratch.update({name + "_send": dma for name in sent})
    landing = dict(
        weigh=(), end=(), pair=(), cross=(2,), ax=(depth, 2), ay=(depth, 2), af=(depth,),
        ac=(depth,), rc=(depth,), rs=(depth, 3), rz=(), az=(depth,),
    )
    scratch.update({name + "_recv": dma(shape) if shape else dma for name, shape in landing.items()})
    scratch.update(up_send=dma((depth,)), dn_send=dma((depth,)))
    names = [name + "_hbm" for name in inputs] + ["out"] + list(scratch)
    return pl.pallas_call(
        functools.partial(layer_kernel, count, names),
        out_shape=jax.ShapeDtypeStruct((kept, width), kind),
        in_specs=[pl.BlockSpec(memory_space=pl.ANY)] * len(inputs),
        out_specs=pl.BlockSpec(memory_space=pl.ANY),
        scratch_shapes=list(scratch.values()),
        compiler_params=pltpu.CompilerParams(
            collective_id=1, has_side_effects=True, vmem_limit_bytes=60 * 1024 * 1024
        ),
    )(*inputs.values())


def shards(
    conv_input,
    gate_branch,
    conv_taps,
    narrow_maps,
    wide_maps,
    decay_param,
    decay_shift,
    mixer_out,
    stream,
    norm_gain,
    routes,
    route_weights,
    expert_gate,
    expert_up,
    expert_down,
):
    seq_rows, channels = conv_input.shape
    tap_count = conv_taps.shape[0]
    tp_count = lax.axis_size("tp")
    tok_local = seq_rows // tp_count
    top_count = routes.shape[1]
    expert_total = expert_gate.shape[0] * lax.axis_size("sp")
    capacity = max(2, 2 * tok_local * top_count // expert_total)
    whole_rows = capacity >= tok_local and expert_gate.shape[0] == 1
    if whole_rows and tp_count == 4 and lax.axis_size("sp") == 8:
        return layer(
            conv_input, gate_branch, conv_taps, narrow_maps, wide_maps, decay_param[None, :],
            decay_shift, mixer_out, stream, norm_gain[None, :], routes.T, route_weights.T,
            expert_gate, expert_up, expert_down,
        )
    own_index = lax.axis_index("tp")
    own_rows = lax.dynamic_slice_in_dim(routes, own_index * tok_local, tok_local, 0)
    own_weights = lax.dynamic_slice_in_dim(route_weights, own_index * tok_local, tok_local, 0)
    soft = jax.nn.softplus(-decay_param)[None, :]
    earlier = shifted(conv_input[seq_rows - tap_count + 1 :], "sp", 1)
    head = jnp.zeros((SUBLANES, channels), jnp.float32)
    head = head.at[SUBLANES - tap_count + 1 :].set(earlier.astype(jnp.float32))
    factors, local_state = mix_local(
        head, conv_input, conv_taps, narrow_maps, wide_maps, soft, decay_shift
    )
    ends = lax.all_gather(jnp.stack([factors[-1], local_state[-1]]), "sp")
    mine = lax.axis_index("sp")
    state = jnp.zeros((channels,), jnp.float32)
    for position in range(lax.axis_size("sp") - 1):
        longer = ends[position, 0] * state + ends[position, 1]
        state = jnp.where(position < mine, longer, state)
    carried = (None, state)
    recurrent = local_state + factors * carried[1]
    gated_rows = (recurrent * jax.nn.gelu(gate_branch.astype(jnp.float32))).astype(jnp.bfloat16)
    mixer_sum = lax.psum_scatter(
        jnp.dot(gated_rows, mixer_out, preferred_element_type=jnp.float32).astype(jnp.bfloat16),
        "tp",
        scatter_dimension=0,
        tiled=True,
    ).astype(jnp.float32)
    hidden_f = stream.astype(jnp.float32) + mixer_sum
    hidden = hidden_f.astype(jnp.bfloat16)
    hidden_f = hidden.astype(jnp.float32)
    normed = (
        hidden_f
        * lax.rsqrt(jnp.mean(hidden_f * hidden_f, axis=-1, keepdims=True) + NORM_EPSILON)
        * norm_gain
    ).astype(jnp.bfloat16)
    model_width = normed.shape[1]
    assignments = tok_local * top_count
    own_routes = own_rows.reshape(assignments)
    own_ranks = slot_ranks(own_routes[None, :], expert_total)[0]
    source = jnp.arange(assignments, dtype=jnp.int32) // top_count
    slot_source = (
        jnp.full((expert_total * capacity,), -1, jnp.int32)
        .at[own_routes * capacity + own_ranks]
        .set(source)
    )
    outgoing = take_rows(normed, slot_source).reshape(expert_total, 1, capacity, model_width)
    partial_value = expert_work(
        lax.all_gather(
            lax.all_to_all(outgoing, "sp", split_axis=0, concat_axis=0, tiled=True),
            "tp",
            axis=1,
            tiled=True,
        ),
        expert_gate,
        expert_up,
        expert_down,
    )
    summed = lax.psum_scatter(
        partial_value.astype(jnp.bfloat16), "tp", scatter_dimension=1, tiled=True
    )
    returned = lax.all_to_all(summed, "sp", split_axis=0, concat_axis=0, tiled=True)
    own_slots = own_routes * capacity + own_ranks
    picked = returned.reshape(expert_total * capacity, model_width)[own_slots]
    combined = jnp.sum(
        picked.reshape(tok_local, top_count, model_width).astype(jnp.float32)
        * own_weights[:, :, None],
        axis=1,
    )
    return (hidden_f + combined).astype(jnp.bfloat16)


def solution(mesh):
    placed = (
        P("sp", "tp"),
        P("sp", "tp"),
        P(None, "tp"),
        P(None, "tp", None, None),
        P(None, "tp", None, None),
        P("tp"),
        P("sp", "tp"),
        P("tp", None),
        P(("sp", "tp"), None),
        P(),
        P("sp", None),
        P("sp", None),
        P("sp", None, "tp"),
        P("sp", None, "tp"),
        P("sp", "tp", None),
    )
    return jax.shard_map(
        shards, mesh=mesh, in_specs=placed, out_specs=P(("sp", "tp"), None), check_vma=False
    )
```

```python
import functools
import types

import jax
import jax.numpy as jnp
from jax import lax
from jax.experimental import pallas as pl
from jax.experimental.pallas import tpu as pltpu
from jax.sharding import PartitionSpec as P

NORM_EPSILON = 1e-06
CLAMP_LIMIT = 7.0
GATE_SLOPE = 1.702
DECAY_SCALE = 8.0


def shifted(block, axis, distance):
    devices = range(lax.axis_size(axis))
    route = [(i - distance, i) for i in devices if i - distance in devices]
    return lax.ppermute(block, axis, route)


def clamp_units(gate_pre, up_pre):
    clamped = jnp.minimum(gate_pre, CLAMP_LIMIT)
    upper = jnp.clip(up_pre, -CLAMP_LIMIT, CLAMP_LIMIT)
    return (upper + 1.0) * clamped * jax.nn.sigmoid(GATE_SLOPE * clamped)


def slot_ranks(flat_routes, expert_total):
    onehot = (
        flat_routes[:, :, None] == jnp.arange(expert_total, dtype=jnp.int32)[None, None, :]
    ).astype(jnp.int32)
    return jnp.sum(jnp.cumsum(onehot, axis=1) * onehot, axis=2) - 1


def take_rows(source_rows, slot_source):
    filled = slot_source >= 0
    picked = source_rows[jnp.maximum(slot_source, 0)]
    return jnp.where(filled[:, None], picked, jnp.zeros_like(picked))


def expert_work(arrived, expert_gate, expert_up, expert_down):
    local_experts = expert_gate.shape[0]
    buffer_shape = arrived.shape
    grouped = arrived.reshape(
        buffer_shape[0] // local_experts,
        local_experts,
        buffer_shape[1] * buffer_shape[2],
        buffer_shape[3],
    )
    gate_pre = jnp.einsum(
        "sxcd,xdf->sxcf", grouped, expert_gate, preferred_element_type=jnp.float32
    )
    up_pre = jnp.einsum("sxcd,xdf->sxcf", grouped, expert_up, preferred_element_type=jnp.float32)
    activation = clamp_units(gate_pre, up_pre).astype(jnp.bfloat16)
    partial_value = jnp.einsum(
        "sxcf,xfd->sxcd", activation, expert_down, preferred_element_type=jnp.float32
    )
    return partial_value.reshape(buffer_shape)


LANES = 128
SUBLANES = 8
DX, DY, DC = 1, 2, 4
SERIES_LIMIT = 0.05
GELU_SCALE = 0.7978845608028654
GELU_CUBIC = 0.044715


def mix_kernel(
    head_ref, conv_ref, taps_ref, narrow_ref, wide_ref, soft_ref, shift_ref,
    factor_ref, state_ref, padded, log_keep, drive_keep,
):
    rows, channels = conv_ref.shape
    taps = taps_ref.shape[0]
    padded[0:SUBLANES, :] = head_ref[...]
    padded[SUBLANES:, :] = conv_ref[...].astype(jnp.float32)
    total = jnp.zeros((rows, channels), jnp.float32)
    for k in range(taps):
        total = total + padded[pl.ds(SUBLANES - taps + 1 + k, rows), :] * taps_ref[k : k + 1, :]
    convolved = total.astype(jnp.bfloat16)
    narrow_size, wide_size = narrow_ref.shape[2], wide_ref.shape[2]
    spans = []
    for j in range(wide_ref.shape[1]):
        base = j * (2 * narrow_size + wide_size)
        spans.append((base, narrow_size, narrow_ref, 2 * j))
        spans.append((base + narrow_size, narrow_size, narrow_ref, 2 * j + 1))
        spans.append((base + 2 * narrow_size, wide_size, wide_ref, j))
    for start, size, maps, head in spans:
        piece = convolved[:, start : start + size]
        decay_pre = jnp.dot(piece, maps[0, head], preferred_element_type=jnp.float32)
        input_pre = jnp.dot(piece, maps[1, head], preferred_element_type=jnp.float32)
        cols = slice(start, start + size)
        log_decay = (
            -DECAY_SCALE * jax.nn.sigmoid(decay_pre) * soft_ref[:, cols] + shift_ref[:, cols]
        )
        decay = jnp.exp(log_decay)
        y = 2.0 * log_decay
        series = -y * (1.0 + y * (0.5 + y * (1.0 / 6.0 + y * (1.0 / 24.0 + y * (1.0 / 120.0)))))
        lost = jnp.where(y > -SERIES_LIMIT, series, 1.0 - decay * decay)
        log_keep[:, cols] = decay
        drive_keep[:, cols] = (
            jnp.sqrt(lost) * jax.nn.sigmoid(input_pre) * piece.astype(jnp.float32)
        )
    row_id = lax.broadcasted_iota(jnp.int32, (SUBLANES, channels), 0)

    def tile(i, carry):
        product, state = carry
        at = pl.ds(pl.multiple_of(i * SUBLANES, SUBLANES), SUBLANES)
        a, b = log_keep[at, :], drive_keep[at, :]
        step = 1
        while step < SUBLANES:
            inside = row_id >= step
            a_before = jnp.where(inside, pltpu.roll(a, step, 0), 1.0)
            b_before = jnp.where(inside, pltpu.roll(b, step, 0), 0.0)
            b = a * b_before + b
            a = a * a_before
            step *= 2
        b = b + a * state
        a = a * product
        factor_ref[at, :] = a
        state_ref[at, :] = b
        last = slice(SUBLANES - 1, SUBLANES)
        return (a[last, :], b[last, :])

    lax.fori_loop(
        0,
        rows // SUBLANES,
        tile,
        (jnp.ones((1, channels), jnp.float32), jnp.zeros((1, channels), jnp.float32)),
    )


def mix_local(head, conv_input, conv_taps, narrow_maps, wide_maps, soft, decay_shift):
    shape = conv_input.shape
    flat = jax.ShapeDtypeStruct(shape, jnp.float32)
    return pl.pallas_call(
        mix_kernel,
        out_shape=(flat, flat),
        in_specs=[pl.BlockSpec(memory_space=pltpu.VMEM)] * 7,
        out_specs=(pl.BlockSpec(memory_space=pltpu.VMEM),) * 2,
        scratch_shapes=[
            pltpu.VMEM((shape[0] + SUBLANES, shape[1]), jnp.float32),
            pltpu.VMEM(shape, jnp.float32),
            pltpu.VMEM(shape, jnp.float32),
        ],
        compiler_params=pltpu.CompilerParams(vmem_limit_bytes=32 * 1024 * 1024),
    )(head, conv_input, conv_taps, narrow_maps, wide_maps, soft, decay_shift)


def turn(z, p, depth):
    return jnp.where(p == 0, 0, jnp.where(z % 2 == 1, p, depth - p))


def layer_kernel(count, names, *refs):
    v = types.SimpleNamespace(**dict(zip(names, refs)))
    rows, channels = v.conv.shape
    kept, width = v.stream.shape
    depth = count // 2
    half = kept // 2
    single, kind = (jnp.float32, jnp.bfloat16)
    sp, tp = (lax.axis_index("sp"), lax.axis_index("tp"))
    z, y = (sp // 2, sp % 2)
    x, c = (tp // 2, tp % 2)
    mesh_id = pl.DeviceIdType.MESH
    peer_c = {"sp": sp, "tp": x * 2 + 1 - c}
    peer_x = {"sp": sp, "tp": (1 - x) * 2 + c}
    peer_y = {"sp": z * 2 + 1 - y, "tp": tp}

    def plane(k):
        return {"sp": ((z + k) % depth) * 2 + y, "tp": tp}

    def later(k):
        return {"sp": (sp + k) % count, "tp": tp}

    def copy(src, dst, send, recv, peer):
        return pltpu.make_async_remote_copy(
            src_ref=src, dst_ref=dst, send_sem=send, recv_sem=recv,
            device_id=peer, device_id_type=mesh_id,
        )

    def all_of(ref, sem):
        return copy(ref, ref, sem, sem, peer_c)

    barrier = pltpu.get_barrier_semaphore()
    peers = [peer_x, peer_c] + [later(k) for k in range(1, count)]
    for peer in peers:
        pl.semaphore_signal(barrier, inc=1, device_id=peer, device_id_type=mesh_id)
    load_names = (
        "conv", "taps", "narrow", "wide", "decay", "shift", "gate", "routes", "shares", "stream",
        "gain", "mixer", "gate_w", "up_w", "down_w",
    )
    loads = {}
    for n, name in enumerate(load_names):
        source = getattr(v, name + "_hbm")
        source = source.at[0] if name.endswith("_w") else source
        loads[name] = pltpu.make_async_copy(source, getattr(v, name), v.load_sem.at[n])
        loads[name].start()

    loads["conv"].wait()
    pl.semaphore_wait(barrier, len(peers))
    halo_rows = v.halo.shape[0]
    halo_copy = copy(
        v.conv.at[pl.ds(rows - halo_rows, halo_rows)], v.halo, v.halo_send, v.halo_recv, later(1)
    )
    halo_copy.start()

    loads["decay"].wait()
    t = jnp.exp(-v.decay[...])
    v.soft[...] = t * (1.0 - t * (0.5 - t * (1.0 / 3.0 - t * (0.25 - t * (0.2 - t * (1.0 / 6.0))))))
    for name in ("taps", "narrow", "wide", "shift"):
        loads[name].wait()
    taps = v.taps.shape[0]
    lead = 2 * SUBLANES
    v.padded[SUBLANES:, :] = v.conv[...].astype(single)
    row_id = lax.broadcasted_iota(jnp.int32, (SUBLANES, channels), 0)

    def drive(first, last):
        at = slice(first, last)
        total = jnp.zeros((last - first, channels), single)
        for k in range(taps):
            shift = SUBLANES - taps + 1 + k
            total = total + v.padded[first + shift : last + shift, :] * v.taps[k : k + 1, :]
        convolved = total.astype(kind)
        narrow_size, wide_size = (v.narrow.shape[2], v.wide.shape[2])
        spans = []
        for j in range(v.wide.shape[1]):
            base = j * (2 * narrow_size + wide_size)
            spans.append((base, narrow_size, v.narrow, 2 * j))
            spans.append((base + narrow_size, narrow_size, v.narrow, 2 * j + 1))
            spans.append((base + 2 * narrow_size, wide_size, v.wide, j))
        for start, size, maps, head in spans:
            cols = slice(start, start + size)
            piece = convolved[:, cols]
            decay_pre = jnp.dot(piece, maps[0, head], preferred_element_type=single)
            input_pre = jnp.dot(piece, maps[1, head], preferred_element_type=single)
            log_decay = (
                -DECAY_SCALE * jax.nn.sigmoid(decay_pre) * v.soft[:, cols] + v.shift[at, cols]
            )
            decay = jnp.exp(log_decay)
            y2 = 2.0 * log_decay
            series = -y2 * (
                1.0 + y2 * (0.5 + y2 * (1.0 / 6.0 + y2 * (1.0 / 24.0 + y2 * (1.0 / 120.0))))
            )
            lost = jnp.where(y2 > -SERIES_LIMIT, series, 1.0 - decay * decay)
            v.log_keep[at, cols] = decay
            v.drive_keep[at, cols] = (
                jnp.sqrt(lost) * jax.nn.sigmoid(input_pre) * piece.astype(single)
            )

    def tile(i, carried):
        product, state = carried
        at = pl.ds(pl.multiple_of(i * SUBLANES, SUBLANES), SUBLANES)
        a, b = (v.log_keep[at, :], v.drive_keep[at, :])
        hop = 1
        while hop < SUBLANES:
            inside = row_id >= hop
            a_before = jnp.where(inside, pltpu.roll(a, hop, 0), 1.0)
            b_before = jnp.where(inside, pltpu.roll(b, hop, 0), 0.0)
            b = a * b_before + b
            a = a * a_before
            hop *= 2
        b = b + a * state
        a = a * product
        v.factor[at, :] = a
        v.state[at, :] = b
        last = slice(SUBLANES - 1, SUBLANES)
        return (a[last, :], b[last, :])

    def scan(first, last):
        start = (jnp.ones((1, channels), single), jnp.zeros((1, channels), single))
        return lax.fori_loop(first // SUBLANES, last // SUBLANES, tile, start, unroll=2)

    drive(lead, rows)
    scan(lead, rows)
    halo_copy.wait()
    before = v.halo[...].astype(single)[halo_rows - SUBLANES :]
    v.padded[0:SUBLANES, :] = jnp.where(sp > 0, before, jnp.zeros_like(before))
    drive(0, lead)
    lead_factor, lead_state = scan(0, lead)
    rest_factor, rest_state = (v.factor[rows - 1 : rows, :], v.state[rows - 1 : rows, :])
    end_factor = rest_factor * lead_factor
    end_state = rest_state + rest_factor * lead_state
    groups = channels // LANES
    for n in range(groups):
        cols = slice(n * LANES, (n + 1) * LANES)
        v.ends[0, n : n + 1, :] = end_factor[:, cols]
        v.ends[0, groups + n : groups + n + 1, :] = end_state[:, cols]
    end_copies = [
        copy(v.ends.at[0], v.ends.at[k], v.end_send, v.end_recv, later(k))
        for k in range(1, count)
    ]
    for one in end_copies:
        one.start()

    loads["routes"].wait()
    loads["shares"].wait()
    lines = v.weigh_out.shape[1]
    line = lax.broadcasted_iota(jnp.int32, (lines, rows), 0)
    for e in range(count):
        share = jnp.zeros((1, rows), single)
        for n in range(v.routes.shape[0]):
            share = share + jnp.where(
                v.routes[n : n + 1, :] == e, v.shares[n : n + 1, :], 0.0
            )
        v.weigh_out[e] = jnp.where(line == sp, share, 0.0)
    weigh_copies = [
        copy(
            v.weigh_out.at[(sp + k) % count], v.weigh_in.at[k], v.weigh_send, v.weigh_recv,
            later(k),
        )
        for k in range(1, count)
    ]
    for one in weigh_copies:
        one.start()

    loads["gate"].wait()
    g = v.gate[...].astype(single)
    v.gelu[...] = 0.5 * g * (1.0 + jnp.tanh(GELU_SCALE * (g + GELU_CUBIC * g * g * g)))
    for name in ("mixer", "stream", "gain"):
        loads[name].wait()

    others = pl.ds(1, count - 1)
    all_of(v.ends.at[others], v.end_recv).wait_recv()
    carry = jnp.zeros((groups, LANES), single)
    for k in range(count - 1, 0, -1):
        longer = v.ends[k, 0:groups, :] * carry + v.ends[k, groups : 2 * groups, :]
        carry = jnp.where(sp >= k, longer, carry)
    carry = jnp.concatenate([carry[n : n + 1, :] for n in range(groups)], axis=1)
    beyond_lead = lead_state + lead_factor * carry
    row = lax.broadcasted_iota(jnp.int32, (kept, channels), 0)
    order = [(1 - x, 1 - c), (x, 1 - c), (1 - x, c), (x, c)]
    for n, (chip, core) in enumerate(order):
        first = (chip * 2 + core) * kept
        at = pl.ds(pl.multiple_of(first, kept), kept)
        entering = jnp.where(row + first < lead, carry, beyond_lead)
        recurrent = v.state[at, :] + v.factor[at, :] * entering
        v.gated[n * kept : (n + 1) * kept, :] = (recurrent * v.gelu[at, :]).astype(kind)

    pieces = 4
    piece = width // pieces

    def pair(n):
        cols = pl.ds(n * piece, piece)
        return copy(
            v.give.at[:, :, cols], v.got.at[:, :, cols], v.pair_send, v.pair_recv, peer_c
        )

    for n in range(pieces):
        cols = slice(n * piece, (n + 1) * piece)
        value = jnp.dot(v.gated[...], v.mixer[:, cols], preferred_element_type=single)
        v.give[:, :, cols] = value[: 2 * kept].astype(kind).reshape(2, kept, piece)
        v.keep[:, :, cols] = value[2 * kept :].reshape(2, kept, piece)
        pair(n).start()
    all_of(v.got, v.pair_recv).wait_recv()

    def part_of(h):
        return pl.ds(h * half, half)

    bands = v.cross_recv.shape[0]
    band = kept // bands

    def band_of(n):
        return pl.ds(n * band, band)

    def cross(n):
        return copy(
            v.over.at[band_of(n)], v.came.at[band_of(n)], v.cross_send, v.cross_recv.at[n], peer_x
        )

    for n in range(bands):
        at = slice(n * band, (n + 1) * band)
        v.over[at, :] = (v.keep[0, at, :] + v.got[0, at, :].astype(single)).astype(kind)
        cross(n).start()

    xs, part = (v.xs, v.part)

    def ax(k, h, at=None):
        at = part_of(h) if at is None else at
        return copy(
            xs.at[k, 0, at], xs.at[k, DX, at], v.ax_send, v.ax_recv.at[k, h], peer_x
        )

    def ay(k, h, at=None):
        at = part_of(h) if at is None else at
        return copy(
            xs.at[k, 0, at], xs.at[k, DY, at], v.ay_send, v.ay_recv.at[k, h], peer_y
        )

    def fy(k):
        return copy(
            xs.at[k, DX, part_of(0)], xs.at[k, DX + DY, part_of(0)], v.af_send,
            v.af_recv.at[k], peer_y,
        )

    def fx(k):
        return copy(
            xs.at[k, DY, part_of(1)], xs.at[k, DX + DY, part_of(1)], v.af_send,
            v.af_recv.at[k], peer_x,
        )

    def ac(k, s):
        return copy(
            xs.at[k, s], xs.at[k, DC + s], v.ac_send, v.ac_recv.at[k], peer_c
        )

    whole = pl.ds(0, kept)

    def upward(i, at):
        return copy(
            xs.at[i - 1, 0, at], xs.at[i, 0, at], v.up_send.at[i], v.az_recv.at[i], plane(1)
        )

    def downward(i, at):
        return copy(
            xs.at[(depth - i + 1) % depth, 0, at], xs.at[depth - i, 0, at], v.dn_send.at[i],
            v.az_recv.at[depth - i], plane(depth - 1),
        )

    def landed(k):
        return all_of(xs.at[k, 0], v.az_recv.at[k])

    for n in range(bands):
        at = slice(n * band, (n + 1) * band)
        cross(n).wait_recv()
        total = v.keep[1, at, :] + v.got[1, at, :].astype(single) + v.came[at, :].astype(single)
        hidden = (v.stream[at, :].astype(single) + total).astype(kind)
        v.hidden[at, :] = hidden
        wide = hidden.astype(single)
        mean = jnp.mean(wide * wide, axis=-1, keepdims=True)
        normed = wide * lax.rsqrt(mean + NORM_EPSILON) * v.gain[...]
        xs[0, 0, at, :] = normed.astype(kind)
        ax(0, n * 2 // bands, band_of(n)).start()
        ay(0, n * 2 // bands, band_of(n)).start()

        @pl.when(z < depth - 1)
        def _():
            upward(1, band_of(n)).start()

        @pl.when(z > 0)
        def _():
            downward(1, band_of(n)).start()

    ac(0, 0).start()
    all_of(v.weigh_in.at[others], v.weigh_recv).wait_recv()
    table = v.weigh_out[sp]
    for k in range(1, count):
        table = table + v.weigh_in[k]
    filled = jnp.concatenate([table, jnp.zeros((LANES - lines, rows), single)], axis=0)
    v.weigh[...] = jnp.transpose(filled)
    for name in ("gate_w", "up_w", "down_w"):
        loads[name].wait()

    def rc(k):
        return copy(
            part.at[k, pl.ds(DC, DC)], v.from_core.at[k], v.rc_send, v.rc_recv.at[k], peer_c
        )

    def rs(k, n):
        sems = (v.rs_send, v.rs_recv.at[k, min(n, 2)])
        if n == 0:
            return copy(part.at[k, DX + DY, part_of(0)], v.first.at[k, 0], *sems, peer_y)
        if n == 1:
            return copy(part.at[k, DX + DY, part_of(1)], v.first.at[k, 1], *sems, peer_x)
        if n == 2:
            return copy(part.at[k, DY, part_of(0)], v.rest.at[k, 0], *sems, peer_y)
        if n == 3:
            return copy(part.at[k, DX, part_of(1)], v.rest.at[k, 1], *sems, peer_x)
        if n == 4:
            return copy(part.at[k, DX, part_of(0)], v.rest.at[k, 2], *sems, peer_x)
        return copy(part.at[k, DY, part_of(1)], v.rest.at[k, 3], *sems, peer_y)

    def zr(k):
        return copy(
            part.at[k, 0], v.from_z.at[k], v.rz_send, v.rz_recv, plane(depth - k)
        )

    lane = lax.broadcasted_iota(jnp.int32, (kept, LANES), 1)

    def share_of(k, j):
        plane_from = (z + depth - k) % depth
        columns = []
        for s in range(DC):
            y_from = 1 - y if s & DY else y
            x_from = 1 - x if s & DX else x
            c_from = 1 - c if j else c
            at = pl.ds(pl.multiple_of((x_from * 2 + c_from) * kept, kept), kept)
            mine = lane == plane_from * 2 + y_from
            columns.append(
                jnp.sum(jnp.where(mine, v.weigh[at, :], 0.0), axis=1, keepdims=True)
            )
        return jnp.concatenate(columns, axis=0)

    def activated(k, j):
        rows_in = xs[k, j * DC : (j + 1) * DC].reshape(DC * kept, width)
        g = jnp.dot(rows_in, v.gate_w[...], preferred_element_type=single)
        u = jnp.dot(rows_in, v.up_w[...], preferred_element_type=single)
        return (clamp_units(g, u) * share_of(k, j)).astype(kind)

    def theirs(k):
        act = activated(k, 1)
        for n in range(pieces):
            cols = slice(n * piece, (n + 1) * piece)
            down = jnp.dot(act, v.down_w[:, cols], preferred_element_type=single)
            part[k, DC : 2 * DC, :, cols] = down.astype(kind).reshape(DC, kept, piece)
        rc(k).start()

    def ours(k):
        act = activated(k, 0)
        rc(k).wait_recv()
        for n in range(pieces):
            cols = slice(n * piece, (n + 1) * piece)
            down = jnp.dot(act, v.down_w[:, cols], preferred_element_type=single)
            down = down.reshape(DC, kept, piece) + v.from_core[k, :, :, cols].astype(single)
            part[k, 0:DC, :, cols] = down.astype(kind)

    def spread_first(k):
        ax(k, 0).wait_recv()
        fy(k).start()
        ay(k, 1).wait_recv()
        fx(k).start()

    def spread_rest(k):
        ax(k, 1).wait_recv()
        ac(k, DX).start()
        ay(k, 0).wait_recv()
        ac(k, DY).start()

    def spread_last(k):
        all_of(xs.at[k, DX + DY], v.af_recv.at[k]).wait_recv()
        ac(k, DX + DY).start()

    def relay(i):
        @pl.when(i <= z)
        def _():
            landed(i).wait_recv()

            @pl.when(z < depth - 1)
            def _():
                upward(i + 1, whole).start()

        @pl.when(z + i < depth)
        def _():
            landed(depth - i).wait_recv()

            @pl.when(z > 0)
            def _():
                downward(i + 1, whole).start()

    def enter(k):
        ax(k, 0).start()
        ay(k, 1).start()
        ax(k, 1).start()
        ay(k, 0).start()
        ac(k, 0).start()

    def reduce_first(k):
        for n in range(4):
            rs(k, n).start()

    def reduce_next(k):
        rs(k, 0).wait_recv()
        now = part[k, DX, 0:half].astype(single) + v.first[k, 0].astype(single)
        part[k, DX, 0:half] = now.astype(kind)
        rs(k, 4).start()
        rs(k, 1).wait_recv()
        now = part[k, DY, half:kept].astype(single) + v.first[k, 1].astype(single)
        part[k, DY, half:kept] = now.astype(kind)
        rs(k, 5).start()

    def reduced(k):
        all_of(v.rest.at[k], v.rs_recv.at[k, 2]).wait_recv()
        upper = part[k, 0, 0:half].astype(single) + v.rest[k, 0].astype(single)
        lower = part[k, 0, half:kept].astype(single) + v.rest[k, 1].astype(single)
        return (upper + v.rest[k, 2].astype(single), lower + v.rest[k, 3].astype(single))

    def reduce_last(k):
        upper, lower = reduced(k)
        part[k, 0, 0:half] = upper.astype(kind)
        part[k, 0, half:kept] = lower.astype(kind)
        zr(k).start()

    def step(q, none):
        k = turn(z, q % depth, depth)
        k_next = turn(z, (q + 1) % depth, depth)
        k_done = turn(z, (q + depth - 1) % depth, depth)
        k_older = turn(z, (q + depth - 2) % depth, depth)
        live, late = (q < depth, q > 0)

        @pl.when(late)
        def _():
            all_of(xs.at[k_done, pl.ds(DC, DC)], v.ac_recv.at[k_done]).wait_recv()
            theirs(k_done)

        @pl.when(live)
        def _():
            spread_first(k)

        @pl.when(q + 1 < depth)
        def _():
            relay(q + 1)
            enter(k_next)

        @pl.when(q > 3)
        def _():
            reduce_next(k_older)

        @pl.when(late)
        def _():
            ours(k_done)

        @pl.when(q > 2)
        def _():
            reduce_first(k_done)

        @pl.when(live)
        def _():
            spread_rest(k)
            spread_last(k)

        return none

    lax.fori_loop(0, depth + 1, step, 0)
    k_1, k_near, k_far = [turn(z, p, depth) for p in (1, depth - 2, depth - 1)]
    reduce_last(k_near)
    reduce_next(k_far)
    reduce_first(k_1)
    reduce_last(k_far)
    reduce_next(k_1)
    reduce_first(0)
    reduce_last(k_1)
    reduce_next(0)
    upper, lower = reduced(0)
    upper = upper + v.hidden[0:half, :].astype(single)
    lower = lower + v.hidden[half:kept, :].astype(single)
    beyond = pl.ds(1, depth - 1)
    all_of(v.from_z.at[beyond], v.rz_recv).wait_recv()
    for k in range(1, depth):
        upper = upper + v.from_z[k, 0:half].astype(single)
        lower = lower + v.from_z[k, half:kept].astype(single)
    results = []
    for h, value in enumerate((upper, lower)):
        v.result[h * half : (h + 1) * half, :] = value.astype(v.result.dtype)
        results.append(
            pltpu.make_async_copy(
                v.result.at[part_of(h)], v.out.at[part_of(h)], v.result_sem.at[h]
            )
        )
        results[h].start()

    every = pl.ds(0, depth)
    quarter = xs.at[every, pl.ds(0, 1)]
    for ref, sem in (
        (v.weigh_in.at[others], v.weigh_send), (v.ends.at[others], v.end_send),
        (v.give, v.pair_send), (v.over, v.cross_send), (quarter, v.ax_send),
        (quarter, v.ay_send), (quarter, v.af_send), (xs.at[every, pl.ds(0, DC)], v.ac_send),
        (part.at[every, pl.ds(DC, DC)], v.rc_send), (part.at[every, pl.ds(0, 3)], v.rs_send),
        (v.from_z.at[beyond], v.rz_send),
    ):
        all_of(ref, sem).wait_send()
    for i in range(1, depth):

        @pl.when((i - 1 <= z) & (z < depth - 1))
        def _():
            upward(i, whole).wait_send()

        @pl.when((z + i <= depth) & (z > 0))
        def _():
            downward(i, whole).wait_send()

    for one in results:
        one.wait()


def layer(
    conv_input, gate_branch, conv_taps, narrow_maps, wide_maps, decay, decay_shift, mixer_out,
    stream, gain, routes, shares, expert_gate, expert_up, expert_down,
):
    count = lax.axis_size("sp")
    depth = count // 2
    rows, channels = conv_input.shape
    kept, width = stream.shape
    half = kept // 2
    pieces = 4
    lines = -(-count // SUBLANES) * SUBLANES
    single, kind = (jnp.float32, jnp.bfloat16)
    dma = pltpu.SemaphoreType.DMA
    inputs = dict(
        conv=conv_input, gate=gate_branch, taps=conv_taps, narrow=narrow_maps, wide=wide_maps,
        decay=decay, shift=decay_shift, mixer=mixer_out, stream=stream, gain=gain, routes=routes,
        shares=shares, gate_w=expert_gate, up_w=expert_up, down_w=expert_down,
    )
    scratch = {
        name: pltpu.VMEM(one.shape[1:] if name.endswith("_w") else one.shape, one.dtype)
        for name, one in inputs.items()
    }
    flat = pltpu.VMEM((rows, channels), single)
    scratch.update(
        soft=pltpu.VMEM(decay.shape, single),
        gelu=flat,
        halo=pltpu.VMEM((2 * SUBLANES, channels), kind),
        factor=flat,
        state=flat,
        padded=pltpu.VMEM((rows + SUBLANES, channels), single),
        log_keep=flat,
        drive_keep=flat,
        ends=pltpu.VMEM((count, 2 * channels // LANES, LANES), single),
        weigh_out=pltpu.VMEM((count, lines, rows), single),
        weigh_in=pltpu.VMEM((count, lines, rows), single),
        weigh=pltpu.VMEM((rows, LANES), single),
        gated=pltpu.VMEM((rows, channels), kind),
        give=pltpu.VMEM((2, kept, width), kind),
        got=pltpu.VMEM((2, kept, width), kind),
        keep=pltpu.VMEM((2, kept, width), single),
        over=pltpu.VMEM((kept, width), kind),
        came=pltpu.VMEM((kept, width), kind),
        hidden=pltpu.VMEM((kept, width), kind),
        xs=pltpu.VMEM((depth, 2 * DC, kept, width), kind),
        part=pltpu.VMEM((depth, 2 * DC, kept, width), kind),
        from_core=pltpu.VMEM((depth, DC, kept, width), kind),
        first=pltpu.VMEM((depth, 2, half, width), kind),
        rest=pltpu.VMEM((depth, 4, half, width), kind),
        from_z=pltpu.VMEM((depth, kept, width), kind),
        result=pltpu.VMEM((kept, width), kind),
        load_sem=dma((len(inputs),)),
        result_sem=dma((2,)),
        halo_send=dma,
        halo_recv=dma,
    )
    sent = ("weigh", "end", "pair", "cross", "ax", "ay", "af", "ac", "rc", "rs", "rz")
    scratch.update({name + "_send": dma for name in sent})
    landing = dict(
        weigh=(), end=(), pair=(), cross=(4,), ax=(depth, 2), ay=(depth, 2), af=(depth,),
        ac=(depth,), rc=(depth,), rs=(depth, 3), rz=(), az=(depth,),
    )
    scratch.update({name + "_recv": dma(shape) if shape else dma for name, shape in landing.items()})
    scratch.update(up_send=dma((depth,)), dn_send=dma((depth,)))
    names = [name + "_hbm" for name in inputs] + ["out"] + list(scratch)
    return pl.pallas_call(
        functools.partial(layer_kernel, count, names),
        out_shape=jax.ShapeDtypeStruct((kept, width), kind),
        in_specs=[pl.BlockSpec(memory_space=pl.ANY)] * len(inputs),
        out_specs=pl.BlockSpec(memory_space=pl.ANY),
        scratch_shapes=list(scratch.values()),
        compiler_params=pltpu.CompilerParams(
            collective_id=1, has_side_effects=True, vmem_limit_bytes=60 * 1024 * 1024
        ),
    )(*inputs.values())


def shards(
    conv_input,
    gate_branch,
    conv_taps,
    narrow_maps,
    wide_maps,
    decay_param,
    decay_shift,
    mixer_out,
    stream,
    norm_gain,
    routes,
    route_weights,
    expert_gate,
    expert_up,
    expert_down,
):
    seq_rows, channels = conv_input.shape
    tap_count = conv_taps.shape[0]
    tp_count = lax.axis_size("tp")
    tok_local = seq_rows // tp_count
    top_count = routes.shape[1]
    expert_total = expert_gate.shape[0] * lax.axis_size("sp")
    capacity = max(2, 2 * tok_local * top_count // expert_total)
    whole_rows = capacity >= tok_local and expert_gate.shape[0] == 1
    if whole_rows and tp_count == 4 and lax.axis_size("sp") == 8:
        return layer(
            conv_input, gate_branch, conv_taps, narrow_maps, wide_maps, decay_param[None, :],
            decay_shift, mixer_out, stream, norm_gain[None, :], routes.T, route_weights.T,
            expert_gate, expert_up, expert_down,
        )
    own_index = lax.axis_index("tp")
    own_rows = lax.dynamic_slice_in_dim(routes, own_index * tok_local, tok_local, 0)
    own_weights = lax.dynamic_slice_in_dim(route_weights, own_index * tok_local, tok_local, 0)
    soft = jax.nn.softplus(-decay_param)[None, :]
    earlier = shifted(conv_input[seq_rows - tap_count + 1 :], "sp", 1)
    head = jnp.zeros((SUBLANES, channels), jnp.float32)
    head = head.at[SUBLANES - tap_count + 1 :].set(earlier.astype(jnp.float32))
    factors, local_state = mix_local(
        head, conv_input, conv_taps, narrow_maps, wide_maps, soft, decay_shift
    )
    ends = lax.all_gather(jnp.stack([factors[-1], local_state[-1]]), "sp")
    mine = lax.axis_index("sp")
    state = jnp.zeros((channels,), jnp.float32)
    for position in range(lax.axis_size("sp") - 1):
        longer = ends[position, 0] * state + ends[position, 1]
        state = jnp.where(position < mine, longer, state)
    carried = (None, state)
    recurrent = local_state + factors * carried[1]
    gated_rows = (recurrent * jax.nn.gelu(gate_branch.astype(jnp.float32))).astype(jnp.bfloat16)
    mixer_sum = lax.psum_scatter(
        jnp.dot(gated_rows, mixer_out, preferred_element_type=jnp.float32).astype(jnp.bfloat16),
        "tp",
        scatter_dimension=0,
        tiled=True,
    ).astype(jnp.float32)
    hidden_f = stream.astype(jnp.float32) + mixer_sum
    hidden = hidden_f.astype(jnp.bfloat16)
    hidden_f = hidden.astype(jnp.float32)
    normed = (
        hidden_f
        * lax.rsqrt(jnp.mean(hidden_f * hidden_f, axis=-1, keepdims=True) + NORM_EPSILON)
        * norm_gain
    ).astype(jnp.bfloat16)
    model_width = normed.shape[1]
    assignments = tok_local * top_count
    own_routes = own_rows.reshape(assignments)
    own_ranks = slot_ranks(own_routes[None, :], expert_total)[0]
    source = jnp.arange(assignments, dtype=jnp.int32) // top_count
    slot_source = (
        jnp.full((expert_total * capacity,), -1, jnp.int32)
        .at[own_routes * capacity + own_ranks]
        .set(source)
    )
    outgoing = take_rows(normed, slot_source).reshape(expert_total, 1, capacity, model_width)
    partial_value = expert_work(
        lax.all_gather(
            lax.all_to_all(outgoing, "sp", split_axis=0, concat_axis=0, tiled=True),
            "tp",
            axis=1,
            tiled=True,
        ),
        expert_gate,
        expert_up,
        expert_down,
    )
    summed = lax.psum_scatter(
        partial_value.astype(jnp.bfloat16), "tp", scatter_dimension=1, tiled=True
    )
    returned = lax.all_to_all(summed, "sp", split_axis=0, concat_axis=0, tiled=True)
    own_slots = own_routes * capacity + own_ranks
    picked = returned.reshape(expert_total * capacity, model_width)[own_slots]
    combined = jnp.sum(
        picked.reshape(tok_local, top_count, model_width).astype(jnp.float32)
        * own_weights[:, :, None],
        axis=1,
    )
    return (hidden_f + combined).astype(jnp.bfloat16)


def solution(mesh):
    placed = (
        P("sp", "tp"),
        P("sp", "tp"),
        P(None, "tp"),
        P(None, "tp", None, None),
        P(None, "tp", None, None),
        P("tp"),
        P("sp", "tp"),
        P("tp", None),
        P(("sp", "tp"), None),
        P(),
        P("sp", None),
        P("sp", None),
        P("sp", None, "tp"),
        P("sp", None, "tp"),
        P("sp", "tp", None),
    )
    return jax.shard_map(
        shards, mesh=mesh, in_specs=placed, out_specs=P(("sp", "tp"), None), check_vma=False
    )
```

```python
import functools
import types

import jax
import jax.numpy as jnp
from jax import lax
from jax.experimental import pallas as pl
from jax.experimental.pallas import tpu as pltpu
from jax.sharding import PartitionSpec as P

NORM_EPSILON = 1e-06
CLAMP_LIMIT = 7.0
GATE_SLOPE = 1.702
DECAY_SCALE = 8.0


def shifted(block, axis, distance):
    devices = range(lax.axis_size(axis))
    route = [(i - distance, i) for i in devices if i - distance in devices]
    return lax.ppermute(block, axis, route)


def clamp_units(gate_pre, up_pre):
    clamped = jnp.minimum(gate_pre, CLAMP_LIMIT)
    upper = jnp.clip(up_pre, -CLAMP_LIMIT, CLAMP_LIMIT)
    return (upper + 1.0) * clamped * jax.nn.sigmoid(GATE_SLOPE * clamped)


def slot_ranks(flat_routes, expert_total):
    onehot = (
        flat_routes[:, :, None] == jnp.arange(expert_total, dtype=jnp.int32)[None, None, :]
    ).astype(jnp.int32)
    return jnp.sum(jnp.cumsum(onehot, axis=1) * onehot, axis=2) - 1


def take_rows(source_rows, slot_source):
    filled = slot_source >= 0
    picked = source_rows[jnp.maximum(slot_source, 0)]
    return jnp.where(filled[:, None], picked, jnp.zeros_like(picked))


def expert_work(arrived, expert_gate, expert_up, expert_down):
    local_experts = expert_gate.shape[0]
    buffer_shape = arrived.shape
    grouped = arrived.reshape(
        buffer_shape[0] // local_experts,
        local_experts,
        buffer_shape[1] * buffer_shape[2],
        buffer_shape[3],
    )
    gate_pre = jnp.einsum(
        "sxcd,xdf->sxcf", grouped, expert_gate, preferred_element_type=jnp.float32
    )
    up_pre = jnp.einsum("sxcd,xdf->sxcf", grouped, expert_up, preferred_element_type=jnp.float32)
    activation = clamp_units(gate_pre, up_pre).astype(jnp.bfloat16)
    partial_value = jnp.einsum(
        "sxcf,xfd->sxcd", activation, expert_down, preferred_element_type=jnp.float32
    )
    return partial_value.reshape(buffer_shape)


LANES = 128
SUBLANES = 8
DX, DY, DC = 1, 2, 4
SERIES_LIMIT = 0.05
GELU_SCALE = 0.7978845608028654
GELU_CUBIC = 0.044715


def mix_kernel(
    head_ref, conv_ref, taps_ref, narrow_ref, wide_ref, soft_ref, shift_ref,
    factor_ref, state_ref, padded, log_keep, drive_keep,
):
    rows, channels = conv_ref.shape
    taps = taps_ref.shape[0]
    padded[0:SUBLANES, :] = head_ref[...]
    padded[SUBLANES:, :] = conv_ref[...].astype(jnp.float32)
    total = jnp.zeros((rows, channels), jnp.float32)
    for k in range(taps):
        total = total + padded[pl.ds(SUBLANES - taps + 1 + k, rows), :] * taps_ref[k : k + 1, :]
    convolved = total.astype(jnp.bfloat16)
    narrow_size, wide_size = narrow_ref.shape[2], wide_ref.shape[2]
    spans = []
    for j in range(wide_ref.shape[1]):
        base = j * (2 * narrow_size + wide_size)
        spans.append((base, narrow_size, narrow_ref, 2 * j))
        spans.append((base + narrow_size, narrow_size, narrow_ref, 2 * j + 1))
        spans.append((base + 2 * narrow_size, wide_size, wide_ref, j))
    for start, size, maps, head in spans:
        piece = convolved[:, start : start + size]
        decay_pre = jnp.dot(piece, maps[0, head], preferred_element_type=jnp.float32)
        input_pre = jnp.dot(piece, maps[1, head], preferred_element_type=jnp.float32)
        cols = slice(start, start + size)
        log_decay = (
            -DECAY_SCALE * jax.nn.sigmoid(decay_pre) * soft_ref[:, cols] + shift_ref[:, cols]
        )
        decay = jnp.exp(log_decay)
        y = 2.0 * log_decay
        series = -y * (1.0 + y * (0.5 + y * (1.0 / 6.0 + y * (1.0 / 24.0 + y * (1.0 / 120.0)))))
        lost = jnp.where(y > -SERIES_LIMIT, series, 1.0 - decay * decay)
        log_keep[:, cols] = decay
        drive_keep[:, cols] = (
            jnp.sqrt(lost) * jax.nn.sigmoid(input_pre) * piece.astype(jnp.float32)
        )
    row_id = lax.broadcasted_iota(jnp.int32, (SUBLANES, channels), 0)

    def tile(i, carry):
        product, state = carry
        at = pl.ds(pl.multiple_of(i * SUBLANES, SUBLANES), SUBLANES)
        a, b = log_keep[at, :], drive_keep[at, :]
        step = 1
        while step < SUBLANES:
            inside = row_id >= step
            a_before = jnp.where(inside, pltpu.roll(a, step, 0), 1.0)
            b_before = jnp.where(inside, pltpu.roll(b, step, 0), 0.0)
            b = a * b_before + b
            a = a * a_before
            step *= 2
        b = b + a * state
        a = a * product
        factor_ref[at, :] = a
        state_ref[at, :] = b
        last = slice(SUBLANES - 1, SUBLANES)
        return (a[last, :], b[last, :])

    lax.fori_loop(
        0,
        rows // SUBLANES,
        tile,
        (jnp.ones((1, channels), jnp.float32), jnp.zeros((1, channels), jnp.float32)),
    )


def mix_local(head, conv_input, conv_taps, narrow_maps, wide_maps, soft, decay_shift):
    shape = conv_input.shape
    flat = jax.ShapeDtypeStruct(shape, jnp.float32)
    return pl.pallas_call(
        mix_kernel,
        out_shape=(flat, flat),
        in_specs=[pl.BlockSpec(memory_space=pltpu.VMEM)] * 7,
        out_specs=(pl.BlockSpec(memory_space=pltpu.VMEM),) * 2,
        scratch_shapes=[
            pltpu.VMEM((shape[0] + SUBLANES, shape[1]), jnp.float32),
            pltpu.VMEM(shape, jnp.float32),
            pltpu.VMEM(shape, jnp.float32),
        ],
        compiler_params=pltpu.CompilerParams(vmem_limit_bytes=32 * 1024 * 1024),
    )(head, conv_input, conv_taps, narrow_maps, wide_maps, soft, decay_shift)


def turn(z, p, depth):
    return jnp.where(p == 0, 0, jnp.where(z % 2 == 1, p, depth - p))


def layer_kernel(count, names, *refs):
    v = types.SimpleNamespace(**dict(zip(names, refs)))
    rows, channels = v.conv.shape
    kept, width = v.stream.shape
    depth = count // 2
    half = kept // 2
    single, kind = (jnp.float32, jnp.bfloat16)
    sp, tp = (lax.axis_index("sp"), lax.axis_index("tp"))
    z, y = (sp // 2, sp % 2)
    x, c = (tp // 2, tp % 2)
    mesh_id = pl.DeviceIdType.MESH
    peer_c = {"sp": sp, "tp": x * 2 + 1 - c}
    peer_x = {"sp": sp, "tp": (1 - x) * 2 + c}
    peer_y = {"sp": z * 2 + 1 - y, "tp": tp}

    def plane(k):
        return {"sp": ((z + k) % depth) * 2 + y, "tp": tp}

    def later(k):
        return {"sp": (sp + k) % count, "tp": tp}

    def copy(src, dst, send, recv, peer):
        return pltpu.make_async_remote_copy(
            src_ref=src, dst_ref=dst, send_sem=send, recv_sem=recv,
            device_id=peer, device_id_type=mesh_id,
        )

    def all_of(ref, sem):
        return copy(ref, ref, sem, sem, peer_c)

    barrier = pltpu.get_barrier_semaphore()
    peers = [peer_x, peer_c] + [later(k) for k in range(1, count)]
    for peer in peers:
        pl.semaphore_signal(barrier, inc=1, device_id=peer, device_id_type=mesh_id)
    load_names = (
        "conv", "taps", "narrow", "wide", "decay", "shift", "gate", "routes", "shares", "stream",
        "gain", "mixer", "gate_w", "up_w", "down_w",
    )
    loads = {}
    for n, name in enumerate(load_names):
        source = getattr(v, name + "_hbm")
        source = source.at[0] if name.endswith("_w") else source
        loads[name] = pltpu.make_async_copy(source, getattr(v, name), v.load_sem.at[n])
        loads[name].start()

    loads["conv"].wait()
    pl.semaphore_wait(barrier, len(peers))
    halo_rows = v.halo.shape[0]
    halo_copy = copy(
        v.conv.at[pl.ds(rows - halo_rows, halo_rows)], v.halo, v.halo_send, v.halo_recv, later(1)
    )
    halo_copy.start()

    loads["decay"].wait()
    t = jnp.exp(-v.decay[...])
    v.soft[...] = t * (1.0 - t * (0.5 - t * (1.0 / 3.0 - t * (0.25 - t * (0.2 - t * (1.0 / 6.0))))))
    for name in ("taps", "narrow", "wide", "shift"):
        loads[name].wait()
    taps = v.taps.shape[0]
    lead = 2 * SUBLANES
    v.padded[SUBLANES:, :] = v.conv[...].astype(single)
    row_id = lax.broadcasted_iota(jnp.int32, (SUBLANES, channels), 0)

    def drive(first, last):
        at = slice(first, last)
        total = jnp.zeros((last - first, channels), single)
        for k in range(taps):
            shift = SUBLANES - taps + 1 + k
            total = total + v.padded[first + shift : last + shift, :] * v.taps[k : k + 1, :]
        convolved = total.astype(kind)
        narrow_size, wide_size = (v.narrow.shape[2], v.wide.shape[2])
        spans = []
        for j in range(v.wide.shape[1]):
            base = j * (2 * narrow_size + wide_size)
            spans.append((base, narrow_size, v.narrow, 2 * j))
            spans.append((base + narrow_size, narrow_size, v.narrow, 2 * j + 1))
            spans.append((base + 2 * narrow_size, wide_size, v.wide, j))
        for start, size, maps, head in spans:
            cols = slice(start, start + size)
            piece = convolved[:, cols]
            decay_pre = jnp.dot(piece, maps[0, head], preferred_element_type=single)
            input_pre = jnp.dot(piece, maps[1, head], preferred_element_type=single)
            log_decay = (
                -DECAY_SCALE * jax.nn.sigmoid(decay_pre) * v.soft[:, cols] + v.shift[at, cols]
            )
            decay = jnp.exp(log_decay)
            y2 = 2.0 * log_decay
            series = -y2 * (
                1.0 + y2 * (0.5 + y2 * (1.0 / 6.0 + y2 * (1.0 / 24.0 + y2 * (1.0 / 120.0))))
            )
            lost = jnp.where(y2 > -SERIES_LIMIT, series, 1.0 - decay * decay)
            v.log_keep[at, cols] = decay
            v.drive_keep[at, cols] = (
                jnp.sqrt(lost) * jax.nn.sigmoid(input_pre) * piece.astype(single)
            )

    def tile(i, carried):
        product, state = carried
        at = pl.ds(pl.multiple_of(i * SUBLANES, SUBLANES), SUBLANES)
        a, b = (v.log_keep[at, :], v.drive_keep[at, :])
        hop = 1
        while hop < SUBLANES:
            inside = row_id >= hop
            a_before = jnp.where(inside, pltpu.roll(a, hop, 0), 1.0)
            b_before = jnp.where(inside, pltpu.roll(b, hop, 0), 0.0)
            b = a * b_before + b
            a = a * a_before
            hop *= 2
        b = b + a * state
        a = a * product
        v.factor[at, :] = a
        v.state[at, :] = b
        last = slice(SUBLANES - 1, SUBLANES)
        return (a[last, :], b[last, :])

    def scan(first, last):
        start = (jnp.ones((1, channels), single), jnp.zeros((1, channels), single))
        return lax.fori_loop(first // SUBLANES, last // SUBLANES, tile, start, unroll=2)

    drive(lead, rows)
    scan(lead, rows)
    halo_copy.wait()
    before = v.halo[...].astype(single)[halo_rows - SUBLANES :]
    v.padded[0:SUBLANES, :] = jnp.where(sp > 0, before, jnp.zeros_like(before))
    drive(0, lead)
    lead_factor, lead_state = scan(0, lead)
    rest_factor, rest_state = (v.factor[rows - 1 : rows, :], v.state[rows - 1 : rows, :])
    end_factor = rest_factor * lead_factor
    end_state = rest_state + rest_factor * lead_state
    groups = channels // LANES
    for n in range(groups):
        cols = slice(n * LANES, (n + 1) * LANES)
        v.ends[0, n : n + 1, :] = end_factor[:, cols]
        v.ends[0, groups + n : groups + n + 1, :] = end_state[:, cols]
    end_copies = [
        copy(v.ends.at[0], v.ends.at[k], v.end_send, v.end_recv, later(k))
        for k in range(1, count)
    ]
    for one in end_copies:
        one.start()

    loads["routes"].wait()
    loads["shares"].wait()
    lines = v.weigh_out.shape[1]
    line = lax.broadcasted_iota(jnp.int32, (lines, rows), 0)
    for e in range(count):
        share = jnp.zeros((1, rows), single)
        for n in range(v.routes.shape[0]):
            share = share + jnp.where(
                v.routes[n : n + 1, :] == e, v.shares[n : n + 1, :], 0.0
            )
        v.weigh_out[e] = jnp.where(line == sp, share, 0.0)
    weigh_copies = [
        copy(
            v.weigh_out.at[(sp + k) % count], v.weigh_in.at[k], v.weigh_send, v.weigh_recv,
            later(k),
        )
        for k in range(1, count)
    ]
    for one in weigh_copies:
        one.start()

    loads["gate"].wait()
    g = v.gate[...].astype(single)
    v.gelu[...] = 0.5 * g * (1.0 + jnp.tanh(GELU_SCALE * (g + GELU_CUBIC * g * g * g)))
    for name in ("mixer", "stream", "gain"):
        loads[name].wait()

    others = pl.ds(1, count - 1)
    all_of(v.ends.at[others], v.end_recv).wait_recv()
    carry = jnp.zeros((groups, LANES), single)
    for k in range(count - 1, 0, -1):
        longer = v.ends[k, 0:groups, :] * carry + v.ends[k, groups : 2 * groups, :]
        carry = jnp.where(sp >= k, longer, carry)
    carry = jnp.concatenate([carry[n : n + 1, :] for n in range(groups)], axis=1)
    beyond_lead = lead_state + lead_factor * carry
    row = lax.broadcasted_iota(jnp.int32, (kept, channels), 0)
    order = [(1 - x, 1 - c), (x, 1 - c), (1 - x, c), (x, c)]
    for n, (chip, core) in enumerate(order):
        first = (chip * 2 + core) * kept
        at = pl.ds(pl.multiple_of(first, kept), kept)
        entering = jnp.where(row + first < lead, carry, beyond_lead)
        recurrent = v.state[at, :] + v.factor[at, :] * entering
        v.gated[n * kept : (n + 1) * kept, :] = (recurrent * v.gelu[at, :]).astype(kind)

    pieces = 4
    piece = width // pieces

    def pair(n):
        cols = pl.ds(n * piece, piece)
        return copy(
            v.give.at[:, :, cols], v.got.at[:, :, cols], v.pair_send, v.pair_recv, peer_c
        )

    for n in range(pieces):
        cols = slice(n * piece, (n + 1) * piece)
        value = jnp.dot(v.gated[...], v.mixer[:, cols], preferred_element_type=single)
        v.give[:, :, cols] = value[: 2 * kept].astype(kind).reshape(2, kept, piece)
        v.keep[:, :, cols] = value[2 * kept :].reshape(2, kept, piece)
        pair(n).start()
    all_of(v.got, v.pair_recv).wait_recv()

    def part_of(h):
        return pl.ds(h * half, half)

    bands = v.cross_recv.shape[0]
    band = kept // bands

    def band_of(n):
        return pl.ds(n * band, band)

    def cross(n):
        return copy(
            v.over.at[band_of(n)], v.came.at[band_of(n)], v.cross_send, v.cross_recv.at[n], peer_x
        )

    for n in range(bands):
        at = slice(n * band, (n + 1) * band)
        v.over[at, :] = (v.keep[0, at, :] + v.got[0, at, :].astype(single)).astype(kind)
        cross(n).start()

    xs, part = (v.xs, v.part)

    def ax(k, h, at=None):
        at = part_of(h) if at is None else at
        return copy(
            xs.at[k, 0, at], xs.at[k, DX, at], v.ax_send, v.ax_recv.at[k, h], peer_x
        )

    def ay(k, h, at=None):
        at = part_of(h) if at is None else at
        return copy(
            xs.at[k, 0, at], xs.at[k, DY, at], v.ay_send, v.ay_recv.at[k, h], peer_y
        )

    def fy(k):
        return copy(
            xs.at[k, DX, part_of(0)], xs.at[k, DX + DY, part_of(0)], v.af_send,
            v.af_recv.at[k], peer_y,
        )

    def fx(k):
        return copy(
            xs.at[k, DY, part_of(1)], xs.at[k, DX + DY, part_of(1)], v.af_send,
            v.af_recv.at[k], peer_x,
        )

    def ac(k, s):
        return copy(
            xs.at[k, s], xs.at[k, DC + s], v.ac_send, v.ac_recv.at[k], peer_c
        )

    whole = pl.ds(0, kept)

    def upward(i, at):
        return copy(
            xs.at[i - 1, 0, at], xs.at[i, 0, at], v.up_send.at[i], v.az_recv.at[i], plane(1)
        )

    def downward(i, at):
        return copy(
            xs.at[(depth - i + 1) % depth, 0, at], xs.at[depth - i, 0, at], v.dn_send.at[i],
            v.az_recv.at[depth - i], plane(depth - 1),
        )

    def landed(k):
        return all_of(xs.at[k, 0], v.az_recv.at[k])

    for n in range(bands):
        at = slice(n * band, (n + 1) * band)
        cross(n).wait_recv()
        total = v.keep[1, at, :] + v.got[1, at, :].astype(single) + v.came[at, :].astype(single)
        hidden = (v.stream[at, :].astype(single) + total).astype(kind)
        v.hidden[at, :] = hidden
        wide = hidden.astype(single)
        mean = jnp.mean(wide * wide, axis=-1, keepdims=True)
        normed = wide * lax.rsqrt(mean + NORM_EPSILON) * v.gain[...]
        xs[0, 0, at, :] = normed.astype(kind)
        ax(0, n * 2 // bands, band_of(n)).start()
        ay(0, n * 2 // bands, band_of(n)).start()

        @pl.when(z < depth - 1)
        def _():
            upward(1, band_of(n)).start()

        @pl.when(z > 0)
        def _():
            downward(1, band_of(n)).start()

    ac(0, 0).start()
    all_of(v.weigh_in.at[others], v.weigh_recv).wait_recv()
    table = v.weigh_out[sp]
    for k in range(1, count):
        table = table + v.weigh_in[k]
    filled = jnp.concatenate([table, jnp.zeros((LANES - lines, rows), single)], axis=0)
    v.weigh[...] = jnp.transpose(filled)
    for name in ("gate_w", "up_w", "down_w"):
        loads[name].wait()

    def rc(k, cols):
        at = pl.ds(cols.start, cols.stop - cols.start)
        return copy(
            part.at[k, pl.ds(DC, DC), :, at], v.from_core.at[k, :, :, at], v.rc_send,
            v.rc_recv.at[k], peer_c,
        )

    def rs(k, n):
        sems = (v.rs_send, v.rs_recv.at[k, min(n, 2)])
        if n == 0:
            return copy(part.at[k, DX + DY, part_of(0)], v.first.at[k, 0], *sems, peer_y)
        if n == 1:
            return copy(part.at[k, DX + DY, part_of(1)], v.first.at[k, 1], *sems, peer_x)
        if n == 2:
            return copy(part.at[k, DY, part_of(0)], v.rest.at[k, 0], *sems, peer_y)
        if n == 3:
            return copy(part.at[k, DX, part_of(1)], v.rest.at[k, 1], *sems, peer_x)
        if n == 4:
            return copy(part.at[k, DX, part_of(0)], v.rest.at[k, 2], *sems, peer_x)
        return copy(part.at[k, DY, part_of(1)], v.rest.at[k, 3], *sems, peer_y)

    last = depth - 1
    at_end = (z == 0) | (z == last)
    beside = z + 1 - 2 * (z % 2)
    inward = jnp.where(z == 0, 1, last - 1)
    across = jnp.where(z == 1, last, 0)

    bulk = v.from_pair.shape[1]
    remnant = pl.ds(bulk, kept - bulk)
    pair_device = {"sp": beside * 2 + y, "tp": tp}
    over_y, over_x = (z * 2 + 1 - y, (1 - x) * 2 + c)
    peer_1 = {"sp": (1 - c) * sp + c * over_y, "tp": (1 - c) * over_x + c * tp}
    peer_2 = {"sp": (1 - c) * over_y + c * sp, "tp": (1 - c) * tp + c * over_x}

    def to_pair(k):
        return copy(
            part.at[k, pl.ds(0, DC), pl.ds(0, bulk)], v.from_pair, v.rp_send, v.rp_recv,
            pair_device,
        )

    def rq(k, n):
        if n == 0:
            there = part.at[k, DX + DY, remnant]
            return copy(there, v.from_1, v.rq_send, v.rq_recv.at[0], peer_1)
        if n == 1:
            there = part.at[k, DX + c, remnant]
            return copy(there, v.from_2.at[0], v.rq_send, v.rq_recv.at[1], peer_1)
        if n == 2:
            there = part.at[k, DY - c, remnant]
            return copy(there, v.from_2.at[1], v.rq_send, v.rq_recv.at[1], peer_2)
        return copy(part.at[k, 0, remnant], v.from_3, v.rq_send, v.rq_recv.at[2], pair_device)

    def remnant_next(k):
        rq(k, 0).wait_recv()
        now = part[k, DY - c, bulk:kept].astype(single) + v.from_1[...].astype(single)
        part[k, DY - c, bulk:kept] = now.astype(kind)
        rq(k, 2).start()

    def remnant_last(k):
        all_of(v.from_2, v.rq_recv.at[1]).wait_recv()
        now = part[k, 0, bulk:kept].astype(single) + v.from_2[0].astype(single)
        part[k, 0, bulk:kept] = (now + v.from_2[1].astype(single)).astype(kind)
        rq(k, 3).start()

    def zr(p, k):
        to = jnp.where(at_end, inward, across) if p == 2 else last - z
        return copy(
            part.at[k, 0], v.from_z.at[p - 2], v.rz_send, v.rz_recv.at[p - 2],
            {"sp": to * 2 + y, "tp": tp},
        )

    lane = lax.broadcasted_iota(jnp.int32, (kept, LANES), 1)

    def share_of(k, j):
        plane_from = (z + depth - k) % depth
        columns = []
        for s in range(DC):
            y_from = 1 - y if s & DY else y
            x_from = 1 - x if s & DX else x
            c_from = 1 - c if j else c
            at = pl.ds(pl.multiple_of((x_from * 2 + c_from) * kept, kept), kept)
            mine = lane == plane_from * 2 + y_from
            columns.append(
                jnp.sum(jnp.where(mine, v.weigh[at, :], 0.0), axis=1, keepdims=True)
            )
        return jnp.concatenate(columns, axis=0)

    def activated(k, j):
        rows_in = xs[k, j * DC : (j + 1) * DC].reshape(DC * kept, width)
        g = jnp.dot(rows_in, v.gate_w[...], preferred_element_type=single)
        u = jnp.dot(rows_in, v.up_w[...], preferred_element_type=single)
        return (clamp_units(g, u) * share_of(k, j)).astype(kind)

    def theirs_first(k):
        v.act[...] = activated(k, 1)

    def theirs_next(k):
        for n in range(pieces):
            cols = slice(n * piece, (n + 1) * piece)
            down = jnp.dot(v.act[...], v.down_w[:, cols], preferred_element_type=single)
            part[k, DC : 2 * DC, :, cols] = down.astype(kind).reshape(DC, kept, piece)
            rc(k, cols).start()

    def ours(k):
        act = activated(k, 0)
        all_of(v.from_core.at[k], v.rc_recv.at[k]).wait_recv()
        for n in range(pieces):
            cols = slice(n * piece, (n + 1) * piece)
            down = jnp.dot(act, v.down_w[:, cols], preferred_element_type=single)
            down = down.reshape(DC, kept, piece) + v.from_core[k, :, :, cols].astype(single)
            part[k, 0:DC, :, cols] = down.astype(kind)

    def spread_first(k):
        ax(k, 0).wait_recv()
        fy(k).start()
        ay(k, 1).wait_recv()
        fx(k).start()

    def spread_rest(k):
        ax(k, 1).wait_recv()
        ac(k, DX).start()
        ay(k, 0).wait_recv()
        ac(k, DY).start()

    def spread_last(k):
        all_of(xs.at[k, DX + DY], v.af_recv.at[k]).wait_recv()
        ac(k, DX + DY).start()

    def relay(i):
        @pl.when(i <= z)
        def _():
            landed(i).wait_recv()

            @pl.when(z < depth - 1)
            def _():
                upward(i + 1, whole).start()

        @pl.when(z + i < depth)
        def _():
            landed(depth - i).wait_recv()

            @pl.when(z > 0)
            def _():
                downward(i + 1, whole).start()

    def enter(k):
        ax(k, 0).start()
        ay(k, 1).start()
        ax(k, 1).start()
        ay(k, 0).start()
        ac(k, 0).start()

    def reduce_first(k):
        for n in range(4):
            rs(k, n).start()

    def reduce_next(k):
        rs(k, 0).wait_recv()
        now = part[k, DX, 0:half].astype(single) + v.first[k, 0].astype(single)
        part[k, DX, 0:half] = now.astype(kind)
        rs(k, 4).start()
        rs(k, 1).wait_recv()
        now = part[k, DY, half:kept].astype(single) + v.first[k, 1].astype(single)
        part[k, DY, half:kept] = now.astype(kind)
        rs(k, 5).start()

    def reduced(k):
        all_of(v.rest.at[k], v.rs_recv.at[k, 2]).wait_recv()
        upper = part[k, 0, 0:half].astype(single) + v.rest[k, 0].astype(single)
        lower = part[k, 0, half:kept].astype(single) + v.rest[k, 1].astype(single)
        return (upper + v.rest[k, 2].astype(single), lower + v.rest[k, 3].astype(single))

    def reduce_last(p, k):
        upper, lower = reduced(k)
        part[k, 0, 0:half] = upper.astype(kind)
        part[k, 0, half:kept] = lower.astype(kind)
        if p == 3:

            @pl.when((z > 0) & (z < last))
            def _():
                all_of(v.from_z.at[0], v.rz_recv.at[0]).wait_recv()
                now = part[k, 0].astype(single) + v.from_z[0].astype(single)
                part[k, 0] = now.astype(kind)

        zr(p, k).start()

    def step(q, none):
        k = turn(z, q % depth, depth)
        k_next = turn(z, (q + 1) % depth, depth)
        k_done = turn(z, (q + depth - 1) % depth, depth)
        k_older = turn(z, (q + depth - 2) % depth, depth)
        live, late = (q < depth, q > 0)

        @pl.when(late)
        def _():
            all_of(xs.at[k_done, pl.ds(DC, DC)], v.ac_recv.at[k_done]).wait_recv()
            theirs_first(k_done)

        @pl.when(live)
        def _():
            spread_first(k)

        @pl.when(late)
        def _():
            theirs_next(k_done)

        @pl.when(q + 1 < depth)
        def _():
            relay(q + 1)
            enter(k_next)

        @pl.when(q > 3)
        def _():
            reduce_next(k_older)

        @pl.when(late)
        def _():
            ours(k_done)

        @pl.when(q == 2)
        def _():
            to_pair(k_done).start()

        @pl.when(q > 2)
        def _():
            reduce_first(k_done)

        @pl.when(live)
        def _():
            spread_rest(k)
            spread_last(k)

        return none

    lax.fori_loop(0, depth + 1, step, 0)
    k_pair, k_near, k_far = [turn(z, p, depth) for p in (1, 2, 3)]
    reduce_last(2, k_near)
    all_of(v.from_pair, v.rp_recv).wait_recv()
    for n in range(DC):
        now = part[0, n, 0:bulk].astype(single) + v.from_pair[n].astype(single)
        part[0, n, 0:bulk] = now.astype(kind)
    reduce_next(k_far)
    rq(k_pair, 0).start()
    rq(k_pair, 1).start()
    reduce_first(0)
    reduce_last(3, k_far)
    remnant_next(k_pair)
    reduce_next(0)
    remnant_last(k_pair)
    upper, lower = reduced(0)
    upper = upper + v.hidden[0:half, :].astype(single)
    lower = lower + v.hidden[half:kept, :].astype(single)

    @pl.when(at_end)
    def _():
        all_of(v.from_z.at[0], v.rz_recv.at[0]).wait_recv()

    all_of(v.from_z.at[1], v.rz_recv.at[1]).wait_recv()
    direct = jnp.where(at_end, 1.0, 0.0)
    upper = upper + direct * v.from_z[0, 0:half].astype(single)
    lower = lower + direct * v.from_z[0, half:kept].astype(single)
    upper = upper + v.from_z[1, 0:half].astype(single)
    lower = lower + v.from_z[1, half:kept].astype(single)
    rq(k_pair, 3).wait_recv()
    rest = jnp.concatenate(
        [jnp.zeros((bulk - half, width), single), v.from_3[...].astype(single)], axis=0
    )
    lower = lower + rest
    for h, value in enumerate((upper, lower)):
        v.out[h * half : (h + 1) * half, :] = value.astype(v.out.dtype)
    every = pl.ds(0, depth)
    quarter = xs.at[every, pl.ds(0, 1)]
    for ref, sem in (
        (v.weigh_in.at[others], v.weigh_send), (v.ends.at[others], v.end_send),
        (v.give, v.pair_send), (v.over, v.cross_send), (quarter, v.ax_send),
        (quarter, v.ay_send), (quarter, v.af_send), (xs.at[every, pl.ds(0, DC)], v.ac_send),
        (part.at[every, pl.ds(DC, DC)], v.rc_send), (part.at[pl.ds(1, last), pl.ds(0, 3)], v.rs_send),
        (v.from_z, v.rz_send), (v.from_pair, v.rp_send), (part.at[0, 0], v.rq_send),
    ):
        all_of(ref, sem).wait_send()
    for i in range(1, depth):

        @pl.when((i - 1 <= z) & (z < depth - 1))
        def _():
            upward(i, whole).wait_send()

        @pl.when((z + i <= depth) & (z > 0))
        def _():
            downward(i, whole).wait_send()


def layer(
    conv_input, gate_branch, conv_taps, narrow_maps, wide_maps, decay, decay_shift, mixer_out,
    stream, gain, routes, shares, expert_gate, expert_up, expert_down,
):
    count = lax.axis_size("sp")
    depth = count // 2
    rows, channels = conv_input.shape
    kept, width = stream.shape
    half = kept // 2
    pieces = 4
    bulk = kept * 3 // 4
    lines = -(-count // SUBLANES) * SUBLANES
    single, kind = (jnp.float32, jnp.bfloat16)
    dma = pltpu.SemaphoreType.DMA
    inputs = dict(
        conv=conv_input, gate=gate_branch, taps=conv_taps, narrow=narrow_maps, wide=wide_maps,
        decay=decay, shift=decay_shift, mixer=mixer_out, stream=stream, gain=gain, routes=routes,
        shares=shares, gate_w=expert_gate, up_w=expert_up, down_w=expert_down,
    )
    scratch = {
        name: pltpu.VMEM(one.shape[1:] if name.endswith("_w") else one.shape, one.dtype)
        for name, one in inputs.items()
    }
    flat = pltpu.VMEM((rows, channels), single)
    scratch.update(
        soft=pltpu.VMEM(decay.shape, single),
        gelu=flat,
        halo=pltpu.VMEM((2 * SUBLANES, channels), kind),
        factor=flat,
        state=flat,
        padded=pltpu.VMEM((rows + SUBLANES, channels), single),
        log_keep=flat,
        drive_keep=flat,
        ends=pltpu.VMEM((count, 2 * channels // LANES, LANES), single),
        weigh_out=pltpu.VMEM((count, lines, rows), single),
        weigh_in=pltpu.VMEM((count, lines, rows), single),
        weigh=pltpu.VMEM((rows, LANES), single),
        gated=pltpu.VMEM((rows, channels), kind),
        give=pltpu.VMEM((2, kept, width), kind),
        got=pltpu.VMEM((2, kept, width), kind),
        keep=pltpu.VMEM((2, kept, width), single),
        over=pltpu.VMEM((kept, width), kind),
        came=pltpu.VMEM((kept, width), kind),
        hidden=pltpu.VMEM((kept, width), kind),
        xs=pltpu.VMEM((depth, 2 * DC, kept, width), kind),
        act=pltpu.VMEM((DC * kept, expert_gate.shape[2]), kind),
        part=pltpu.VMEM((depth, 2 * DC, kept, width), kind),
        from_core=pltpu.VMEM((depth, DC, kept, width), kind),
        first=pltpu.VMEM((depth, 2, half, width), kind),
        rest=pltpu.VMEM((depth, 4, half, width), kind),
        from_z=pltpu.VMEM((2, kept, width), kind),
        from_pair=pltpu.VMEM((DC, bulk, width), kind),
        from_1=pltpu.VMEM((kept - bulk, width), kind),
        from_2=pltpu.VMEM((2, kept - bulk, width), kind),
        from_3=pltpu.VMEM((kept - bulk, width), kind),
        load_sem=dma((len(inputs),)),
        halo_send=dma,
        halo_recv=dma,
    )
    sent = ("weigh", "end", "pair", "cross", "ax", "ay", "af", "ac", "rc", "rs", "rz", "rp", "rq")
    scratch.update({name + "_send": dma for name in sent})
    landing = dict(
        weigh=(), end=(), pair=(), cross=(4,), ax=(depth, 2), ay=(depth, 2), af=(depth,),
        ac=(depth,), rc=(depth,), rs=(depth, 3), rz=(2,), rp=(), rq=(3,), az=(depth,),
    )
    scratch.update({name + "_recv": dma(shape) if shape else dma for name, shape in landing.items()})
    scratch.update(up_send=dma((depth,)), dn_send=dma((depth,)))
    names = [name + "_hbm" for name in inputs] + ["out"] + list(scratch)
    return pl.pallas_call(
        functools.partial(layer_kernel, count, names),
        out_shape=pltpu.VMEM((kept, width), kind),
        in_specs=[pl.BlockSpec(memory_space=pl.ANY)] * len(inputs),
        out_specs=pl.BlockSpec(memory_space=pltpu.VMEM),
        scratch_shapes=list(scratch.values()),
        compiler_params=pltpu.CompilerParams(
            collective_id=1, has_side_effects=True, vmem_limit_bytes=60 * 1024 * 1024
        ),
    )(*inputs.values())


def shards(
    conv_input,
    gate_branch,
    conv_taps,
    narrow_maps,
    wide_maps,
    decay_param,
    decay_shift,
    mixer_out,
    stream,
    norm_gain,
    routes,
    route_weights,
    expert_gate,
    expert_up,
    expert_down,
):
    seq_rows, channels = conv_input.shape
    tap_count = conv_taps.shape[0]
    tp_count = lax.axis_size("tp")
    tok_local = seq_rows // tp_count
    top_count = routes.shape[1]
    expert_total = expert_gate.shape[0] * lax.axis_size("sp")
    capacity = max(2, 2 * tok_local * top_count // expert_total)
    whole_rows = capacity >= tok_local and expert_gate.shape[0] == 1
    if whole_rows and tp_count == 4 and lax.axis_size("sp") == 8:
        return layer(
            conv_input, gate_branch, conv_taps, narrow_maps, wide_maps, decay_param[None, :],
            decay_shift, mixer_out, stream, norm_gain[None, :], routes.T, route_weights.T,
            expert_gate, expert_up, expert_down,
        )
    own_index = lax.axis_index("tp")
    own_rows = lax.dynamic_slice_in_dim(routes, own_index * tok_local, tok_local, 0)
    own_weights = lax.dynamic_slice_in_dim(route_weights, own_index * tok_local, tok_local, 0)
    soft = jax.nn.softplus(-decay_param)[None, :]
    earlier = shifted(conv_input[seq_rows - tap_count + 1 :], "sp", 1)
    head = jnp.zeros((SUBLANES, channels), jnp.float32)
    head = head.at[SUBLANES - tap_count + 1 :].set(earlier.astype(jnp.float32))
    factors, local_state = mix_local(
        head, conv_input, conv_taps, narrow_maps, wide_maps, soft, decay_shift
    )
    ends = lax.all_gather(jnp.stack([factors[-1], local_state[-1]]), "sp")
    mine = lax.axis_index("sp")
    state = jnp.zeros((channels,), jnp.float32)
    for position in range(lax.axis_size("sp") - 1):
        longer = ends[position, 0] * state + ends[position, 1]
        state = jnp.where(position < mine, longer, state)
    carried = (None, state)
    recurrent = local_state + factors * carried[1]
    gated_rows = (recurrent * jax.nn.gelu(gate_branch.astype(jnp.float32))).astype(jnp.bfloat16)
    mixer_sum = lax.psum_scatter(
        jnp.dot(gated_rows, mixer_out, preferred_element_type=jnp.float32).astype(jnp.bfloat16),
        "tp",
        scatter_dimension=0,
        tiled=True,
    ).astype(jnp.float32)
    hidden_f = stream.astype(jnp.float32) + mixer_sum
    hidden = hidden_f.astype(jnp.bfloat16)
    hidden_f = hidden.astype(jnp.float32)
    normed = (
        hidden_f
        * lax.rsqrt(jnp.mean(hidden_f * hidden_f, axis=-1, keepdims=True) + NORM_EPSILON)
        * norm_gain
    ).astype(jnp.bfloat16)
    model_width = normed.shape[1]
    assignments = tok_local * top_count
    own_routes = own_rows.reshape(assignments)
    own_ranks = slot_ranks(own_routes[None, :], expert_total)[0]
    source = jnp.arange(assignments, dtype=jnp.int32) // top_count
    slot_source = (
        jnp.full((expert_total * capacity,), -1, jnp.int32)
        .at[own_routes * capacity + own_ranks]
        .set(source)
    )
    outgoing = take_rows(normed, slot_source).reshape(expert_total, 1, capacity, model_width)
    partial_value = expert_work(
        lax.all_gather(
            lax.all_to_all(outgoing, "sp", split_axis=0, concat_axis=0, tiled=True),
            "tp",
            axis=1,
            tiled=True,
        ),
        expert_gate,
        expert_up,
        expert_down,
    )
    summed = lax.psum_scatter(
        partial_value.astype(jnp.bfloat16), "tp", scatter_dimension=1, tiled=True
    )
    returned = lax.all_to_all(summed, "sp", split_axis=0, concat_axis=0, tiled=True)
    own_slots = own_routes * capacity + own_ranks
    picked = returned.reshape(expert_total * capacity, model_width)[own_slots]
    combined = jnp.sum(
        picked.reshape(tok_local, top_count, model_width).astype(jnp.float32)
        * own_weights[:, :, None],
        axis=1,
    )
    return (hidden_f + combined).astype(jnp.bfloat16)


def solution(mesh):
    placed = (
        P("sp", "tp"),
        P("sp", "tp"),
        P(None, "tp"),
        P(None, "tp", None, None),
        P(None, "tp", None, None),
        P("tp"),
        P("sp", "tp"),
        P("tp", None),
        P(("sp", "tp"), None),
        P(),
        P("sp", None),
        P("sp", None),
        P("sp", None, "tp"),
        P("sp", None, "tp"),
        P("sp", "tp", None),
    )
    return jax.shard_map(
        shards, mesh=mesh, in_specs=placed, out_specs=P(("sp", "tp"), None), check_vma=False
    )
```

```python
import functools
import types

import jax
import jax.numpy as jnp
from jax import lax
from jax.experimental import pallas as pl
from jax.experimental.pallas import tpu as pltpu
from jax.sharding import PartitionSpec as P

NORM_EPSILON = 1e-06
CLAMP_LIMIT = 7.0
GATE_SLOPE = 1.702
DECAY_SCALE = 8.0


def shifted(block, axis, distance):
    devices = range(lax.axis_size(axis))
    route = [(i - distance, i) for i in devices if i - distance in devices]
    return lax.ppermute(block, axis, route)


def clamp_units(gate_pre, up_pre):
    clamped = jnp.minimum(gate_pre, CLAMP_LIMIT)
    upper = jnp.clip(up_pre, -CLAMP_LIMIT, CLAMP_LIMIT)
    return (upper + 1.0) * clamped * jax.nn.sigmoid(GATE_SLOPE * clamped)


def slot_ranks(flat_routes, expert_total):
    onehot = (
        flat_routes[:, :, None] == jnp.arange(expert_total, dtype=jnp.int32)[None, None, :]
    ).astype(jnp.int32)
    return jnp.sum(jnp.cumsum(onehot, axis=1) * onehot, axis=2) - 1


def take_rows(source_rows, slot_source):
    filled = slot_source >= 0
    picked = source_rows[jnp.maximum(slot_source, 0)]
    return jnp.where(filled[:, None], picked, jnp.zeros_like(picked))


def expert_work(arrived, expert_gate, expert_up, expert_down):
    local_experts = expert_gate.shape[0]
    buffer_shape = arrived.shape
    grouped = arrived.reshape(
        buffer_shape[0] // local_experts,
        local_experts,
        buffer_shape[1] * buffer_shape[2],
        buffer_shape[3],
    )
    gate_pre = jnp.einsum(
        "sxcd,xdf->sxcf", grouped, expert_gate, preferred_element_type=jnp.float32
    )
    up_pre = jnp.einsum("sxcd,xdf->sxcf", grouped, expert_up, preferred_element_type=jnp.float32)
    activation = clamp_units(gate_pre, up_pre).astype(jnp.bfloat16)
    partial_value = jnp.einsum(
        "sxcf,xfd->sxcd", activation, expert_down, preferred_element_type=jnp.float32
    )
    return partial_value.reshape(buffer_shape)


LANES = 128
SUBLANES = 8
DX, DY, DC = 1, 2, 4
SERIES_LIMIT = 0.05
GELU_SCALE = 0.7978845608028654
GELU_CUBIC = 0.044715


def mix_kernel(
    head_ref, conv_ref, taps_ref, narrow_ref, wide_ref, soft_ref, shift_ref,
    factor_ref, state_ref, padded, log_keep, drive_keep,
):
    rows, channels = conv_ref.shape
    taps = taps_ref.shape[0]
    padded[0:SUBLANES, :] = head_ref[...]
    padded[SUBLANES:, :] = conv_ref[...].astype(jnp.float32)
    total = jnp.zeros((rows, channels), jnp.float32)
    for k in range(taps):
        total = total + padded[pl.ds(SUBLANES - taps + 1 + k, rows), :] * taps_ref[k : k + 1, :]
    convolved = total.astype(jnp.bfloat16)
    narrow_size, wide_size = narrow_ref.shape[2], wide_ref.shape[2]
    spans = []
    for j in range(wide_ref.shape[1]):
        base = j * (2 * narrow_size + wide_size)
        spans.append((base, narrow_size, narrow_ref, 2 * j))
        spans.append((base + narrow_size, narrow_size, narrow_ref, 2 * j + 1))
        spans.append((base + 2 * narrow_size, wide_size, wide_ref, j))
    for start, size, maps, head in spans:
        piece = convolved[:, start : start + size]
        decay_pre = jnp.dot(piece, maps[0, head], preferred_element_type=jnp.float32)
        input_pre = jnp.dot(piece, maps[1, head], preferred_element_type=jnp.float32)
        cols = slice(start, start + size)
        log_decay = (
            -DECAY_SCALE * jax.nn.sigmoid(decay_pre) * soft_ref[:, cols] + shift_ref[:, cols]
        )
        decay = jnp.exp(log_decay)
        y = 2.0 * log_decay
        series = -y * (1.0 + y * (0.5 + y * (1.0 / 6.0 + y * (1.0 / 24.0 + y * (1.0 / 120.0)))))
        lost = jnp.where(y > -SERIES_LIMIT, series, 1.0 - decay * decay)
        log_keep[:, cols] = decay
        drive_keep[:, cols] = (
            jnp.sqrt(lost) * jax.nn.sigmoid(input_pre) * piece.astype(jnp.float32)
        )
    row_id = lax.broadcasted_iota(jnp.int32, (SUBLANES, channels), 0)

    def tile(i, carry):
        product, state = carry
        at = pl.ds(pl.multiple_of(i * SUBLANES, SUBLANES), SUBLANES)
        a, b = log_keep[at, :], drive_keep[at, :]
        step = 1
        while step < SUBLANES:
            inside = row_id >= step
            a_before = jnp.where(inside, pltpu.roll(a, step, 0), 1.0)
            b_before = jnp.where(inside, pltpu.roll(b, step, 0), 0.0)
            b = a * b_before + b
            a = a * a_before
            step *= 2
        b = b + a * state
        a = a * product
        factor_ref[at, :] = a
        state_ref[at, :] = b
        last = slice(SUBLANES - 1, SUBLANES)
        return (a[last, :], b[last, :])

    lax.fori_loop(
        0,
        rows // SUBLANES,
        tile,
        (jnp.ones((1, channels), jnp.float32), jnp.zeros((1, channels), jnp.float32)),
    )


def mix_local(head, conv_input, conv_taps, narrow_maps, wide_maps, soft, decay_shift):
    shape = conv_input.shape
    flat = jax.ShapeDtypeStruct(shape, jnp.float32)
    return pl.pallas_call(
        mix_kernel,
        out_shape=(flat, flat),
        in_specs=[pl.BlockSpec(memory_space=pltpu.VMEM)] * 7,
        out_specs=(pl.BlockSpec(memory_space=pltpu.VMEM),) * 2,
        scratch_shapes=[
            pltpu.VMEM((shape[0] + SUBLANES, shape[1]), jnp.float32),
            pltpu.VMEM(shape, jnp.float32),
            pltpu.VMEM(shape, jnp.float32),
        ],
        compiler_params=pltpu.CompilerParams(vmem_limit_bytes=32 * 1024 * 1024),
    )(head, conv_input, conv_taps, narrow_maps, wide_maps, soft, decay_shift)


def turn(z, p, depth):
    return jnp.where(p == 0, 0, jnp.where(z % 2 == 1, p, depth - p))


def layer_kernel(count, names, *refs):
    v = types.SimpleNamespace(**dict(zip(names, refs)))
    rows, channels = v.conv.shape
    kept, width = v.stream.shape
    depth = count // 2
    half = kept // 2
    single, kind = (jnp.float32, jnp.bfloat16)
    sp, tp = (lax.axis_index("sp"), lax.axis_index("tp"))
    z, y = (sp // 2, sp % 2)
    x, c = (tp // 2, tp % 2)
    mesh_id = pl.DeviceIdType.MESH
    peer_c = {"sp": sp, "tp": x * 2 + 1 - c}
    peer_x = {"sp": sp, "tp": (1 - x) * 2 + c}
    peer_y = {"sp": z * 2 + 1 - y, "tp": tp}

    def plane(k):
        return {"sp": ((z + k) % depth) * 2 + y, "tp": tp}

    def later(k):
        return {"sp": (sp + k) % count, "tp": tp}

    def copy(src, dst, send, recv, peer):
        return pltpu.make_async_remote_copy(
            src_ref=src, dst_ref=dst, send_sem=send, recv_sem=recv,
            device_id=peer, device_id_type=mesh_id,
        )

    def all_of(ref, sem):
        return copy(ref, ref, sem, sem, peer_c)

    barrier = pltpu.get_barrier_semaphore()
    peers = [peer_x, peer_c] + [later(k) for k in range(1, count)]
    for peer in peers:
        pl.semaphore_signal(barrier, inc=1, device_id=peer, device_id_type=mesh_id)
    load_names = (
        "conv", "taps", "narrow", "wide", "decay", "shift", "gate", "routes", "shares", "stream",
        "gain", "mixer", "gate_w", "up_w", "down_w",
    )
    loads = {}
    for n, name in enumerate(load_names):
        source = getattr(v, name + "_hbm")
        source = source.at[0] if name.endswith("_w") else source
        loads[name] = pltpu.make_async_copy(source, getattr(v, name), v.load_sem.at[n])
        loads[name].start()

    loads["conv"].wait()
    pl.semaphore_wait(barrier, len(peers))
    halo_rows = v.halo.shape[0]
    halo_copy = copy(
        v.conv.at[pl.ds(rows - halo_rows, halo_rows)], v.halo, v.halo_send, v.halo_recv, later(1)
    )
    halo_copy.start()

    loads["decay"].wait()
    t = jnp.exp(-v.decay[...])
    v.soft[...] = t * (1.0 - t * (0.5 - t * (1.0 / 3.0 - t * (0.25 - t * (0.2 - t * (1.0 / 6.0))))))
    for name in ("taps", "narrow", "wide", "shift"):
        loads[name].wait()
    taps = v.taps.shape[0]
    lead = 2 * SUBLANES
    v.padded[SUBLANES:, :] = v.conv[...].astype(single)
    row_id = lax.broadcasted_iota(jnp.int32, (SUBLANES, channels), 0)

    def drive(first, last):
        at = slice(first, last)
        total = jnp.zeros((last - first, channels), single)
        for k in range(taps):
            shift = SUBLANES - taps + 1 + k
            total = total + v.padded[first + shift : last + shift, :] * v.taps[k : k + 1, :]
        convolved = total.astype(kind)
        narrow_size, wide_size = (v.narrow.shape[2], v.wide.shape[2])
        spans = []
        for j in range(v.wide.shape[1]):
            base = j * (2 * narrow_size + wide_size)
            spans.append((base, narrow_size, v.narrow, 2 * j))
            spans.append((base + narrow_size, narrow_size, v.narrow, 2 * j + 1))
            spans.append((base + 2 * narrow_size, wide_size, v.wide, j))
        for start, size, maps, head in spans:
            cols = slice(start, start + size)
            piece = convolved[:, cols]
            decay_pre = jnp.dot(piece, maps[0, head], preferred_element_type=single)
            input_pre = jnp.dot(piece, maps[1, head], preferred_element_type=single)
            log_decay = (
                -DECAY_SCALE * jax.nn.sigmoid(decay_pre) * v.soft[:, cols] + v.shift[at, cols]
            )
            decay = jnp.exp(log_decay)
            y2 = 2.0 * log_decay
            series = -y2 * (
                1.0 + y2 * (0.5 + y2 * (1.0 / 6.0 + y2 * (1.0 / 24.0 + y2 * (1.0 / 120.0))))
            )
            lost = jnp.where(y2 > -SERIES_LIMIT, series, 1.0 - decay * decay)
            v.log_keep[at, cols] = decay
            v.drive_keep[at, cols] = (
                jnp.sqrt(lost) * jax.nn.sigmoid(input_pre) * piece.astype(single)
            )

    def tile(i, carried):
        product, state = carried
        at = pl.ds(pl.multiple_of(i * SUBLANES, SUBLANES), SUBLANES)
        a, b = (v.log_keep[at, :], v.drive_keep[at, :])
        hop = 1
        while hop < SUBLANES:
            inside = row_id >= hop
            a_before = jnp.where(inside, pltpu.roll(a, hop, 0), 1.0)
            b_before = jnp.where(inside, pltpu.roll(b, hop, 0), 0.0)
            b = a * b_before + b
            a = a * a_before
            hop *= 2
        b = b + a * state
        a = a * product
        v.factor[at, :] = a
        v.state[at, :] = b
        last = slice(SUBLANES - 1, SUBLANES)
        return (a[last, :], b[last, :])

    def scan(first, last):
        start = (jnp.ones((1, channels), single), jnp.zeros((1, channels), single))
        return lax.fori_loop(first // SUBLANES, last // SUBLANES, tile, start, unroll=2)

    drive(lead, rows)
    scan(lead, rows)
    halo_copy.wait()
    before = v.halo[...].astype(single)[halo_rows - SUBLANES :]
    v.padded[0:SUBLANES, :] = jnp.where(sp > 0, before, jnp.zeros_like(before))
    drive(0, lead)
    lead_factor, lead_state = scan(0, lead)
    rest_factor, rest_state = (v.factor[rows - 1 : rows, :], v.state[rows - 1 : rows, :])
    end_factor = rest_factor * lead_factor
    end_state = rest_state + rest_factor * lead_state
    groups = channels // LANES
    for n in range(groups):
        cols = slice(n * LANES, (n + 1) * LANES)
        v.ends[0, n : n + 1, :] = end_factor[:, cols]
        v.ends[0, groups + n : groups + n + 1, :] = end_state[:, cols]
    end_copies = [
        copy(v.ends.at[0], v.ends.at[k], v.end_send, v.end_recv, later(k))
        for k in range(1, count)
    ]
    for one in end_copies:
        one.start()

    loads["routes"].wait()
    loads["shares"].wait()
    lines = v.weigh_out.shape[1]
    line = lax.broadcasted_iota(jnp.int32, (lines, rows), 0)
    for e in range(count):
        share = jnp.zeros((1, rows), single)
        for n in range(v.routes.shape[0]):
            share = share + jnp.where(
                v.routes[n : n + 1, :] == e, v.shares[n : n + 1, :], 0.0
            )
        v.weigh_out[e] = jnp.where(line == sp, share, 0.0)
    weigh_copies = [
        copy(
            v.weigh_out.at[(sp + k) % count], v.weigh_in.at[k], v.weigh_send, v.weigh_recv,
            later(k),
        )
        for k in range(1, count)
    ]
    for one in weigh_copies:
        one.start()

    loads["gate"].wait()
    g = v.gate[...].astype(single)
    v.gelu[...] = 0.5 * g * (1.0 + jnp.tanh(GELU_SCALE * (g + GELU_CUBIC * g * g * g)))
    for name in ("mixer", "stream", "gain"):
        loads[name].wait()

    others = pl.ds(1, count - 1)
    all_of(v.ends.at[others], v.end_recv).wait_recv()
    carry = jnp.zeros((groups, LANES), single)
    for k in range(count - 1, 0, -1):
        longer = v.ends[k, 0:groups, :] * carry + v.ends[k, groups : 2 * groups, :]
        carry = jnp.where(sp >= k, longer, carry)
    carry = jnp.concatenate([carry[n : n + 1, :] for n in range(groups)], axis=1)
    beyond_lead = lead_state + lead_factor * carry
    row = lax.broadcasted_iota(jnp.int32, (kept, channels), 0)
    order = [(1 - x, 1 - c), (x, 1 - c), (1 - x, c), (x, c)]
    for n, (chip, core) in enumerate(order):
        first = (chip * 2 + core) * kept
        at = pl.ds(pl.multiple_of(first, kept), kept)
        entering = jnp.where(row + first < lead, carry, beyond_lead)
        recurrent = v.state[at, :] + v.factor[at, :] * entering
        v.gated[n * kept : (n + 1) * kept, :] = (recurrent * v.gelu[at, :]).astype(kind)

    pieces = 4
    piece = width // pieces

    def pair(n):
        cols = pl.ds(n * piece, piece)
        return copy(
            v.give.at[:, :, cols], v.got.at[:, :, cols], v.pair_send, v.pair_recv, peer_c
        )

    for n in range(pieces):
        cols = slice(n * piece, (n + 1) * piece)
        value = jnp.dot(v.gated[...], v.mixer[:, cols], preferred_element_type=single)
        v.give[:, :, cols] = value[: 2 * kept].astype(kind).reshape(2, kept, piece)
        v.keep[:, :, cols] = value[2 * kept :].reshape(2, kept, piece)
        pair(n).start()
    all_of(v.got, v.pair_recv).wait_recv()

    def part_of(h):
        return pl.ds(h * half, half)

    bands = v.cross_recv.shape[0]
    band = kept // bands

    def band_of(n):
        return pl.ds(n * band, band)

    def cross(n):
        return copy(
            v.over.at[band_of(n)], v.came.at[band_of(n)], v.cross_send, v.cross_recv.at[n], peer_x
        )

    for n in range(bands):
        at = slice(n * band, (n + 1) * band)
        v.over[at, :] = (v.keep[0, at, :] + v.got[0, at, :].astype(single)).astype(kind)
        cross(n).start()

    xs, part = (v.xs, v.part)

    def ax(k, h, at=None):
        at = part_of(h) if at is None else at
        return copy(
            xs.at[k, 0, at], xs.at[k, DX, at], v.ax_send, v.ax_recv.at[k, h], peer_x
        )

    def ay(k, h, at=None):
        at = part_of(h) if at is None else at
        return copy(
            xs.at[k, 0, at], xs.at[k, DY, at], v.ay_send, v.ay_recv.at[k, h], peer_y
        )

    def fy(k):
        return copy(
            xs.at[k, DX, part_of(0)], xs.at[k, DX + DY, part_of(0)], v.af_send,
            v.af_recv.at[k], peer_y,
        )

    def fx(k):
        return copy(
            xs.at[k, DY, part_of(1)], xs.at[k, DX + DY, part_of(1)], v.af_send,
            v.af_recv.at[k], peer_x,
        )

    def ac(k, s):
        return copy(
            xs.at[k, s], xs.at[k, DC + s], v.ac_send, v.ac_recv.at[k], peer_c
        )

    whole = pl.ds(0, kept)
    beside = z + 1 - 2 * (z % 2)
    pair_device = {"sp": beside * 2 + y, "tp": tp}
    pair_slot = 1 + (z % 2) * (depth - 2)

    def lift_x():
        return copy(
            xs.at[0, DX, part_of(0)], xs.at[pair_slot, DX, part_of(0)], v.ax_send,
            v.ax_recv.at[pair_slot, 0], pair_device,
        )

    def lift_y():
        return copy(
            xs.at[0, DY, part_of(1)], xs.at[pair_slot, DY, part_of(1)], v.ay_send,
            v.ay_recv.at[pair_slot, 1], pair_device,
        )

    def upward(i, at):
        return copy(
            xs.at[i - 1, 0, at], xs.at[i, 0, at], v.up_send.at[i], v.az_recv.at[i], plane(1)
        )

    def downward(i, at):
        return copy(
            xs.at[(depth - i + 1) % depth, 0, at], xs.at[depth - i, 0, at], v.dn_send.at[i],
            v.az_recv.at[depth - i], plane(depth - 1),
        )

    def landed(k):
        return all_of(xs.at[k, 0], v.az_recv.at[k])

    for n in range(bands):
        at = slice(n * band, (n + 1) * band)
        cross(n).wait_recv()
        total = v.keep[1, at, :] + v.got[1, at, :].astype(single) + v.came[at, :].astype(single)
        hidden = (v.stream[at, :].astype(single) + total).astype(kind)
        v.hidden[at, :] = hidden
        wide = hidden.astype(single)
        mean = jnp.mean(wide * wide, axis=-1, keepdims=True)
        normed = wide * lax.rsqrt(mean + NORM_EPSILON) * v.gain[...]
        xs[0, 0, at, :] = normed.astype(kind)
        ax(0, n * 2 // bands, band_of(n)).start()
        ay(0, n * 2 // bands, band_of(n)).start()

        @pl.when(z < depth - 1)
        def _():
            upward(1, band_of(n)).start()

        @pl.when(z > 0)
        def _():
            downward(1, band_of(n)).start()

    ac(0, 0).start()
    all_of(v.weigh_in.at[others], v.weigh_recv).wait_recv()
    table = v.weigh_out[sp]
    for k in range(1, count):
        table = table + v.weigh_in[k]
    filled = jnp.concatenate([table, jnp.zeros((LANES - lines, rows), single)], axis=0)
    v.weigh[...] = jnp.transpose(filled)
    for name in ("gate_w", "up_w", "down_w"):
        loads[name].wait()

    def rc(k, cols):
        at = pl.ds(cols.start, cols.stop - cols.start)
        return copy(
            part.at[k, pl.ds(DC, DC), :, at], v.from_core.at[k, :, :, at], v.rc_send,
            v.rc_recv.at[k], peer_c,
        )

    def rs(k, n):
        sems = (v.rs_send, v.rs_recv.at[k, min(n, 2)])
        if n == 0:
            return copy(part.at[k, DX + DY, part_of(0)], v.first.at[k, 0], *sems, peer_y)
        if n == 1:
            return copy(part.at[k, DX + DY, part_of(1)], v.first.at[k, 1], *sems, peer_x)
        if n == 2:
            return copy(part.at[k, DY, part_of(0)], v.rest.at[k, 0], *sems, peer_y)
        if n == 3:
            return copy(part.at[k, DX, part_of(1)], v.rest.at[k, 1], *sems, peer_x)
        if n == 4:
            return copy(part.at[k, DX, part_of(0)], v.rest.at[k, 2], *sems, peer_x)
        return copy(part.at[k, DY, part_of(1)], v.rest.at[k, 3], *sems, peer_y)

    last = depth - 1
    at_end = (z == 0) | (z == last)
    inward = jnp.where(z == 0, 1, last - 1)
    across = jnp.where(z == 1, last, 0)

    bulk = v.from_pair.shape[1]
    remnant = pl.ds(bulk, kept - bulk)
    over_y, over_x = (z * 2 + 1 - y, (1 - x) * 2 + c)
    peer_1 = {"sp": (1 - c) * sp + c * over_y, "tp": (1 - c) * over_x + c * tp}
    peer_2 = {"sp": (1 - c) * over_y + c * sp, "tp": (1 - c) * tp + c * over_x}

    def to_pair(k):
        return copy(
            part.at[k, pl.ds(0, DC), pl.ds(0, bulk)], v.from_pair, v.rp_send, v.rp_recv,
            pair_device,
        )

    def rq(k, n):
        if n == 0:
            there = part.at[k, DX + DY, remnant]
            return copy(there, v.from_1, v.rq_send, v.rq_recv.at[0], peer_1)
        if n == 1:
            there = part.at[k, DX + c, remnant]
            return copy(there, v.from_2.at[0], v.rq_send, v.rq_recv.at[1], peer_1)
        if n == 2:
            there = part.at[k, DY - c, remnant]
            return copy(there, v.from_2.at[1], v.rq_send, v.rq_recv.at[1], peer_2)
        return copy(part.at[k, 0, remnant], v.from_3, v.rq_send, v.rq_recv.at[2], pair_device)

    def remnant_next(k):
        rq(k, 0).wait_recv()
        now = part[k, DY - c, bulk:kept].astype(single) + v.from_1[...].astype(single)
        part[k, DY - c, bulk:kept] = now.astype(kind)
        rq(k, 2).start()

    def remnant_last(k):
        all_of(v.from_2, v.rq_recv.at[1]).wait_recv()
        now = part[k, 0, bulk:kept].astype(single) + v.from_2[0].astype(single)
        part[k, 0, bulk:kept] = (now + v.from_2[1].astype(single)).astype(kind)
        rq(k, 3).start()

    def zr_near(k):
        to = jnp.where(at_end, inward, across)
        return copy(
            part.at[k, 0], v.from_z.at[0], v.rz_send, v.rz_recv.at[0], {"sp": to * 2 + y, "tp": tp}
        )

    small = half // 2

    def slim(h, t):
        return pl.ds(h * half + t * small, small)

    def zr_far(k, h, t):
        return copy(
            part.at[k, 0, slim(h, t)], v.from_z.at[1, slim(h, t)], v.rz_send, v.rz_recv.at[1],
            {"sp": (last - z) * 2 + y, "tp": tp},
        )

    def rt(k, t, n):
        here = slim(0, t)
        sems = (v.rs_send, v.rt_recv.at[t, min(n, 2)])
        if n == 0:
            return copy(part.at[k, DX + DY, here], v.first.at[k, 0, here], *sems, peer_y)
        if n == 1:
            return copy(part.at[k, DX + DY, slim(1, t)], v.first.at[k, 1, here], *sems, peer_x)
        if n == 2:
            return copy(part.at[k, DY, here], v.rest.at[k, 0, here], *sems, peer_y)
        if n == 3:
            return copy(part.at[k, DX, slim(1, t)], v.rest.at[k, 1, here], *sems, peer_x)
        if n == 4:
            return copy(part.at[k, DX, here], v.rest.at[k, 2, here], *sems, peer_x)
        return copy(part.at[k, DY, slim(1, t)], v.rest.at[k, 3, here], *sems, peer_y)

    def slim_next(k, t):
        here = slice(t * small, (t + 1) * small)
        there = slice(half + t * small, half + (t + 1) * small)
        rt(k, t, 0).wait_recv()
        now = part[k, DX, here].astype(single) + v.first[k, 0, here].astype(single)
        part[k, DX, here] = now.astype(kind)
        rt(k, t, 4).start()
        rt(k, t, 1).wait_recv()
        now = part[k, DY, there].astype(single) + v.first[k, 1, here].astype(single)
        part[k, DY, there] = now.astype(kind)
        rt(k, t, 5).start()

    def slim_last(k, t):
        here = slice(t * small, (t + 1) * small)
        all_of(v.rest.at[k, pl.ds(0, 4), slim(0, t)], v.rt_recv.at[t, 2]).wait_recv()
        inner = (z > 0) & (z < last)
        if t == 0:

            @pl.when(inner)
            def _():
                all_of(v.from_z.at[0], v.rz_recv.at[0]).wait_recv()

        for h in range(2):
            rows_h = slice(h * half + t * small, h * half + (t + 1) * small)
            now = part[k, 0, rows_h].astype(single) + v.rest[k, h, here].astype(single)
            now = now + v.rest[k, h + 2, here].astype(single)
            part[k, 0, rows_h] = now.astype(kind)

            @pl.when(inner)
            def _():
                more = part[k, 0, rows_h].astype(single) + v.from_z[0, rows_h].astype(single)
                part[k, 0, rows_h] = more.astype(kind)

            zr_far(k, h, t).start()

    lane = lax.broadcasted_iota(jnp.int32, (kept, LANES), 1)

    def share_of(k, j):
        plane_from = (z + depth - k) % depth
        columns = []
        for s in range(DC):
            y_from = 1 - y if s & DY else y
            x_from = 1 - x if s & DX else x
            c_from = 1 - c if j else c
            at = pl.ds(pl.multiple_of((x_from * 2 + c_from) * kept, kept), kept)
            mine = lane == plane_from * 2 + y_from
            columns.append(
                jnp.sum(jnp.where(mine, v.weigh[at, :], 0.0), axis=1, keepdims=True)
            )
        return jnp.concatenate(columns, axis=0)

    def activated(k, j):
        rows_in = xs[k, j * DC : (j + 1) * DC].reshape(DC * kept, width)
        g = jnp.dot(rows_in, v.gate_w[...], preferred_element_type=single)
        u = jnp.dot(rows_in, v.up_w[...], preferred_element_type=single)
        return (clamp_units(g, u) * share_of(k, j)).astype(kind)

    def theirs_first(k):
        v.act[...] = activated(k, 1)

    def theirs_next(k):
        for n in range(pieces):
            cols = slice(n * piece, (n + 1) * piece)
            down = jnp.dot(v.act[...], v.down_w[:, cols], preferred_element_type=single)
            part[k, DC : 2 * DC, :, cols] = down.astype(kind).reshape(DC, kept, piece)
            rc(k, cols).start()

    def ours(k):
        act = activated(k, 0)
        all_of(v.from_core.at[k], v.rc_recv.at[k]).wait_recv()
        for n in range(pieces):
            cols = slice(n * piece, (n + 1) * piece)
            down = jnp.dot(act, v.down_w[:, cols], preferred_element_type=single)
            down = down.reshape(DC, kept, piece) + v.from_core[k, :, :, cols].astype(single)
            part[k, 0:DC, :, cols] = down.astype(kind)

    def spread_first(k, q):
        ax(k, 0).wait_recv()
        fy(k).start()

        @pl.when((q == 0) & (c == 0))
        def _():
            lift_x().start()

        ay(k, 1).wait_recv()
        fx(k).start()

        @pl.when((q == 0) & (c == 1))
        def _():
            lift_y().start()

    def spread_second(k):
        ax(k, 0).wait_recv()
        fy(k).start()
        ay(k, 1).wait_recv()
        fx(k).start()

    def spread_rest(k):
        ax(k, 1).wait_recv()
        ac(k, DX).start()
        ay(k, 0).wait_recv()
        ac(k, DY).start()

    def spread_last(k):
        all_of(xs.at[k, DX + DY], v.af_recv.at[k]).wait_recv()
        ac(k, DX + DY).start()

    def relay(i):
        @pl.when(i <= z)
        def _():
            landed(i).wait_recv()

            @pl.when(z < depth - 1)
            def _():
                upward(i + 1, whole).start()

        @pl.when(z + i < depth)
        def _():
            landed(depth - i).wait_recv()

            @pl.when(z > 0)
            def _():
                downward(i + 1, whole).start()

    def enter(k, q):
        @pl.when((q > 0) | (c == 1))
        def _():
            ax(k, 0).start()

        @pl.when((q > 0) | (c == 0))
        def _():
            ay(k, 1).start()

        ax(k, 1).start()
        ay(k, 0).start()
        ac(k, 0).start()

    def reduce_first(k):
        for n in range(4):
            rs(k, n).start()

    def reduce_next(k):
        rs(k, 0).wait_recv()
        now = part[k, DX, 0:half].astype(single) + v.first[k, 0].astype(single)
        part[k, DX, 0:half] = now.astype(kind)
        rs(k, 4).start()
        rs(k, 1).wait_recv()
        now = part[k, DY, half:kept].astype(single) + v.first[k, 1].astype(single)
        part[k, DY, half:kept] = now.astype(kind)
        rs(k, 5).start()

    def reduced(k):
        all_of(v.rest.at[k], v.rs_recv.at[k, 2]).wait_recv()
        upper = part[k, 0, 0:half].astype(single) + v.rest[k, 0].astype(single)
        lower = part[k, 0, half:kept].astype(single) + v.rest[k, 1].astype(single)
        return (upper + v.rest[k, 2].astype(single), lower + v.rest[k, 3].astype(single))

    def reduce_last(k):
        upper, lower = reduced(k)
        part[k, 0, 0:half] = upper.astype(kind)
        part[k, 0, half:kept] = lower.astype(kind)
        zr_near(k).start()

    def step(q, none):
        k = turn(z, q % depth, depth)
        k_next = turn(z, (q + 1) % depth, depth)
        k_done = turn(z, (q + depth - 1) % depth, depth)
        k_older = turn(z, (q + depth - 2) % depth, depth)
        live, late = (q < depth, q > 0)

        @pl.when(q < last)
        def _():
            spread_first(k, q)

        @pl.when(late)
        def _():
            all_of(xs.at[k_done, pl.ds(DC, DC)], v.ac_recv.at[k_done]).wait_recv()
            theirs_first(k_done)

        @pl.when(q == last)
        def _():
            spread_second(k)

        @pl.when(late)
        def _():
            theirs_next(k_done)

        @pl.when(q + 1 < depth)
        def _():
            relay(q + 1)
            enter(k_next, q)
            spread_rest(k)

        @pl.when(q > 3)
        def _():
            reduce_next(k_older)

        @pl.when(late)
        def _():
            ours(k_done)

        @pl.when(q == 2)
        def _():
            to_pair(k_done).start()

        @pl.when(q == last)
        def _():
            reduce_first(k_done)

        @pl.when(q > last)
        def _():
            for n in range(4):
                rt(k_done, 0, n).start()
            rt(k_done, 1, 0).start()
            rt(k_done, 1, 1).start()

        @pl.when(q == last)
        def _():
            spread_rest(k)

        @pl.when(live)
        def _():
            spread_last(k)

        return none

    lax.fori_loop(0, depth + 1, step, 0)
    k_pair, k_near, k_far = [turn(z, p, depth) for p in (1, 2, 3)]
    reduce_last(k_near)
    slim_next(k_far, 0)
    rt(k_far, 1, 2).start()
    rt(k_far, 1, 3).start()
    all_of(v.from_pair, v.rp_recv).wait_recv()
    for n in range(DC):
        now = part[0, n, 0:bulk].astype(single) + v.from_pair[n].astype(single)
        part[0, n, 0:bulk] = now.astype(kind)
    slim_next(k_far, 1)
    rq(k_pair, 0).start()
    rq(k_pair, 1).start()
    reduce_first(0)
    slim_last(k_far, 0)
    slim_last(k_far, 1)
    remnant_next(k_pair)
    reduce_next(0)
    remnant_last(k_pair)
    upper, lower = reduced(0)
    upper = upper + v.hidden[0:half, :].astype(single)
    lower = lower + v.hidden[half:kept, :].astype(single)

    @pl.when(at_end)
    def _():
        all_of(v.from_z.at[0], v.rz_recv.at[0]).wait_recv()

    all_of(v.from_z.at[1], v.rz_recv.at[1]).wait_recv()
    direct = jnp.where(at_end, 1.0, 0.0)
    upper = upper + direct * v.from_z[0, 0:half].astype(single)
    lower = lower + direct * v.from_z[0, half:kept].astype(single)
    upper = upper + v.from_z[1, 0:half].astype(single)
    lower = lower + v.from_z[1, half:kept].astype(single)
    rq(k_pair, 3).wait_recv()
    rest = jnp.concatenate(
        [jnp.zeros((bulk - half, width), single), v.from_3[...].astype(single)], axis=0
    )
    lower = lower + rest
    for h, value in enumerate((upper, lower)):
        v.out[h * half : (h + 1) * half, :] = value.astype(v.out.dtype)
    every = pl.ds(0, depth)
    quarter = xs.at[every, pl.ds(0, 1)]
    for ref, sem in (
        (v.weigh_in.at[others], v.weigh_send), (v.ends.at[others], v.end_send),
        (v.give, v.pair_send), (v.over, v.cross_send), (quarter, v.ax_send),
        (quarter, v.ay_send), (quarter, v.af_send), (xs.at[every, pl.ds(0, DC)], v.ac_send),
        (part.at[every, pl.ds(DC, DC)], v.rc_send), (part.at[pl.ds(1, last), pl.ds(0, 3)], v.rs_send),
        (v.from_z, v.rz_send), (v.from_pair, v.rp_send), (part.at[0, 0], v.rq_send),
    ):
        all_of(ref, sem).wait_send()
    for i in range(1, depth):

        @pl.when((i - 1 <= z) & (z < depth - 1))
        def _():
            upward(i, whole).wait_send()

        @pl.when((z + i <= depth) & (z > 0))
        def _():
            downward(i, whole).wait_send()


def layer(
    conv_input, gate_branch, conv_taps, narrow_maps, wide_maps, decay, decay_shift, mixer_out,
    stream, gain, routes, shares, expert_gate, expert_up, expert_down,
):
    count = lax.axis_size("sp")
    depth = count // 2
    rows, channels = conv_input.shape
    kept, width = stream.shape
    half = kept // 2
    pieces = 4
    bulk = kept * 3 // 4
    lines = -(-count // SUBLANES) * SUBLANES
    single, kind = (jnp.float32, jnp.bfloat16)
    dma = pltpu.SemaphoreType.DMA
    inputs = dict(
        conv=conv_input, gate=gate_branch, taps=conv_taps, narrow=narrow_maps, wide=wide_maps,
        decay=decay, shift=decay_shift, mixer=mixer_out, stream=stream, gain=gain, routes=routes,
        shares=shares, gate_w=expert_gate, up_w=expert_up, down_w=expert_down,
    )
    scratch = {
        name: pltpu.VMEM(one.shape[1:] if name.endswith("_w") else one.shape, one.dtype)
        for name, one in inputs.items()
    }
    flat = pltpu.VMEM((rows, channels), single)
    scratch.update(
        soft=pltpu.VMEM(decay.shape, single),
        gelu=flat,
        halo=pltpu.VMEM((2 * SUBLANES, channels), kind),
        factor=flat,
        state=flat,
        padded=pltpu.VMEM((rows + SUBLANES, channels), single),
        log_keep=flat,
        drive_keep=flat,
        ends=pltpu.VMEM((count, 2 * channels // LANES, LANES), single),
        weigh_out=pltpu.VMEM((count, lines, rows), single),
        weigh_in=pltpu.VMEM((count, lines, rows), single),
        weigh=pltpu.VMEM((rows, LANES), single),
        gated=pltpu.VMEM((rows, channels), kind),
        give=pltpu.VMEM((2, kept, width), kind),
        got=pltpu.VMEM((2, kept, width), kind),
        keep=pltpu.VMEM((2, kept, width), single),
        over=pltpu.VMEM((kept, width), kind),
        came=pltpu.VMEM((kept, width), kind),
        hidden=pltpu.VMEM((kept, width), kind),
        xs=pltpu.VMEM((depth, 2 * DC, kept, width), kind),
        act=pltpu.VMEM((DC * kept, expert_gate.shape[2]), kind),
        part=pltpu.VMEM((depth, 2 * DC, kept, width), kind),
        from_core=pltpu.VMEM((depth, DC, kept, width), kind),
        first=pltpu.VMEM((depth, 2, half, width), kind),
        rest=pltpu.VMEM((depth, 4, half, width), kind),
        from_z=pltpu.VMEM((2, kept, width), kind),
        from_pair=pltpu.VMEM((DC, bulk, width), kind),
        from_1=pltpu.VMEM((kept - bulk, width), kind),
        from_2=pltpu.VMEM((2, kept - bulk, width), kind),
        from_3=pltpu.VMEM((kept - bulk, width), kind),
        load_sem=dma((len(inputs),)),
        halo_send=dma,
        halo_recv=dma,
    )
    sent = ("weigh", "end", "pair", "cross", "ax", "ay", "af", "ac", "rc", "rs", "rz", "rp", "rq")
    scratch.update({name + "_send": dma for name in sent})
    landing = dict(
        weigh=(), end=(), pair=(), cross=(4,), ax=(depth, 2), ay=(depth, 2), af=(depth,),
        ac=(depth,), rc=(depth,), rs=(depth, 3), rz=(2,), rp=(), rq=(3,), az=(depth,), rt=(2, 3),
    )
    scratch.update({name + "_recv": dma(shape) if shape else dma for name, shape in landing.items()})
    scratch.update(up_send=dma((depth,)), dn_send=dma((depth,)))
    names = [name + "_hbm" for name in inputs] + ["out"] + list(scratch)
    return pl.pallas_call(
        functools.partial(layer_kernel, count, names),
        out_shape=pltpu.VMEM((kept, width), kind),
        in_specs=[pl.BlockSpec(memory_space=pl.ANY)] * len(inputs),
        out_specs=pl.BlockSpec(memory_space=pltpu.VMEM),
        scratch_shapes=list(scratch.values()),
        compiler_params=pltpu.CompilerParams(
            collective_id=1, has_side_effects=True, vmem_limit_bytes=60 * 1024 * 1024
        ),
    )(*inputs.values())


def shards(
    conv_input,
    gate_branch,
    conv_taps,
    narrow_maps,
    wide_maps,
    decay_param,
    decay_shift,
    mixer_out,
    stream,
    norm_gain,
    routes,
    route_weights,
    expert_gate,
    expert_up,
    expert_down,
):
    seq_rows, channels = conv_input.shape
    tap_count = conv_taps.shape[0]
    tp_count = lax.axis_size("tp")
    tok_local = seq_rows // tp_count
    top_count = routes.shape[1]
    expert_total = expert_gate.shape[0] * lax.axis_size("sp")
    capacity = max(2, 2 * tok_local * top_count // expert_total)
    whole_rows = capacity >= tok_local and expert_gate.shape[0] == 1
    if whole_rows and tp_count == 4 and lax.axis_size("sp") == 8:
        return layer(
            conv_input, gate_branch, conv_taps, narrow_maps, wide_maps, decay_param[None, :],
            decay_shift, mixer_out, stream, norm_gain[None, :], routes.T, route_weights.T,
            expert_gate, expert_up, expert_down,
        )
    own_index = lax.axis_index("tp")
    own_rows = lax.dynamic_slice_in_dim(routes, own_index * tok_local, tok_local, 0)
    own_weights = lax.dynamic_slice_in_dim(route_weights, own_index * tok_local, tok_local, 0)
    soft = jax.nn.softplus(-decay_param)[None, :]
    earlier = shifted(conv_input[seq_rows - tap_count + 1 :], "sp", 1)
    head = jnp.zeros((SUBLANES, channels), jnp.float32)
    head = head.at[SUBLANES - tap_count + 1 :].set(earlier.astype(jnp.float32))
    factors, local_state = mix_local(
        head, conv_input, conv_taps, narrow_maps, wide_maps, soft, decay_shift
    )
    ends = lax.all_gather(jnp.stack([factors[-1], local_state[-1]]), "sp")
    mine = lax.axis_index("sp")
    state = jnp.zeros((channels,), jnp.float32)
    for position in range(lax.axis_size("sp") - 1):
        longer = ends[position, 0] * state + ends[position, 1]
        state = jnp.where(position < mine, longer, state)
    carried = (None, state)
    recurrent = local_state + factors * carried[1]
    gated_rows = (recurrent * jax.nn.gelu(gate_branch.astype(jnp.float32))).astype(jnp.bfloat16)
    mixer_sum = lax.psum_scatter(
        jnp.dot(gated_rows, mixer_out, preferred_element_type=jnp.float32).astype(jnp.bfloat16),
        "tp",
        scatter_dimension=0,
        tiled=True,
    ).astype(jnp.float32)
    hidden_f = stream.astype(jnp.float32) + mixer_sum
    hidden = hidden_f.astype(jnp.bfloat16)
    hidden_f = hidden.astype(jnp.float32)
    normed = (
        hidden_f
        * lax.rsqrt(jnp.mean(hidden_f * hidden_f, axis=-1, keepdims=True) + NORM_EPSILON)
        * norm_gain
    ).astype(jnp.bfloat16)
    model_width = normed.shape[1]
    assignments = tok_local * top_count
    own_routes = own_rows.reshape(assignments)
    own_ranks = slot_ranks(own_routes[None, :], expert_total)[0]
    source = jnp.arange(assignments, dtype=jnp.int32) // top_count
    slot_source = (
        jnp.full((expert_total * capacity,), -1, jnp.int32)
        .at[own_routes * capacity + own_ranks]
        .set(source)
    )
    outgoing = take_rows(normed, slot_source).reshape(expert_total, 1, capacity, model_width)
    partial_value = expert_work(
        lax.all_gather(
            lax.all_to_all(outgoing, "sp", split_axis=0, concat_axis=0, tiled=True),
            "tp",
            axis=1,
            tiled=True,
        ),
        expert_gate,
        expert_up,
        expert_down,
    )
    summed = lax.psum_scatter(
        partial_value.astype(jnp.bfloat16), "tp", scatter_dimension=1, tiled=True
    )
    returned = lax.all_to_all(summed, "sp", split_axis=0, concat_axis=0, tiled=True)
    own_slots = own_routes * capacity + own_ranks
    picked = returned.reshape(expert_total * capacity, model_width)[own_slots]
    combined = jnp.sum(
        picked.reshape(tok_local, top_count, model_width).astype(jnp.float32)
        * own_weights[:, :, None],
        axis=1,
    )
    return (hidden_f + combined).astype(jnp.bfloat16)


def solution(mesh):
    placed = (
        P("sp", "tp"),
        P("sp", "tp"),
        P(None, "tp"),
        P(None, "tp", None, None),
        P(None, "tp", None, None),
        P("tp"),
        P("sp", "tp"),
        P("tp", None),
        P(("sp", "tp"), None),
        P(),
        P("sp", None),
        P("sp", None),
        P("sp", None, "tp"),
        P("sp", None, "tp"),
        P("sp", "tp", None),
    )
    return jax.shard_map(
        shards, mesh=mesh, in_specs=placed, out_specs=P(("sp", "tp"), None), check_vma=False
    )
```

```python
import functools
import types

import jax
import jax.numpy as jnp
from jax import lax
from jax.experimental import pallas as pl
from jax.experimental.pallas import tpu as pltpu
from jax.sharding import PartitionSpec as P

NORM_EPSILON = 1e-06
CLAMP_LIMIT = 7.0
GATE_SLOPE = 1.702
DECAY_SCALE = 8.0


def shifted(block, axis, distance):
    devices = range(lax.axis_size(axis))
    route = [(i - distance, i) for i in devices if i - distance in devices]
    return lax.ppermute(block, axis, route)


def clamp_units(gate_pre, up_pre):
    clamped = jnp.minimum(gate_pre, CLAMP_LIMIT)
    upper = jnp.clip(up_pre, -CLAMP_LIMIT, CLAMP_LIMIT)
    return (upper + 1.0) * clamped * jax.nn.sigmoid(GATE_SLOPE * clamped)


def slot_ranks(flat_routes, expert_total):
    onehot = (
        flat_routes[:, :, None] == jnp.arange(expert_total, dtype=jnp.int32)[None, None, :]
    ).astype(jnp.int32)
    return jnp.sum(jnp.cumsum(onehot, axis=1) * onehot, axis=2) - 1


def take_rows(source_rows, slot_source):
    filled = slot_source >= 0
    picked = source_rows[jnp.maximum(slot_source, 0)]
    return jnp.where(filled[:, None], picked, jnp.zeros_like(picked))


def expert_work(arrived, expert_gate, expert_up, expert_down):
    local_experts = expert_gate.shape[0]
    buffer_shape = arrived.shape
    grouped = arrived.reshape(
        buffer_shape[0] // local_experts,
        local_experts,
        buffer_shape[1] * buffer_shape[2],
        buffer_shape[3],
    )
    gate_pre = jnp.einsum(
        "sxcd,xdf->sxcf", grouped, expert_gate, preferred_element_type=jnp.float32
    )
    up_pre = jnp.einsum("sxcd,xdf->sxcf", grouped, expert_up, preferred_element_type=jnp.float32)
    activation = clamp_units(gate_pre, up_pre).astype(jnp.bfloat16)
    partial_value = jnp.einsum(
        "sxcf,xfd->sxcd", activation, expert_down, preferred_element_type=jnp.float32
    )
    return partial_value.reshape(buffer_shape)


LANES = 128
SUBLANES = 8
DX, DY, DC = 1, 2, 4
SERIES_LIMIT = 0.05
GELU_SCALE = 0.7978845608028654
GELU_CUBIC = 0.044715


def mix_kernel(
    head_ref, conv_ref, taps_ref, narrow_ref, wide_ref, soft_ref, shift_ref,
    factor_ref, state_ref, padded, log_keep, drive_keep,
):
    rows, channels = conv_ref.shape
    taps = taps_ref.shape[0]
    padded[0:SUBLANES, :] = head_ref[...]
    padded[SUBLANES:, :] = conv_ref[...].astype(jnp.float32)
    total = jnp.zeros((rows, channels), jnp.float32)
    for k in range(taps):
        total = total + padded[pl.ds(SUBLANES - taps + 1 + k, rows), :] * taps_ref[k : k + 1, :]
    convolved = total.astype(jnp.bfloat16)
    narrow_size, wide_size = narrow_ref.shape[2], wide_ref.shape[2]
    spans = []
    for j in range(wide_ref.shape[1]):
        base = j * (2 * narrow_size + wide_size)
        spans.append((base, narrow_size, narrow_ref, 2 * j))
        spans.append((base + narrow_size, narrow_size, narrow_ref, 2 * j + 1))
        spans.append((base + 2 * narrow_size, wide_size, wide_ref, j))
    for start, size, maps, head in spans:
        piece = convolved[:, start : start + size]
        decay_pre = jnp.dot(piece, maps[0, head], preferred_element_type=jnp.float32)
        input_pre = jnp.dot(piece, maps[1, head], preferred_element_type=jnp.float32)
        cols = slice(start, start + size)
        log_decay = (
            -DECAY_SCALE * jax.nn.sigmoid(decay_pre) * soft_ref[:, cols] + shift_ref[:, cols]
        )
        decay = jnp.exp(log_decay)
        y = 2.0 * log_decay
        series = -y * (1.0 + y * (0.5 + y * (1.0 / 6.0 + y * (1.0 / 24.0 + y * (1.0 / 120.0)))))
        lost = jnp.where(y > -SERIES_LIMIT, series, 1.0 - decay * decay)
        log_keep[:, cols] = decay
        drive_keep[:, cols] = (
            jnp.sqrt(lost) * jax.nn.sigmoid(input_pre) * piece.astype(jnp.float32)
        )
    row_id = lax.broadcasted_iota(jnp.int32, (SUBLANES, channels), 0)

    def tile(i, carry):
        product, state = carry
        at = pl.ds(pl.multiple_of(i * SUBLANES, SUBLANES), SUBLANES)
        a, b = log_keep[at, :], drive_keep[at, :]
        step = 1
        while step < SUBLANES:
            inside = row_id >= step
            a_before = jnp.where(inside, pltpu.roll(a, step, 0), 1.0)
            b_before = jnp.where(inside, pltpu.roll(b, step, 0), 0.0)
            b = a * b_before + b
            a = a * a_before
            step *= 2
        b = b + a * state
        a = a * product
        factor_ref[at, :] = a
        state_ref[at, :] = b
        last = slice(SUBLANES - 1, SUBLANES)
        return (a[last, :], b[last, :])

    lax.fori_loop(
        0,
        rows // SUBLANES,
        tile,
        (jnp.ones((1, channels), jnp.float32), jnp.zeros((1, channels), jnp.float32)),
    )


def mix_local(head, conv_input, conv_taps, narrow_maps, wide_maps, soft, decay_shift):
    shape = conv_input.shape
    flat = jax.ShapeDtypeStruct(shape, jnp.float32)
    return pl.pallas_call(
        mix_kernel,
        out_shape=(flat, flat),
        in_specs=[pl.BlockSpec(memory_space=pltpu.VMEM)] * 7,
        out_specs=(pl.BlockSpec(memory_space=pltpu.VMEM),) * 2,
        scratch_shapes=[
            pltpu.VMEM((shape[0] + SUBLANES, shape[1]), jnp.float32),
            pltpu.VMEM(shape, jnp.float32),
            pltpu.VMEM(shape, jnp.float32),
        ],
        compiler_params=pltpu.CompilerParams(vmem_limit_bytes=32 * 1024 * 1024),
    )(head, conv_input, conv_taps, narrow_maps, wide_maps, soft, decay_shift)


def turn(z, p, depth):
    return jnp.where(p == 0, 0, jnp.where(z % 2 == 1, p, depth - p))


def layer_kernel(count, names, *refs):
    v = types.SimpleNamespace(**dict(zip(names, refs)))
    rows, channels = v.conv.shape
    kept, width = v.stream.shape
    depth = count // 2
    half = kept // 2
    single, kind = (jnp.float32, jnp.bfloat16)
    sp, tp = (lax.axis_index("sp"), lax.axis_index("tp"))
    z, y = (sp // 2, sp % 2)
    x, c = (tp // 2, tp % 2)
    mesh_id = pl.DeviceIdType.MESH
    peer_c = {"sp": sp, "tp": x * 2 + 1 - c}
    peer_x = {"sp": sp, "tp": (1 - x) * 2 + c}
    peer_y = {"sp": z * 2 + 1 - y, "tp": tp}

    def plane(k):
        return {"sp": ((z + k) % depth) * 2 + y, "tp": tp}

    def later(k):
        return {"sp": (sp + k) % count, "tp": tp}

    def copy(src, dst, send, recv, peer):
        return pltpu.make_async_remote_copy(
            src_ref=src, dst_ref=dst, send_sem=send, recv_sem=recv,
            device_id=peer, device_id_type=mesh_id,
        )

    def all_of(ref, sem):
        return copy(ref, ref, sem, sem, peer_c)

    barrier = pltpu.get_barrier_semaphore()
    peers = [later(k) for k in range(count - 1, 0, -1)] + [peer_x, peer_c]
    for peer in peers:
        pl.semaphore_signal(barrier, inc=1, device_id=peer, device_id_type=mesh_id)
    load_names = (
        "conv", "taps", "narrow", "wide", "decay", "shift", "gate", "routes", "shares", "stream",
        "gain", "mixer", "gate_w", "up_w", "down_w",
    )
    loads = {}
    for n, name in enumerate(load_names):
        source = getattr(v, name + "_hbm")
        source = source.at[0] if name.endswith("_w") else source
        loads[name] = pltpu.make_async_copy(source, getattr(v, name), v.load_sem.at[n])
        loads[name].start()

    loads["conv"].wait()
    pl.semaphore_wait(barrier, len(peers))
    halo_rows = v.halo.shape[0]
    halo_copy = copy(
        v.conv.at[pl.ds(rows - halo_rows, halo_rows)], v.halo, v.halo_send, v.halo_recv, later(1)
    )
    halo_copy.start()

    loads["decay"].wait()
    t = jnp.exp(-v.decay[...])
    v.soft[...] = t * (1.0 - t * (0.5 - t * (1.0 / 3.0 - t * (0.25 - t * (0.2 - t * (1.0 / 6.0))))))
    for name in ("taps", "narrow", "wide", "shift"):
        loads[name].wait()
    taps = v.taps.shape[0]
    lead = 2 * SUBLANES
    v.padded[SUBLANES:, :] = v.conv[...].astype(single)
    row_id = lax.broadcasted_iota(jnp.int32, (SUBLANES, channels), 0)

    def drive(first, last):
        at = slice(first, last)
        total = jnp.zeros((last - first, channels), single)
        for k in range(taps):
            shift = SUBLANES - taps + 1 + k
            total = total + v.padded[first + shift : last + shift, :] * v.taps[k : k + 1, :]
        convolved = total.astype(kind)
        narrow_size, wide_size = (v.narrow.shape[2], v.wide.shape[2])
        spans = []
        for j in range(v.wide.shape[1]):
            base = j * (2 * narrow_size + wide_size)
            spans.append((base, narrow_size, v.narrow, 2 * j))
            spans.append((base + narrow_size, narrow_size, v.narrow, 2 * j + 1))
            spans.append((base + 2 * narrow_size, wide_size, v.wide, j))
        for start, size, maps, head in spans:
            cols = slice(start, start + size)
            piece = convolved[:, cols]
            decay_pre = jnp.dot(piece, maps[0, head], preferred_element_type=single)
            input_pre = jnp.dot(piece, maps[1, head], preferred_element_type=single)
            log_decay = (
                -DECAY_SCALE * jax.nn.sigmoid(decay_pre) * v.soft[:, cols] + v.shift[at, cols]
            )
            decay = jnp.exp(log_decay)
            y2 = 2.0 * log_decay
            series = -y2 * (
                1.0 + y2 * (0.5 + y2 * (1.0 / 6.0 + y2 * (1.0 / 24.0 + y2 * (1.0 / 120.0))))
            )
            lost = jnp.where(y2 > -SERIES_LIMIT, series, 1.0 - decay * decay)
            v.log_keep[at, cols] = decay
            v.drive_keep[at, cols] = (
                jnp.sqrt(lost) * jax.nn.sigmoid(input_pre) * piece.astype(single)
            )

    def tile(i, carried):
        product, state = carried
        at = pl.ds(pl.multiple_of(i * SUBLANES, SUBLANES), SUBLANES)
        a, b = (v.log_keep[at, :], v.drive_keep[at, :])
        hop = 1
        while hop < SUBLANES:
            inside = row_id >= hop
            a_before = jnp.where(inside, pltpu.roll(a, hop, 0), 1.0)
            b_before = jnp.where(inside, pltpu.roll(b, hop, 0), 0.0)
            b = a * b_before + b
            a = a * a_before
            hop *= 2
        b = b + a * state
        a = a * product
        v.factor[at, :] = a
        v.state[at, :] = b
        last = slice(SUBLANES - 1, SUBLANES)
        return (a[last, :], b[last, :])

    def scan(first, last):
        start = (jnp.ones((1, channels), single), jnp.zeros((1, channels), single))
        return lax.fori_loop(first // SUBLANES, last // SUBLANES, tile, start, unroll=2)

    drive(lead, rows)
    scan(lead, rows)
    halo_copy.wait()
    before = v.halo[...].astype(single)[halo_rows - SUBLANES :]
    v.padded[0:SUBLANES, :] = jnp.where(sp > 0, before, jnp.zeros_like(before))
    drive(0, lead)
    lead_factor, lead_state = scan(0, lead)
    rest_factor, rest_state = (v.factor[rows - 1 : rows, :], v.state[rows - 1 : rows, :])
    end_factor = rest_factor * lead_factor
    end_state = rest_state + rest_factor * lead_state
    groups = channels // LANES
    for n in range(groups):
        cols = slice(n * LANES, (n + 1) * LANES)
        v.ends[0, n : n + 1, :] = end_factor[:, cols]
        v.ends[0, groups + n : groups + n + 1, :] = end_state[:, cols]
    end_copies = [
        copy(v.ends.at[0], v.ends.at[k], v.end_send, v.end_recv, later(k))
        for k in range(count - 1, 0, -1)
    ]
    for one in end_copies:
        one.start()

    loads["routes"].wait()
    loads["shares"].wait()
    lines = v.weigh_out.shape[1]
    line = lax.broadcasted_iota(jnp.int32, (lines, rows), 0)
    for e in range(count):
        share = jnp.zeros((1, rows), single)
        for n in range(v.routes.shape[0]):
            share = share + jnp.where(
                v.routes[n : n + 1, :] == e, v.shares[n : n + 1, :], 0.0
            )
        v.weigh_out[e] = jnp.where(line == sp, share, 0.0)
    weigh_copies = [
        copy(
            v.weigh_out.at[(sp + k) % count], v.weigh_in.at[k], v.weigh_send, v.weigh_recv,
            later(k),
        )
        for k in range(1, count)
    ]
    for one in weigh_copies:
        one.start()

    loads["gate"].wait()
    g = v.gate[...].astype(single)
    v.gelu[...] = 0.5 * g * (1.0 + jnp.tanh(GELU_SCALE * (g + GELU_CUBIC * g * g * g)))
    for name in ("mixer", "stream", "gain"):
        loads[name].wait()

    others = pl.ds(1, count - 1)
    all_of(v.ends.at[others], v.end_recv).wait_recv()
    carry = jnp.zeros((groups, LANES), single)
    for k in range(count - 1, 0, -1):
        longer = v.ends[k, 0:groups, :] * carry + v.ends[k, groups : 2 * groups, :]
        carry = jnp.where(sp >= k, longer, carry)
    carry = jnp.concatenate([carry[n : n + 1, :] for n in range(groups)], axis=1)
    beyond_lead = lead_state + lead_factor * carry
    row = lax.broadcasted_iota(jnp.int32, (half, channels), 0)
    order = [(1 - x, 1 - c), (x, 1 - c), (1 - x, c), (x, c)]
    for h in range(2):
        for n, (chip, core) in enumerate(order):
            first = (chip * 2 + core) * kept + h * half
            at = pl.ds(pl.multiple_of(first, half), half)
            entering = jnp.where(row + first < lead, carry, beyond_lead)
            recurrent = v.state[at, :] + v.factor[at, :] * entering
            to = (4 * h + n) * half
            v.gated[to : to + half, :] = (recurrent * v.gelu[at, :]).astype(kind)

    pieces = 4
    piece = width // pieces

    def part_of(h):
        return pl.ds(h * half, half)

    def pair(h):
        return copy(
            v.give.at[:, part_of(h)], v.got.at[:, part_of(h)], v.pair_send, v.pair_recv.at[h],
            peer_c,
        )

    bands = v.cross_recv.shape[0]
    band = kept // bands

    def band_of(n):
        return pl.ds(n * band, band)

    def cross(n):
        return copy(
            v.over.at[band_of(n)], v.came.at[band_of(n)], v.cross_send, v.cross_recv.at[n], peer_x
        )

    def send_across(h):
        pair(h).wait_recv()
        for n in range(h * bands // 2, (h + 1) * bands // 2):
            at = slice(n * band, (n + 1) * band)
            v.over[at, :] = (v.keep[0, at, :] + v.got[0, at, :].astype(single)).astype(kind)
            cross(n).start()

    for h in range(2):
        at = slice(h * half, (h + 1) * half)
        for n in range(pieces):
            cols = slice(n * piece, (n + 1) * piece)
            value = jnp.dot(
                v.gated[4 * h * half : 4 * (h + 1) * half, :], v.mixer[:, cols],
                preferred_element_type=single,
            )
            v.give[:, at, cols] = value[: 2 * half].astype(kind).reshape(2, half, piece)
            v.keep[:, at, cols] = value[2 * half :].reshape(2, half, piece)
        pair(h).start()
        if h == 0:

            @pl.when(c == 0)
            def _():
                send_across(0)

    @pl.when(c == 1)
    def _():
        send_across(0)

    send_across(1)

    xs, part = (v.xs, v.part)

    def ax(k, h, at=None, sem=None):
        at = part_of(h) if at is None else at
        sem = v.ax_send if sem is None else sem
        return copy(xs.at[k, 0, at], xs.at[k, DX, at], sem, v.ax_recv.at[k, h], peer_x)

    def ay(k, h, at=None, sem=None):
        at = part_of(h) if at is None else at
        sem = v.ay_send if sem is None else sem
        return copy(xs.at[k, 0, at], xs.at[k, DY, at], sem, v.ay_recv.at[k, h], peer_y)

    def fy(k):
        return copy(
            xs.at[k, DX, part_of(0)], xs.at[k, DX + DY, part_of(0)], v.af_send,
            v.af_recv.at[k], peer_y,
        )

    def fx(k):
        return copy(
            xs.at[k, DY, part_of(1)], xs.at[k, DX + DY, part_of(1)], v.af_send,
            v.af_recv.at[k], peer_x,
        )

    def ac(k, s):
        return copy(
            xs.at[k, s], xs.at[k, DC + s], v.ac_send, v.ac_recv.at[k], peer_c
        )

    whole = pl.ds(0, kept)
    beside = z + 1 - 2 * (z % 2)
    pair_device = {"sp": beside * 2 + y, "tp": tp}
    pair_slot = 1 + (z % 2) * (depth - 2)

    def lift_x():
        return copy(
            xs.at[0, DX, part_of(0)], xs.at[pair_slot, DX, part_of(0)], v.ax_send,
            v.ax_recv.at[pair_slot, 0], pair_device,
        )

    def lift_y():
        return copy(
            xs.at[0, DY, part_of(1)], xs.at[pair_slot, DY, part_of(1)], v.ay_send,
            v.ay_recv.at[pair_slot, 1], pair_device,
        )

    def upward(i, at):
        return copy(
            xs.at[i - 1, 0, at], xs.at[i, 0, at], v.up_send.at[i], v.az_recv.at[i], plane(1)
        )

    def downward(i, at):
        return copy(
            xs.at[(depth - i + 1) % depth, 0, at], xs.at[depth - i, 0, at], v.dn_send.at[i],
            v.az_recv.at[depth - i], plane(depth - 1),
        )

    def landed(k):
        return all_of(xs.at[k, 0], v.az_recv.at[k])

    for n in range(bands):
        at = slice(n * band, (n + 1) * band)
        cross(n).wait_recv()
        total = v.keep[1, at, :] + v.got[1, at, :].astype(single) + v.came[at, :].astype(single)
        hidden = (v.stream[at, :].astype(single) + total).astype(kind)
        v.hidden[at, :] = hidden
        wide = hidden.astype(single)
        mean = jnp.mean(wide * wide, axis=-1, keepdims=True)
        normed = wide * lax.rsqrt(mean + NORM_EPSILON) * v.gain[...]
        xs[0, 0, at, :] = normed.astype(kind)
        ax(0, n * 2 // bands, band_of(n)).start()
        ay(0, n * 2 // bands, band_of(n)).start()

        @pl.when(z < depth - 1)
        def _():
            upward(1, band_of(n)).start()

        @pl.when(z > 0)
        def _():
            downward(1, band_of(n)).start()

    ac(0, 0).start()
    all_of(v.weigh_in.at[others], v.weigh_recv).wait_recv()
    table = v.weigh_out[sp]
    for k in range(1, count):
        table = table + v.weigh_in[k]
    filled = jnp.concatenate([table, jnp.zeros((LANES - lines, rows), single)], axis=0)
    v.weigh[...] = jnp.transpose(filled)
    for name in ("gate_w", "up_w", "down_w"):
        loads[name].wait()

    def rc(k, cols):
        at = pl.ds(cols.start, cols.stop - cols.start)
        return copy(
            part.at[k, pl.ds(DC, DC), :, at], v.from_core.at[k, :, :, at], v.rc_send,
            v.rc_recv.at[k], peer_c,
        )

    def rs(k, n):
        sems = (v.rs_send, v.rs_recv.at[k, min(n, 2)])
        if n == 0:
            return copy(part.at[k, DX + DY, part_of(0)], v.first.at[k, 0], *sems, peer_y)
        if n == 1:
            return copy(part.at[k, DX + DY, part_of(1)], v.first.at[k, 1], *sems, peer_x)
        if n == 2:
            return copy(part.at[k, DY, part_of(0)], v.rest.at[k, 0], *sems, peer_y)
        if n == 3:
            return copy(part.at[k, DX, part_of(1)], v.rest.at[k, 1], *sems, peer_x)
        if n == 4:
            return copy(part.at[k, DX, part_of(0)], v.rest.at[k, 2], *sems, peer_x)
        return copy(part.at[k, DY, part_of(1)], v.rest.at[k, 3], *sems, peer_y)

    last = depth - 1
    at_end = (z == 0) | (z == last)
    inward = jnp.where(z == 0, 1, last - 1)
    across = jnp.where(z == 1, last, 0)

    bulk = v.from_pair.shape[1]
    remnant = pl.ds(bulk, kept - bulk)
    over_y, over_x = (z * 2 + 1 - y, (1 - x) * 2 + c)
    peer_1 = {"sp": (1 - c) * sp + c * over_y, "tp": (1 - c) * over_x + c * tp}
    peer_2 = {"sp": (1 - c) * over_y + c * sp, "tp": (1 - c) * tp + c * over_x}

    def to_pair(k):
        return copy(
            part.at[k, pl.ds(0, DC), pl.ds(0, bulk)], v.from_pair, v.rp_send, v.rp_recv,
            pair_device,
        )

    def rq(k, n):
        if n == 0:
            there = part.at[k, DX + DY, remnant]
            return copy(there, v.from_1, v.rq_send, v.rq_recv.at[0], peer_1)
        if n == 1:
            there = part.at[k, DX + c, remnant]
            return copy(there, v.from_2.at[0], v.rq_send, v.rq_recv.at[1], peer_1)
        if n == 2:
            there = part.at[k, DY - c, remnant]
            return copy(there, v.from_2.at[1], v.rq_send, v.rq_recv.at[1], peer_2)
        return copy(part.at[k, 0, remnant], v.from_3, v.rq_send, v.rq_recv.at[2], pair_device)

    def remnant_next(k):
        rq(k, 0).wait_recv()
        now = part[k, DY - c, bulk:kept].astype(single) + v.from_1[...].astype(single)
        part[k, DY - c, bulk:kept] = now.astype(kind)
        rq(k, 2).start()

    def remnant_last(k):
        all_of(v.from_2, v.rq_recv.at[1]).wait_recv()
        now = part[k, 0, bulk:kept].astype(single) + v.from_2[0].astype(single)
        part[k, 0, bulk:kept] = (now + v.from_2[1].astype(single)).astype(kind)
        rq(k, 3).start()

    small = half // 2

    def slim(h, t):
        return pl.ds(h * half + t * small, small)

    def zr_near(k, h, t):
        to = jnp.where(at_end, inward, across)
        return copy(
            part.at[k, 0, slim(h, t)], v.from_z.at[0, slim(h, t)], v.rz_send, v.rz_recv.at[t],
            {"sp": to * 2 + y, "tp": tp},
        )

    def near_landed(t):
        all_of(v.from_z.at[0, pl.ds(0, half)], v.rz_recv.at[t]).wait_recv()

    def zr_far(k, h, t):
        return copy(
            part.at[k, 0, slim(h, t)], v.from_z.at[1, slim(h, t)], v.rz_send, v.rz_recv.at[2],
            {"sp": (last - z) * 2 + y, "tp": tp},
        )

    def rt(k, t, n):
        here = slim(0, t)
        sems = (v.rs_send, v.rt_recv.at[t, min(n, 2)])
        if n == 0:
            return copy(part.at[k, DX + DY, here], v.first.at[k, 0, here], *sems, peer_y)
        if n == 1:
            return copy(part.at[k, DX + DY, slim(1, t)], v.first.at[k, 1, here], *sems, peer_x)
        if n == 2:
            return copy(part.at[k, DY, here], v.rest.at[k, 0, here], *sems, peer_y)
        if n == 3:
            return copy(part.at[k, DX, slim(1, t)], v.rest.at[k, 1, here], *sems, peer_x)
        if n == 4:
            return copy(part.at[k, DX, here], v.rest.at[k, 2, here], *sems, peer_x)
        return copy(part.at[k, DY, slim(1, t)], v.rest.at[k, 3, here], *sems, peer_y)

    def slim_next(k, t):
        here = slice(t * small, (t + 1) * small)
        there = slice(half + t * small, half + (t + 1) * small)
        rt(k, t, 0).wait_recv()
        now = part[k, DX, here].astype(single) + v.first[k, 0, here].astype(single)
        part[k, DX, here] = now.astype(kind)
        rt(k, t, 4).start()
        rt(k, t, 1).wait_recv()
        now = part[k, DY, there].astype(single) + v.first[k, 1, here].astype(single)
        part[k, DY, there] = now.astype(kind)
        rt(k, t, 5).start()

    def slim_last(k, t):
        here = slice(t * small, (t + 1) * small)
        all_of(v.rest.at[k, pl.ds(0, 4), slim(0, t)], v.rt_recv.at[t, 2]).wait_recv()
        inner = (z > 0) & (z < last)

        @pl.when(inner)
        def _():
            near_landed(t)

        for h in range(2):
            rows_h = slice(h * half + t * small, h * half + (t + 1) * small)
            now = part[k, 0, rows_h].astype(single) + v.rest[k, h, here].astype(single)
            now = now + v.rest[k, h + 2, here].astype(single)
            part[k, 0, rows_h] = now.astype(kind)

            @pl.when(inner)
            def _():
                more = part[k, 0, rows_h].astype(single) + v.from_z[0, rows_h].astype(single)
                part[k, 0, rows_h] = more.astype(kind)

            zr_far(k, h, t).start()

    lane = lax.broadcasted_iota(jnp.int32, (kept, LANES), 1)

    def share_of(k, j):
        plane_from = (z + depth - k) % depth
        columns = []
        for s in range(DC):
            y_from = 1 - y if s & DY else y
            x_from = 1 - x if s & DX else x
            c_from = 1 - c if j else c
            at = pl.ds(pl.multiple_of((x_from * 2 + c_from) * kept, kept), kept)
            mine = lane == plane_from * 2 + y_from
            columns.append(
                jnp.sum(jnp.where(mine, v.weigh[at, :], 0.0), axis=1, keepdims=True)
            )
        return jnp.concatenate(columns, axis=0)

    def activated(k, j):
        rows_in = xs[k, j * DC : (j + 1) * DC].reshape(DC * kept, width)
        g = jnp.dot(rows_in, v.gate_w[...], preferred_element_type=single)
        u = jnp.dot(rows_in, v.up_w[...], preferred_element_type=single)
        return (clamp_units(g, u) * share_of(k, j)).astype(kind)

    def theirs_first(k):
        v.act[...] = activated(k, 1)

    def theirs_next(k):
        for n in range(pieces):
            cols = slice(n * piece, (n + 1) * piece)
            down = jnp.dot(v.act[...], v.down_w[:, cols], preferred_element_type=single)
            part[k, DC : 2 * DC, :, cols] = down.astype(kind).reshape(DC, kept, piece)
            rc(k, cols).start()

    def ours(k):
        act = activated(k, 0)
        all_of(v.from_core.at[k], v.rc_recv.at[k]).wait_recv()
        for n in range(pieces):
            cols = slice(n * piece, (n + 1) * piece)
            down = jnp.dot(act, v.down_w[:, cols], preferred_element_type=single)
            down = down.reshape(DC, kept, piece) + v.from_core[k, :, :, cols].astype(single)
            part[k, 0:DC, :, cols] = down.astype(kind)

    far_slot = 1 + (1 - z % 2) * (depth - 2)
    inner_device = {"sp": (depth - 1 - z) * 2 + y, "tp": tp}

    def haul_x(k, n):
        return copy(
            xs.at[k, DX, part_of(0)], xs.at[far_slot, DX, part_of(0)], v.haul_send.at[n],
            v.ax_recv.at[far_slot, 0], inner_device if n == 0 else pair_device,
        )

    def haul_y(k, n):
        return copy(
            xs.at[k, DY, part_of(1)], xs.at[far_slot, DY, part_of(1)], v.haul_send.at[n],
            v.ay_recv.at[far_slot, 1], inner_device if n == 0 else pair_device,
        )

    def haul(k, n):
        inner = (z > 0) & (z < depth - 1)

        @pl.when(inner & (c == 0))
        def _():
            haul_x(k, n).start()

        @pl.when(inner & (c == 1))
        def _():
            haul_y(k, n).start()

    def spread_first(k, q):
        ax(k, 0).wait_recv()
        fy(k).start()

        @pl.when((q == 0) & (c == 0))
        def _():
            lift_x().start()

        ay(k, 1).wait_recv()
        fx(k).start()

        @pl.when((q == 0) & (c == 1))
        def _():
            lift_y().start()

    def spread_second(k):
        ax(k, 0).wait_recv()
        fy(k).start()
        ay(k, 1).wait_recv()
        fx(k).start()

    def spread_rest(k):
        ax(k, 1).wait_recv()
        ac(k, DX).start()
        ay(k, 0).wait_recv()
        ac(k, DY).start()

    def spread_last(k):
        all_of(xs.at[k, DX + DY], v.af_recv.at[k]).wait_recv()
        ac(k, DX + DY).start()

    def relay(i):
        @pl.when(i <= z)
        def _():
            landed(i).wait_recv()

            @pl.when(z < depth - 1)
            def _():
                upward(i + 1, whole).start()

        @pl.when(z + i < depth)
        def _():
            landed(depth - i).wait_recv()

            @pl.when(z > 0)
            def _():
                downward(i + 1, whole).start()

    def enter(k, q):
        @pl.when((q == 1) | ((q == 0) & (c == 1)))
        def _():
            ax(k, 0).start()

        @pl.when((q == 1) | ((q == 0) & (c == 0)))
        def _():
            ay(k, 1).start()

        @pl.when((q == 2) & (c == 1))
        def _():
            ax(k, 0, sem=v.odd_send).start()

        @pl.when((q == 2) & (c == 0))
        def _():
            ay(k, 1, sem=v.odd_send).start()

        @pl.when(q < 2)
        def _():
            ax(k, 1).start()
            ay(k, 0).start()

        @pl.when(q == 2)
        def _():
            ax(k, 1, sem=v.odd_send).start()
            ay(k, 0, sem=v.odd_send).start()

        ac(k, 0).start()

    def reduce_first(k):
        for n in range(4):
            rs(k, n).start()

    def reduce_next(k):
        rs(k, 0).wait_recv()
        now = part[k, DX, 0:half].astype(single) + v.first[k, 0].astype(single)
        part[k, DX, 0:half] = now.astype(kind)
        rs(k, 4).start()
        rs(k, 1).wait_recv()
        now = part[k, DY, half:kept].astype(single) + v.first[k, 1].astype(single)
        part[k, DY, half:kept] = now.astype(kind)
        rs(k, 5).start()

    def reduced(k):
        all_of(v.rest.at[k], v.rs_recv.at[k, 2]).wait_recv()
        upper = part[k, 0, 0:half].astype(single) + v.rest[k, 0].astype(single)
        lower = part[k, 0, half:kept].astype(single) + v.rest[k, 1].astype(single)
        return (upper + v.rest[k, 2].astype(single), lower + v.rest[k, 3].astype(single))

    def reduce_last(k):
        upper, lower = reduced(k)
        part[k, 0, 0:half] = upper.astype(kind)
        part[k, 0, half:kept] = lower.astype(kind)
        for t in range(2):
            for h in range(2):
                zr_near(k, h, t).start()

    def step(q, none):
        k = turn(z, q % depth, depth)
        k_next = turn(z, (q + 1) % depth, depth)
        k_done = turn(z, (q + depth - 1) % depth, depth)
        k_older = turn(z, (q + depth - 2) % depth, depth)
        live, late = (q < depth, q > 0)

        @pl.when(q < last)
        def _():
            spread_first(k, q)

        @pl.when(q == 1)
        def _():
            haul(0, 0)

        @pl.when(q == 2)
        def _():
            haul(k, 1)

        @pl.when(late)
        def _():
            all_of(xs.at[k_done, pl.ds(DC, DC)], v.ac_recv.at[k_done]).wait_recv()
            theirs_first(k_done)

        @pl.when(q == last)
        def _():
            spread_second(k)
            rq(turn(z, 1, depth), 0).start()
            rq(turn(z, 1, depth), 1).start()

        @pl.when(late)
        def _():
            theirs_next(k_done)

        @pl.when(q + 1 < depth)
        def _():
            relay(q + 1)
            enter(k_next, q)
            spread_rest(k)

        @pl.when(q > 3)
        def _():
            reduce_next(k_older)

        @pl.when(late)
        def _():
            ours(k_done)

        @pl.when(q == 2)
        def _():
            to_pair(k_done).start()

        @pl.when(q == last)
        def _():
            reduce_first(k_done)

        @pl.when(q > last)
        def _():
            for n in range(4):
                rt(k_done, 0, n).start()
            rt(k_done, 1, 0).start()
            rt(k_done, 1, 1).start()

        @pl.when(q == last)
        def _():
            spread_rest(k)

        @pl.when(live)
        def _():
            spread_last(k)

        return none

    lax.fori_loop(0, depth + 1, step, 0)
    k_pair, k_near, k_far = [turn(z, p, depth) for p in (1, 2, 3)]
    reduce_last(k_near)
    slim_next(k_far, 0)
    rt(k_far, 1, 2).start()
    rt(k_far, 1, 3).start()
    all_of(v.from_pair, v.rp_recv).wait_recv()
    for n in range(DC):
        now = part[0, n, 0:bulk].astype(single) + v.from_pair[n].astype(single)
        part[0, n, 0:bulk] = now.astype(kind)
    slim_next(k_far, 1)
    remnant_next(k_pair)
    reduce_first(0)
    slim_last(k_far, 0)
    slim_last(k_far, 1)
    remnant_last(k_pair)
    reduce_next(0)
    upper, lower = reduced(0)
    upper = upper + v.hidden[0:half, :].astype(single)
    lower = lower + v.hidden[half:kept, :].astype(single)

    @pl.when(at_end)
    def _():
        for t in range(2):
            near_landed(t)

    all_of(v.from_z.at[1], v.rz_recv.at[2]).wait_recv()
    direct = jnp.where(at_end, 1.0, 0.0)
    upper = upper + direct * v.from_z[0, 0:half].astype(single)
    lower = lower + direct * v.from_z[0, half:kept].astype(single)
    upper = upper + v.from_z[1, 0:half].astype(single)
    lower = lower + v.from_z[1, half:kept].astype(single)
    rq(k_pair, 3).wait_recv()
    rest = jnp.concatenate(
        [jnp.zeros((bulk - half, width), single), v.from_3[...].astype(single)], axis=0
    )
    lower = lower + rest
    for h, value in enumerate((upper, lower)):
        v.out[h * half : (h + 1) * half, :] = value.astype(v.out.dtype)
    every = pl.ds(0, depth)
    quarter, six = (xs.at[every, pl.ds(0, 1)], v.first.at[pl.ds(0, 3)])
    for ref, sem in (
        (v.weigh_in.at[others], v.weigh_send), (v.ends.at[others], v.end_send),
        (v.give, v.pair_send), (v.over, v.cross_send), (six, v.ax_send),
        (six, v.ay_send), (v.rest.at[0, pl.ds(0, 3)], v.odd_send), (quarter, v.af_send), (xs.at[every, pl.ds(0, DC)], v.ac_send),
        (part.at[every, pl.ds(DC, DC)], v.rc_send), (part.at[pl.ds(1, last), pl.ds(0, 3)], v.rs_send),
        (v.from_z, v.rz_send), (v.from_pair, v.rp_send), (part.at[0, 0], v.rq_send),
    ):
        all_of(ref, sem).wait_send()

    @pl.when((z > 0) & (z < last))
    def _():
        for n in range(2):
            haul_x(0, n).wait_send()

    for i in range(1, depth):

        @pl.when((i - 1 <= z) & (z < depth - 1))
        def _():
            upward(i, whole).wait_send()

        @pl.when((z + i <= depth) & (z > 0))
        def _():
            downward(i, whole).wait_send()


def layer(
    conv_input, gate_branch, conv_taps, narrow_maps, wide_maps, decay, decay_shift, mixer_out,
    stream, gain, routes, shares, expert_gate, expert_up, expert_down,
):
    count = lax.axis_size("sp")
    depth = count // 2
    rows, channels = conv_input.shape
    kept, width = stream.shape
    half = kept // 2
    pieces = 4
    bulk = kept * 3 // 4
    lines = -(-count // SUBLANES) * SUBLANES
    single, kind = (jnp.float32, jnp.bfloat16)
    dma = pltpu.SemaphoreType.DMA
    inputs = dict(
        conv=conv_input, gate=gate_branch, taps=conv_taps, narrow=narrow_maps, wide=wide_maps,
        decay=decay, shift=decay_shift, mixer=mixer_out, stream=stream, gain=gain, routes=routes,
        shares=shares, gate_w=expert_gate, up_w=expert_up, down_w=expert_down,
    )
    scratch = {
        name: pltpu.VMEM(one.shape[1:] if name.endswith("_w") else one.shape, one.dtype)
        for name, one in inputs.items()
    }
    flat = pltpu.VMEM((rows, channels), single)
    scratch.update(
        soft=pltpu.VMEM(decay.shape, single),
        gelu=flat,
        halo=pltpu.VMEM((2 * SUBLANES, channels), kind),
        factor=flat,
        state=flat,
        padded=pltpu.VMEM((rows + SUBLANES, channels), single),
        log_keep=flat,
        drive_keep=flat,
        ends=pltpu.VMEM((count, 2 * channels // LANES, LANES), single),
        weigh_out=pltpu.VMEM((count, lines, rows), single),
        weigh_in=pltpu.VMEM((count, lines, rows), single),
        weigh=pltpu.VMEM((rows, LANES), single),
        gated=pltpu.VMEM((rows, channels), kind),
        give=pltpu.VMEM((2, kept, width), kind),
        got=pltpu.VMEM((2, kept, width), kind),
        keep=pltpu.VMEM((2, kept, width), single),
        over=pltpu.VMEM((kept, width), kind),
        came=pltpu.VMEM((kept, width), kind),
        hidden=pltpu.VMEM((kept, width), kind),
        xs=pltpu.VMEM((depth, 2 * DC, kept, width), kind),
        act=pltpu.VMEM((DC * kept, expert_gate.shape[2]), kind),
        part=pltpu.VMEM((depth, 2 * DC, kept, width), kind),
        from_core=pltpu.VMEM((depth, DC, kept, width), kind),
        first=pltpu.VMEM((depth, 2, half, width), kind),
        rest=pltpu.VMEM((depth, 4, half, width), kind),
        from_z=pltpu.VMEM((2, kept, width), kind),
        from_pair=pltpu.VMEM((DC, bulk, width), kind),
        from_1=pltpu.VMEM((kept - bulk, width), kind),
        from_2=pltpu.VMEM((2, kept - bulk, width), kind),
        from_3=pltpu.VMEM((kept - bulk, width), kind),
        load_sem=dma((len(inputs),)),
        halo_send=dma,
        halo_recv=dma,
    )
    sent = ("weigh", "end", "pair", "cross", "ax", "ay", "af", "ac", "rc", "rs", "rz", "rp", "rq")
    scratch.update({name + "_send": dma for name in sent})
    landing = dict(
        weigh=(), end=(), pair=(2,), cross=(4,), ax=(depth, 2), ay=(depth, 2), af=(depth,),
        ac=(depth,), rc=(depth,), rs=(depth, 3), rz=(3,), rp=(), rq=(3,), az=(depth,), rt=(2, 3),
    )
    scratch.update({name + "_recv": dma(shape) if shape else dma for name, shape in landing.items()})
    scratch.update(
        up_send=dma((depth,)), dn_send=dma((depth,)), haul_send=dma((2,)), odd_send=dma
    )
    names = [name + "_hbm" for name in inputs] + ["out"] + list(scratch)
    return pl.pallas_call(
        functools.partial(layer_kernel, count, names),
        out_shape=pltpu.VMEM((kept, width), kind),
        in_specs=[pl.BlockSpec(memory_space=pl.ANY)] * len(inputs),
        out_specs=pl.BlockSpec(memory_space=pltpu.VMEM),
        scratch_shapes=list(scratch.values()),
        compiler_params=pltpu.CompilerParams(
            collective_id=1, has_side_effects=True, vmem_limit_bytes=60 * 1024 * 1024
        ),
    )(*inputs.values())


def shards(
    conv_input,
    gate_branch,
    conv_taps,
    narrow_maps,
    wide_maps,
    decay_param,
    decay_shift,
    mixer_out,
    stream,
    norm_gain,
    routes,
    route_weights,
    expert_gate,
    expert_up,
    expert_down,
):
    seq_rows, channels = conv_input.shape
    tap_count = conv_taps.shape[0]
    tp_count = lax.axis_size("tp")
    tok_local = seq_rows // tp_count
    top_count = routes.shape[1]
    expert_total = expert_gate.shape[0] * lax.axis_size("sp")
    capacity = max(2, 2 * tok_local * top_count // expert_total)
    whole_rows = capacity >= tok_local and expert_gate.shape[0] == 1
    if whole_rows and tp_count == 4 and lax.axis_size("sp") == 8:
        return layer(
            conv_input, gate_branch, conv_taps, narrow_maps, wide_maps, decay_param[None, :],
            decay_shift, mixer_out, stream, norm_gain[None, :], routes.T, route_weights.T,
            expert_gate, expert_up, expert_down,
        )
    own_index = lax.axis_index("tp")
    own_rows = lax.dynamic_slice_in_dim(routes, own_index * tok_local, tok_local, 0)
    own_weights = lax.dynamic_slice_in_dim(route_weights, own_index * tok_local, tok_local, 0)
    soft = jax.nn.softplus(-decay_param)[None, :]
    earlier = shifted(conv_input[seq_rows - tap_count + 1 :], "sp", 1)
    head = jnp.zeros((SUBLANES, channels), jnp.float32)
    head = head.at[SUBLANES - tap_count + 1 :].set(earlier.astype(jnp.float32))
    factors, local_state = mix_local(
        head, conv_input, conv_taps, narrow_maps, wide_maps, soft, decay_shift
    )
    ends = lax.all_gather(jnp.stack([factors[-1], local_state[-1]]), "sp")
    mine = lax.axis_index("sp")
    state = jnp.zeros((channels,), jnp.float32)
    for position in range(lax.axis_size("sp") - 1):
        longer = ends[position, 0] * state + ends[position, 1]
        state = jnp.where(position < mine, longer, state)
    carried = (None, state)
    recurrent = local_state + factors * carried[1]
    gated_rows = (recurrent * jax.nn.gelu(gate_branch.astype(jnp.float32))).astype(jnp.bfloat16)
    mixer_sum = lax.psum_scatter(
        jnp.dot(gated_rows, mixer_out, preferred_element_type=jnp.float32).astype(jnp.bfloat16),
        "tp",
        scatter_dimension=0,
        tiled=True,
    ).astype(jnp.float32)
    hidden_f = stream.astype(jnp.float32) + mixer_sum
    hidden = hidden_f.astype(jnp.bfloat16)
    hidden_f = hidden.astype(jnp.float32)
    normed = (
        hidden_f
        * lax.rsqrt(jnp.mean(hidden_f * hidden_f, axis=-1, keepdims=True) + NORM_EPSILON)
        * norm_gain
    ).astype(jnp.bfloat16)
    model_width = normed.shape[1]
    assignments = tok_local * top_count
    own_routes = own_rows.reshape(assignments)
    own_ranks = slot_ranks(own_routes[None, :], expert_total)[0]
    source = jnp.arange(assignments, dtype=jnp.int32) // top_count
    slot_source = (
        jnp.full((expert_total * capacity,), -1, jnp.int32)
        .at[own_routes * capacity + own_ranks]
        .set(source)
    )
    outgoing = take_rows(normed, slot_source).reshape(expert_total, 1, capacity, model_width)
    partial_value = expert_work(
        lax.all_gather(
            lax.all_to_all(outgoing, "sp", split_axis=0, concat_axis=0, tiled=True),
            "tp",
            axis=1,
            tiled=True,
        ),
        expert_gate,
        expert_up,
        expert_down,
    )
    summed = lax.psum_scatter(
        partial_value.astype(jnp.bfloat16), "tp", scatter_dimension=1, tiled=True
    )
    returned = lax.all_to_all(summed, "sp", split_axis=0, concat_axis=0, tiled=True)
    own_slots = own_routes * capacity + own_ranks
    picked = returned.reshape(expert_total * capacity, model_width)[own_slots]
    combined = jnp.sum(
        picked.reshape(tok_local, top_count, model_width).astype(jnp.float32)
        * own_weights[:, :, None],
        axis=1,
    )
    return (hidden_f + combined).astype(jnp.bfloat16)


def solution(mesh):
    placed = (
        P("sp", "tp"),
        P("sp", "tp"),
        P(None, "tp"),
        P(None, "tp", None, None),
        P(None, "tp", None, None),
        P("tp"),
        P("sp", "tp"),
        P("tp", None),
        P(("sp", "tp"), None),
        P(),
        P("sp", None),
        P("sp", None),
        P("sp", None, "tp"),
        P("sp", None, "tp"),
        P("sp", "tp", None),
    )
    return jax.shard_map(
        shards, mesh=mesh, in_specs=placed, out_specs=P(("sp", "tp"), None), check_vma=False
    )
```

```python
import functools
import types

import jax
import jax.numpy as jnp
from jax import lax
from jax.experimental import pallas as pl
from jax.experimental.pallas import tpu as pltpu
from jax.sharding import PartitionSpec as P

NORM_EPSILON = 1e-06
CLAMP_LIMIT = 7.0
GATE_SLOPE = 1.702
DECAY_SCALE = 8.0


def shifted(block, axis, distance):
    devices = range(lax.axis_size(axis))
    route = [(i - distance, i) for i in devices if i - distance in devices]
    return lax.ppermute(block, axis, route)


def clamp_units(gate_pre, up_pre):
    clamped = jnp.minimum(gate_pre, CLAMP_LIMIT)
    upper = jnp.clip(up_pre, -CLAMP_LIMIT, CLAMP_LIMIT)
    return (upper + 1.0) * clamped * jax.nn.sigmoid(GATE_SLOPE * clamped)


def slot_ranks(flat_routes, expert_total):
    onehot = (
        flat_routes[:, :, None] == jnp.arange(expert_total, dtype=jnp.int32)[None, None, :]
    ).astype(jnp.int32)
    return jnp.sum(jnp.cumsum(onehot, axis=1) * onehot, axis=2) - 1


def take_rows(source_rows, slot_source):
    filled = slot_source >= 0
    picked = source_rows[jnp.maximum(slot_source, 0)]
    return jnp.where(filled[:, None], picked, jnp.zeros_like(picked))


def expert_work(arrived, expert_gate, expert_up, expert_down):
    local_experts = expert_gate.shape[0]
    buffer_shape = arrived.shape
    grouped = arrived.reshape(
        buffer_shape[0] // local_experts,
        local_experts,
        buffer_shape[1] * buffer_shape[2],
        buffer_shape[3],
    )
    gate_pre = jnp.einsum(
        "sxcd,xdf->sxcf", grouped, expert_gate, preferred_element_type=jnp.float32
    )
    up_pre = jnp.einsum("sxcd,xdf->sxcf", grouped, expert_up, preferred_element_type=jnp.float32)
    activation = clamp_units(gate_pre, up_pre).astype(jnp.bfloat16)
    partial_value = jnp.einsum(
        "sxcf,xfd->sxcd", activation, expert_down, preferred_element_type=jnp.float32
    )
    return partial_value.reshape(buffer_shape)


LANES = 128
SUBLANES = 8
DX, DY, DC = 1, 2, 4
SERIES_LIMIT = 0.05
GELU_SCALE = 0.7978845608028654
GELU_CUBIC = 0.044715


def mix_kernel(
    head_ref, conv_ref, taps_ref, narrow_ref, wide_ref, soft_ref, shift_ref,
    factor_ref, state_ref, padded, log_keep, drive_keep,
):
    rows, channels = conv_ref.shape
    taps = taps_ref.shape[0]
    padded[0:SUBLANES, :] = head_ref[...]
    padded[SUBLANES:, :] = conv_ref[...].astype(jnp.float32)
    total = jnp.zeros((rows, channels), jnp.float32)
    for k in range(taps):
        total = total + padded[pl.ds(SUBLANES - taps + 1 + k, rows), :] * taps_ref[k : k + 1, :]
    convolved = total.astype(jnp.bfloat16)
    narrow_size, wide_size = narrow_ref.shape[2], wide_ref.shape[2]
    spans = []
    for j in range(wide_ref.shape[1]):
        base = j * (2 * narrow_size + wide_size)
        spans.append((base, narrow_size, narrow_ref, 2 * j))
        spans.append((base + narrow_size, narrow_size, narrow_ref, 2 * j + 1))
        spans.append((base + 2 * narrow_size, wide_size, wide_ref, j))
    for start, size, maps, head in spans:
        piece = convolved[:, start : start + size]
        decay_pre = jnp.dot(piece, maps[0, head], preferred_element_type=jnp.float32)
        input_pre = jnp.dot(piece, maps[1, head], preferred_element_type=jnp.float32)
        cols = slice(start, start + size)
        log_decay = (
            -DECAY_SCALE * jax.nn.sigmoid(decay_pre) * soft_ref[:, cols] + shift_ref[:, cols]
        )
        decay = jnp.exp(log_decay)
        y = 2.0 * log_decay
        series = -y * (1.0 + y * (0.5 + y * (1.0 / 6.0 + y * (1.0 / 24.0 + y * (1.0 / 120.0)))))
        lost = jnp.where(y > -SERIES_LIMIT, series, 1.0 - decay * decay)
        log_keep[:, cols] = decay
        drive_keep[:, cols] = (
            jnp.sqrt(lost) * jax.nn.sigmoid(input_pre) * piece.astype(jnp.float32)
        )
    row_id = lax.broadcasted_iota(jnp.int32, (SUBLANES, channels), 0)

    def tile(i, carry):
        product, state = carry
        at = pl.ds(pl.multiple_of(i * SUBLANES, SUBLANES), SUBLANES)
        a, b = log_keep[at, :], drive_keep[at, :]
        step = 1
        while step < SUBLANES:
            inside = row_id >= step
            a_before = jnp.where(inside, pltpu.roll(a, step, 0), 1.0)
            b_before = jnp.where(inside, pltpu.roll(b, step, 0), 0.0)
            b = a * b_before + b
            a = a * a_before
            step *= 2
        b = b + a * state
        a = a * product
        factor_ref[at, :] = a
        state_ref[at, :] = b
        last = slice(SUBLANES - 1, SUBLANES)
        return (a[last, :], b[last, :])

    lax.fori_loop(
        0,
        rows // SUBLANES,
        tile,
        (jnp.ones((1, channels), jnp.float32), jnp.zeros((1, channels), jnp.float32)),
    )


def mix_local(head, conv_input, conv_taps, narrow_maps, wide_maps, soft, decay_shift):
    shape = conv_input.shape
    flat = jax.ShapeDtypeStruct(shape, jnp.float32)
    return pl.pallas_call(
        mix_kernel,
        out_shape=(flat, flat),
        in_specs=[pl.BlockSpec(memory_space=pltpu.VMEM)] * 7,
        out_specs=(pl.BlockSpec(memory_space=pltpu.VMEM),) * 2,
        scratch_shapes=[
            pltpu.VMEM((shape[0] + SUBLANES, shape[1]), jnp.float32),
            pltpu.VMEM(shape, jnp.float32),
            pltpu.VMEM(shape, jnp.float32),
        ],
        compiler_params=pltpu.CompilerParams(vmem_limit_bytes=32 * 1024 * 1024),
    )(head, conv_input, conv_taps, narrow_maps, wide_maps, soft, decay_shift)


def turn(z, p, depth):
    return jnp.where(p == 0, 0, jnp.where(z % 2 == 1, p, depth - p))


def layer_kernel(count, names, *refs):
    v = types.SimpleNamespace(**dict(zip(names, refs)))
    rows, channels = v.conv.shape
    kept, width = v.stream.shape
    depth = count // 2
    half = kept // 2
    single, kind = (jnp.float32, jnp.bfloat16)
    sp, tp = (lax.axis_index("sp"), lax.axis_index("tp"))
    z, y = (sp // 2, sp % 2)
    x, c = (tp // 2, tp % 2)
    mesh_id = pl.DeviceIdType.MESH
    peer_c = {"sp": sp, "tp": x * 2 + 1 - c}
    peer_x = {"sp": sp, "tp": (1 - x) * 2 + c}
    peer_y = {"sp": z * 2 + 1 - y, "tp": tp}

    def plane(k):
        return {"sp": ((z + k) % depth) * 2 + y, "tp": tp}

    def later(k):
        return {"sp": (sp + k) % count, "tp": tp}

    def copy(src, dst, send, recv, peer):
        return pltpu.make_async_remote_copy(
            src_ref=src, dst_ref=dst, send_sem=send, recv_sem=recv,
            device_id=peer, device_id_type=mesh_id,
        )

    def all_of(ref, sem):
        return copy(ref, ref, sem, sem, peer_c)

    barrier = pltpu.get_barrier_semaphore()
    peers = [later(k) for k in range(count - 1, 0, -1)] + [peer_x, peer_c]
    for peer in peers:
        pl.semaphore_signal(barrier, inc=1, device_id=peer, device_id_type=mesh_id)
    load_names = (
        "conv", "taps", "narrow", "wide", "decay", "shift", "gate", "routes", "shares", "stream",
        "gain", "mixer", "gate_w", "up_w", "down_w",
    )
    loads = {}
    for n, name in enumerate(load_names):
        source = getattr(v, name + "_hbm")
        source = source.at[0] if name.endswith("_w") else source
        loads[name] = pltpu.make_async_copy(source, getattr(v, name), v.load_sem.at[n])
        loads[name].start()

    loads["conv"].wait()
    pl.semaphore_wait(barrier, len(peers))
    halo_rows = v.halo.shape[0]
    halo_copy = copy(
        v.conv.at[pl.ds(rows - halo_rows, halo_rows)], v.halo, v.halo_send, v.halo_recv, later(1)
    )
    halo_copy.start()

    loads["decay"].wait()
    t = jnp.exp(-v.decay[...])
    v.soft[...] = t * (1.0 - t * (0.5 - t * (1.0 / 3.0 - t * (0.25 - t * (0.2 - t * (1.0 / 6.0))))))
    for name in ("taps", "narrow", "wide", "shift"):
        loads[name].wait()
    taps = v.taps.shape[0]
    lead = 2 * SUBLANES
    v.padded[SUBLANES:, :] = v.conv[...].astype(single)
    row_id = lax.broadcasted_iota(jnp.int32, (SUBLANES, channels), 0)

    def drive(first, last):
        at = slice(first, last)
        total = jnp.zeros((last - first, channels), single)
        for k in range(taps):
            shift = SUBLANES - taps + 1 + k
            total = total + v.padded[first + shift : last + shift, :] * v.taps[k : k + 1, :]
        convolved = total.astype(kind)
        narrow_size, wide_size = (v.narrow.shape[2], v.wide.shape[2])
        spans = []
        for j in range(v.wide.shape[1]):
            base = j * (2 * narrow_size + wide_size)
            spans.append((base, narrow_size, v.narrow, 2 * j))
            spans.append((base + narrow_size, narrow_size, v.narrow, 2 * j + 1))
            spans.append((base + 2 * narrow_size, wide_size, v.wide, j))
        for start, size, maps, head in spans:
            cols = slice(start, start + size)
            piece = convolved[:, cols]
            decay_pre = jnp.dot(piece, maps[0, head], preferred_element_type=single)
            input_pre = jnp.dot(piece, maps[1, head], preferred_element_type=single)
            log_decay = (
                -DECAY_SCALE * jax.nn.sigmoid(decay_pre) * v.soft[:, cols] + v.shift[at, cols]
            )
            decay = jnp.exp(log_decay)
            y2 = 2.0 * log_decay
            series = -y2 * (
                1.0 + y2 * (0.5 + y2 * (1.0 / 6.0 + y2 * (1.0 / 24.0 + y2 * (1.0 / 120.0))))
            )
            lost = jnp.where(y2 > -SERIES_LIMIT, series, 1.0 - decay * decay)
            v.log_keep[at, cols] = decay
            v.drive_keep[at, cols] = (
                jnp.sqrt(lost) * jax.nn.sigmoid(input_pre) * piece.astype(single)
            )

    def tile(i, carried):
        product, state = carried
        at = pl.ds(pl.multiple_of(i * SUBLANES, SUBLANES), SUBLANES)
        a, b = (v.log_keep[at, :], v.drive_keep[at, :])
        hop = 1
        while hop < SUBLANES:
            inside = row_id >= hop
            a_before = jnp.where(inside, pltpu.roll(a, hop, 0), 1.0)
            b_before = jnp.where(inside, pltpu.roll(b, hop, 0), 0.0)
            b = a * b_before + b
            a = a * a_before
            hop *= 2
        b = b + a * state
        a = a * product
        v.factor[at, :] = a
        v.state[at, :] = b
        last = slice(SUBLANES - 1, SUBLANES)
        return (a[last, :], b[last, :])

    def scan(first, last):
        start = (jnp.ones((1, channels), single), jnp.zeros((1, channels), single))
        return lax.fori_loop(first // SUBLANES, last // SUBLANES, tile, start, unroll=2)

    drive(lead, rows)
    scan(lead, rows)
    halo_copy.wait()
    before = v.halo[...].astype(single)[halo_rows - SUBLANES :]
    v.padded[0:SUBLANES, :] = jnp.where(sp > 0, before, jnp.zeros_like(before))
    drive(0, lead)
    lead_factor, lead_state = scan(0, lead)
    rest_factor, rest_state = (v.factor[rows - 1 : rows, :], v.state[rows - 1 : rows, :])
    end_factor = rest_factor * lead_factor
    end_state = rest_state + rest_factor * lead_state
    groups = channels // LANES
    for n in range(groups):
        cols = slice(n * LANES, (n + 1) * LANES)
        v.ends[0, n : n + 1, :] = end_factor[:, cols]
        v.ends[0, groups + n : groups + n + 1, :] = end_state[:, cols]
    end_copies = [
        copy(v.ends.at[0], v.ends.at[k], v.end_send, v.end_recv, later(k))
        for k in range(count - 1, 0, -1)
    ]
    for one in end_copies:
        one.start()

    loads["routes"].wait()
    loads["shares"].wait()
    lines = v.weigh_out.shape[1]
    line = lax.broadcasted_iota(jnp.int32, (lines, rows), 0)
    for e in range(count):
        share = jnp.zeros((1, rows), single)
        for n in range(v.routes.shape[0]):
            share = share + jnp.where(
                v.routes[n : n + 1, :] == e, v.shares[n : n + 1, :], 0.0
            )
        v.weigh_out[e] = jnp.where(line == sp, share, 0.0)
    weigh_copies = [
        copy(
            v.weigh_out.at[(sp + k) % count], v.weigh_in.at[k], v.weigh_send, v.weigh_recv,
            later(k),
        )
        for k in range(1, count)
    ]
    for one in weigh_copies:
        one.start()

    loads["gate"].wait()
    g = v.gate[...].astype(single)
    v.gelu[...] = 0.5 * g * (1.0 + jnp.tanh(GELU_SCALE * (g + GELU_CUBIC * g * g * g)))
    for name in ("mixer", "stream", "gain"):
        loads[name].wait()

    others = pl.ds(1, count - 1)
    all_of(v.ends.at[others], v.end_recv).wait_recv()
    carry = jnp.zeros((groups, LANES), single)
    for k in range(count - 1, 0, -1):
        longer = v.ends[k, 0:groups, :] * carry + v.ends[k, groups : 2 * groups, :]
        carry = jnp.where(sp >= k, longer, carry)
    carry = jnp.concatenate([carry[n : n + 1, :] for n in range(groups)], axis=1)
    beyond_lead = lead_state + lead_factor * carry
    row = lax.broadcasted_iota(jnp.int32, (half, channels), 0)
    order = [(1 - x, 1 - c), (x, 1 - c), (1 - x, c), (x, c)]
    for h in range(2):
        for n, (chip, core) in enumerate(order):
            first = (chip * 2 + core) * kept + h * half
            at = pl.ds(pl.multiple_of(first, half), half)
            entering = jnp.where(row + first < lead, carry, beyond_lead)
            recurrent = v.state[at, :] + v.factor[at, :] * entering
            to = (4 * h + n) * half
            v.gated[to : to + half, :] = (recurrent * v.gelu[at, :]).astype(kind)

    pieces = 4
    piece = width // pieces

    def part_of(h):
        return pl.ds(h * half, half)

    def pair(h):
        return copy(
            v.give.at[:, part_of(h)], v.got.at[:, part_of(h)], v.pair_send, v.pair_recv.at[h],
            peer_c,
        )

    bands = v.cross_recv.shape[0]
    band = kept // bands

    def band_of(n):
        return pl.ds(n * band, band)

    def cross(n):
        return copy(
            v.over.at[band_of(n)], v.came.at[band_of(n)], v.cross_send, v.cross_recv.at[n], peer_x
        )

    def send_across(h):
        pair(h).wait_recv()
        for n in range(h * bands // 2, (h + 1) * bands // 2):
            at = slice(n * band, (n + 1) * band)
            v.over[at, :] = (v.keep[0, at, :] + v.got[0, at, :].astype(single)).astype(kind)
            cross(n).start()

    for h in range(2):
        at = slice(h * half, (h + 1) * half)
        for n in range(pieces):
            cols = slice(n * piece, (n + 1) * piece)
            value = jnp.dot(
                v.gated[4 * h * half : 4 * (h + 1) * half, :], v.mixer[:, cols],
                preferred_element_type=single,
            )
            v.give[:, at, cols] = value[: 2 * half].astype(kind).reshape(2, half, piece)
            v.keep[:, at, cols] = value[2 * half :].reshape(2, half, piece)
        pair(h).start()
        if h == 0:

            @pl.when(c == 0)
            def _():
                send_across(0)

    @pl.when(c == 1)
    def _():
        send_across(0)

    send_across(1)

    xs, part = (v.xs, v.part)

    def ax(k, h, at=None, sem=None):
        at = part_of(h) if at is None else at
        sem = v.ax_send if sem is None else sem
        return copy(xs.at[k, 0, at], xs.at[k, DX, at], sem, v.ax_recv.at[k, h], peer_x)

    def ay(k, h, at=None, sem=None):
        at = part_of(h) if at is None else at
        sem = v.ay_send if sem is None else sem
        return copy(xs.at[k, 0, at], xs.at[k, DY, at], sem, v.ay_recv.at[k, h], peer_y)

    def fy(k):
        return copy(
            xs.at[k, DX, part_of(0)], xs.at[k, DX + DY, part_of(0)], v.af_send,
            v.af_recv.at[k], peer_y,
        )

    def fx(k):
        return copy(
            xs.at[k, DY, part_of(1)], xs.at[k, DX + DY, part_of(1)], v.af_send,
            v.af_recv.at[k], peer_x,
        )

    def ac(k, s):
        return copy(
            xs.at[k, s], xs.at[k, DC + s], v.ac_send, v.ac_recv.at[k], peer_c
        )

    whole = pl.ds(0, kept)
    beside = z + 1 - 2 * (z % 2)
    pair_device = {"sp": beside * 2 + y, "tp": tp}
    pair_slot = 1 + (z % 2) * (depth - 2)

    def lift_x():
        return copy(
            xs.at[0, DX, part_of(0)], xs.at[pair_slot, DX, part_of(0)], v.ax_send,
            v.ax_recv.at[pair_slot, 0], pair_device,
        )

    def lift_y():
        return copy(
            xs.at[0, DY, part_of(1)], xs.at[pair_slot, DY, part_of(1)], v.ay_send,
            v.ay_recv.at[pair_slot, 1], pair_device,
        )

    def upward(i, at):
        return copy(
            xs.at[i - 1, 0, at], xs.at[i, 0, at], v.up_send.at[i], v.az_recv.at[i], plane(1)
        )

    def downward(i, at):
        return copy(
            xs.at[(depth - i + 1) % depth, 0, at], xs.at[depth - i, 0, at], v.dn_send.at[i],
            v.az_recv.at[depth - i], plane(depth - 1),
        )

    def landed(k):
        return all_of(xs.at[k, 0], v.az_recv.at[k])

    for n in range(bands):
        at = slice(n * band, (n + 1) * band)
        cross(n).wait_recv()
        total = v.keep[1, at, :] + v.got[1, at, :].astype(single) + v.came[at, :].astype(single)
        hidden = (v.stream[at, :].astype(single) + total).astype(kind)
        v.hidden[at, :] = hidden
        wide = hidden.astype(single)
        mean = jnp.mean(wide * wide, axis=-1, keepdims=True)
        normed = wide * lax.rsqrt(mean + NORM_EPSILON) * v.gain[...]
        xs[0, 0, at, :] = normed.astype(kind)
        ax(0, n * 2 // bands, band_of(n)).start()
        ay(0, n * 2 // bands, band_of(n)).start()

        @pl.when(z < depth - 1)
        def _():
            upward(1, band_of(n)).start()

        @pl.when(z > 0)
        def _():
            downward(1, band_of(n)).start()

    ac(0, 0).start()
    all_of(v.weigh_in.at[others], v.weigh_recv).wait_recv()
    table = v.weigh_out[sp]
    for k in range(1, count):
        table = table + v.weigh_in[k]
    filled = jnp.concatenate([table, jnp.zeros((LANES - lines, rows), single)], axis=0)
    v.weigh[...] = jnp.transpose(filled)
    for name in ("gate_w", "up_w", "down_w"):
        loads[name].wait()

    def rc(k, cols):
        at = pl.ds(cols.start, cols.stop - cols.start)
        return copy(
            part.at[k, pl.ds(DC, DC), :, at], v.from_core.at[k, :, :, at], v.rc_send,
            v.rc_recv.at[k], peer_c,
        )

    def rs(k, n):
        sems = (v.rs_send, v.rs_recv.at[k, min(n, 2)])
        if n == 0:
            return copy(part.at[k, DX + DY, part_of(0)], v.first.at[k, 0], *sems, peer_y)
        if n == 1:
            return copy(part.at[k, DX + DY, part_of(1)], v.first.at[k, 1], *sems, peer_x)
        if n == 2:
            return copy(part.at[k, DY, part_of(0)], v.rest.at[k, 0], *sems, peer_y)
        if n == 3:
            return copy(part.at[k, DX, part_of(1)], v.rest.at[k, 1], *sems, peer_x)
        if n == 4:
            return copy(part.at[k, DX, part_of(0)], v.rest.at[k, 2], *sems, peer_x)
        return copy(part.at[k, DY, part_of(1)], v.rest.at[k, 3], *sems, peer_y)

    last = depth - 1
    at_end = (z == 0) | (z == last)
    inward = jnp.where(z == 0, 1, last - 1)
    across = jnp.where(z == 1, last, 0)

    bulk = v.from_pair.shape[1]
    remnant = pl.ds(bulk, kept - bulk)
    over_y, over_x = (z * 2 + 1 - y, (1 - x) * 2 + c)
    peer_1 = {"sp": (1 - c) * sp + c * over_y, "tp": (1 - c) * over_x + c * tp}
    peer_2 = {"sp": (1 - c) * over_y + c * sp, "tp": (1 - c) * tp + c * over_x}

    def to_pair(k):
        return copy(
            part.at[k, pl.ds(0, DC), pl.ds(0, bulk)], v.from_pair, v.rp_send, v.rp_recv,
            pair_device,
        )

    def rq(k, n):
        if n == 0:
            there = part.at[k, DX + DY, remnant]
            return copy(there, v.from_1, v.rq_send, v.rq_recv.at[0], peer_1)
        if n == 1:
            there = part.at[k, DX + c, remnant]
            return copy(there, v.from_2.at[0], v.rq_send, v.rq_recv.at[1], peer_1)
        if n == 2:
            there = part.at[k, DY - c, remnant]
            return copy(there, v.from_2.at[1], v.rq_send, v.rq_recv.at[1], peer_2)
        return copy(part.at[k, 0, remnant], v.from_3, v.rq_send, v.rq_recv.at[2], pair_device)

    def remnant_next(k):
        rq(k, 0).wait_recv()
        now = part[k, DY - c, bulk:kept].astype(single) + v.from_1[...].astype(single)
        part[k, DY - c, bulk:kept] = now.astype(kind)
        rq(k, 2).start()

    def remnant_last(k):
        all_of(v.from_2, v.rq_recv.at[1]).wait_recv()
        now = part[k, 0, bulk:kept].astype(single) + v.from_2[0].astype(single)
        part[k, 0, bulk:kept] = (now + v.from_2[1].astype(single)).astype(kind)
        rq(k, 3).start()

    small = half // 2

    def slim(h, t):
        return pl.ds(h * half + t * small, small)

    def zr_near(k, h, t):
        to = jnp.where(at_end, inward, across)
        return copy(
            part.at[k, 0, slim(h, t)], v.from_z.at[0, slim(h, t)], v.rz_send, v.rz_recv.at[t],
            {"sp": to * 2 + y, "tp": tp},
        )

    def near_landed(t):
        all_of(v.from_z.at[0, pl.ds(0, half)], v.rz_recv.at[t]).wait_recv()

    def zr_far(k, h, t):
        return copy(
            part.at[k, 0, slim(h, t)], v.from_z.at[1, slim(h, t)], v.rz_send, v.rz_recv.at[2],
            {"sp": (last - z) * 2 + y, "tp": tp},
        )

    def rt(k, t, n):
        here = slim(0, t)
        sems = (v.rs_send, v.rt_recv.at[t, min(n, 2)])
        if n == 0:
            return copy(part.at[k, DX + DY, here], v.first.at[k, 0, here], *sems, peer_y)
        if n == 1:
            return copy(part.at[k, DX + DY, slim(1, t)], v.first.at[k, 1, here], *sems, peer_x)
        if n == 2:
            return copy(part.at[k, DY, here], v.rest.at[k, 0, here], *sems, peer_y)
        if n == 3:
            return copy(part.at[k, DX, slim(1, t)], v.rest.at[k, 1, here], *sems, peer_x)
        if n == 4:
            return copy(part.at[k, DX, here], v.rest.at[k, 2, here], *sems, peer_x)
        return copy(part.at[k, DY, slim(1, t)], v.rest.at[k, 3, here], *sems, peer_y)

    def slim_next(k, t):
        here = slice(t * small, (t + 1) * small)
        there = slice(half + t * small, half + (t + 1) * small)
        rt(k, t, 0).wait_recv()
        now = part[k, DX, here].astype(single) + v.first[k, 0, here].astype(single)
        part[k, DX, here] = now.astype(kind)
        rt(k, t, 4).start()
        rt(k, t, 1).wait_recv()
        now = part[k, DY, there].astype(single) + v.first[k, 1, here].astype(single)
        part[k, DY, there] = now.astype(kind)
        rt(k, t, 5).start()

    def slim_last(k, t):
        here = slice(t * small, (t + 1) * small)
        all_of(v.rest.at[k, pl.ds(0, 4), slim(0, t)], v.rt_recv.at[t, 2]).wait_recv()
        inner = (z > 0) & (z < last)

        @pl.when(inner)
        def _():
            near_landed(t)

        for h in range(2):
            rows_h = slice(h * half + t * small, h * half + (t + 1) * small)
            now = part[k, 0, rows_h].astype(single) + v.rest[k, h, here].astype(single)
            now = now + v.rest[k, h + 2, here].astype(single)
            part[k, 0, rows_h] = now.astype(kind)

            @pl.when(inner)
            def _():
                more = part[k, 0, rows_h].astype(single) + v.from_z[0, rows_h].astype(single)
                part[k, 0, rows_h] = more.astype(kind)

            zr_far(k, h, t).start()

    lane = lax.broadcasted_iota(jnp.int32, (kept, LANES), 1)

    def share_of(k, j):
        plane_from = (z + depth - k) % depth
        columns = []
        for s in range(DC):
            y_from = 1 - y if s & DY else y
            x_from = 1 - x if s & DX else x
            c_from = 1 - c if j else c
            at = pl.ds(pl.multiple_of((x_from * 2 + c_from) * kept, kept), kept)
            mine = lane == plane_from * 2 + y_from
            columns.append(
                jnp.sum(jnp.where(mine, v.weigh[at, :], 0.0), axis=1, keepdims=True)
            )
        return jnp.concatenate(columns, axis=0)

    def activated(k, j):
        rows_in = xs[k, j * DC : (j + 1) * DC].reshape(DC * kept, width)
        g = jnp.dot(rows_in, v.gate_w[...], preferred_element_type=single)
        u = jnp.dot(rows_in, v.up_w[...], preferred_element_type=single)
        return (clamp_units(g, u) * share_of(k, j)).astype(kind)

    def theirs_first(k):
        v.act[...] = activated(k, 1)

    def theirs_next(k):
        for n in range(pieces):
            cols = slice(n * piece, (n + 1) * piece)
            down = jnp.dot(v.act[...], v.down_w[:, cols], preferred_element_type=single)
            part[k, DC : 2 * DC, :, cols] = down.astype(kind).reshape(DC, kept, piece)
            rc(k, cols).start()

    def ours(k, q):
        @pl.when(q != last)
        def _():
            v.own_act[...] = activated(k, 0)

        all_of(v.from_core.at[k], v.rc_recv.at[k]).wait_recv()
        for n in range(pieces):
            cols = slice(n * piece, (n + 1) * piece)
            down = jnp.dot(v.own_act[...], v.down_w[:, cols], preferred_element_type=single)
            down = down.reshape(DC, kept, piece) + v.from_core[k, :, :, cols].astype(single)
            part[k, 0:DC, :, cols] = down.astype(kind)

    far_slot = 1 + (1 - z % 2) * (depth - 2)
    inner_device = {"sp": (depth - 1 - z) * 2 + y, "tp": tp}

    def haul_x(k, n):
        at = part_of(n // 2)
        return copy(
            xs.at[k, DX, at], xs.at[far_slot, DX, at], v.haul_send.at[n],
            v.ax_recv.at[far_slot, n // 2], pair_device if n % 2 else inner_device,
        )

    def haul_y(k, n):
        at = part_of(1 - n // 2)
        return copy(
            xs.at[k, DY, at], xs.at[far_slot, DY, at], v.haul_send.at[n],
            v.ay_recv.at[far_slot, 1 - n // 2], pair_device if n % 2 else inner_device,
        )

    def haul(k, n):
        inner = (z > 0) & (z < depth - 1)

        @pl.when(inner & (c == 0))
        def _():
            haul_x(k, n).start()

        @pl.when(inner & (c == 1))
        def _():
            haul_y(k, n).start()

    def spread_first(k, q):
        ax(k, 0).wait_recv()
        fy(k).start()

        @pl.when((q == 0) & (c == 0))
        def _():
            lift_x().start()

        ay(k, 1).wait_recv()
        fx(k).start()

        @pl.when((q == 0) & (c == 1))
        def _():
            lift_y().start()

    def spread_second(k):
        ax(k, 0).wait_recv()
        fy(k).start()
        ay(k, 1).wait_recv()
        fx(k).start()

    def spread_rest(k):
        ax(k, 1).wait_recv()
        ac(k, DX).start()
        ay(k, 0).wait_recv()
        ac(k, DY).start()

    def spread_last(k):
        all_of(xs.at[k, DX + DY], v.af_recv.at[k]).wait_recv()
        ac(k, DX + DY).start()

    def relay(i):
        @pl.when(i <= z)
        def _():
            landed(i).wait_recv()

            @pl.when(z < depth - 1)
            def _():
                upward(i + 1, whole).start()

        @pl.when(z + i < depth)
        def _():
            landed(depth - i).wait_recv()

            @pl.when(z > 0)
            def _():
                downward(i + 1, whole).start()

    def enter(k, q):
        @pl.when((q == 1) | ((q == 0) & (c == 1)))
        def _():
            ax(k, 0).start()

        @pl.when((q == 1) | ((q == 0) & (c == 0)))
        def _():
            ay(k, 1).start()

        @pl.when((q == 2) & (c == 1))
        def _():
            ax(k, 0, sem=v.odd_send).start()
            ax(k, 1, sem=v.odd_send).start()

        @pl.when((q == 2) & (c == 0))
        def _():
            ay(k, 1, sem=v.odd_send).start()
            ay(k, 0, sem=v.odd_send).start()

        @pl.when(q < 2)
        def _():
            ax(k, 1).start()
            ay(k, 0).start()

        ac(k, 0).start()

    def reduce_first(k):
        for n in range(4):
            rs(k, n).start()

    def reduce_next(k):
        rs(k, 0).wait_recv()
        now = part[k, DX, 0:half].astype(single) + v.first[k, 0].astype(single)
        part[k, DX, 0:half] = now.astype(kind)
        rs(k, 4).start()
        rs(k, 1).wait_recv()
        now = part[k, DY, half:kept].astype(single) + v.first[k, 1].astype(single)
        part[k, DY, half:kept] = now.astype(kind)
        rs(k, 5).start()

    def reduced(k):
        all_of(v.rest.at[k], v.rs_recv.at[k, 2]).wait_recv()
        upper = part[k, 0, 0:half].astype(single) + v.rest[k, 0].astype(single)
        lower = part[k, 0, half:kept].astype(single) + v.rest[k, 1].astype(single)
        return (upper + v.rest[k, 2].astype(single), lower + v.rest[k, 3].astype(single))

    def reduce_last(k):
        upper, lower = reduced(k)
        part[k, 0, 0:half] = upper.astype(kind)
        part[k, 0, half:kept] = lower.astype(kind)
        for t in range(2):
            for h in range(2):
                zr_near(k, h, t).start()

    def step(q, none):
        k = turn(z, q % depth, depth)
        k_next = turn(z, (q + 1) % depth, depth)
        k_done = turn(z, (q + depth - 1) % depth, depth)
        k_older = turn(z, (q + depth - 2) % depth, depth)
        live, late = (q < depth, q > 0)

        @pl.when(q < last)
        def _():
            spread_first(k, q)

        @pl.when(q == 1)
        def _():
            haul(0, 0)
            haul(0, 2)

        @pl.when(q == 2)
        def _():
            haul(k, 1)

        @pl.when(q == last)
        def _():
            rq(turn(z, 1, depth), 0).start()
            rq(turn(z, 1, depth), 1).start()
            v.own_act[...] = activated(k_done, 0)

        @pl.when(late)
        def _():
            all_of(xs.at[k_done, pl.ds(DC, DC)], v.ac_recv.at[k_done]).wait_recv()
            theirs_first(k_done)

        @pl.when(q == last)
        def _():
            spread_second(k)

        @pl.when(late)
        def _():
            theirs_next(k_done)

        @pl.when(q + 1 < depth)
        def _():
            relay(q + 1)
            enter(k_next, q)
            spread_rest(k)

        @pl.when(q == 2)
        def _():
            haul(k, 3)

        @pl.when(q > 3)
        def _():
            reduce_next(k_older)

        @pl.when(late)
        def _():
            ours(k_done, q)

        @pl.when(q == 2)
        def _():
            to_pair(k_done).start()

        @pl.when(q == last)
        def _():
            reduce_first(k_done)

        @pl.when(q > last)
        def _():
            for n in range(4):
                rt(k_done, 0, n).start()
            rt(k_done, 1, 0).start()
            rt(k_done, 1, 1).start()

        @pl.when(q == last)
        def _():
            spread_rest(k)

        @pl.when(live)
        def _():
            spread_last(k)

        return none

    lax.fori_loop(0, depth + 1, step, 0)
    k_pair, k_near, k_far = [turn(z, p, depth) for p in (1, 2, 3)]
    reduce_last(k_near)
    slim_next(k_far, 0)
    rt(k_far, 1, 2).start()
    rt(k_far, 1, 3).start()
    all_of(v.from_pair, v.rp_recv).wait_recv()
    for n in range(DC):
        now = part[0, n, 0:bulk].astype(single) + v.from_pair[n].astype(single)
        part[0, n, 0:bulk] = now.astype(kind)
    slim_next(k_far, 1)
    remnant_next(k_pair)
    reduce_first(0)
    slim_last(k_far, 0)
    slim_last(k_far, 1)
    remnant_last(k_pair)
    reduce_next(0)
    upper, lower = reduced(0)
    upper = upper + v.hidden[0:half, :].astype(single)
    lower = lower + v.hidden[half:kept, :].astype(single)

    @pl.when(at_end)
    def _():
        for t in range(2):
            near_landed(t)

    all_of(v.from_z.at[1], v.rz_recv.at[2]).wait_recv()
    direct = jnp.where(at_end, 1.0, 0.0)
    upper = upper + direct * v.from_z[0, 0:half].astype(single)
    lower = lower + direct * v.from_z[0, half:kept].astype(single)
    upper = upper + v.from_z[1, 0:half].astype(single)
    lower = lower + v.from_z[1, half:kept].astype(single)
    rq(k_pair, 3).wait_recv()
    rest = jnp.concatenate(
        [jnp.zeros((bulk - half, width), single), v.from_3[...].astype(single)], axis=0
    )
    lower = lower + rest
    for h, value in enumerate((upper, lower)):
        v.out[h * half : (h + 1) * half, :] = value.astype(v.out.dtype)
    every = pl.ds(0, depth)
    quarter, six = (xs.at[every, pl.ds(0, 1)], v.first.at[pl.ds(0, 3)])
    for ref, sem in (
        (v.weigh_in.at[others], v.weigh_send), (v.ends.at[others], v.end_send),
        (v.give, v.pair_send), (v.over, v.cross_send), (six, v.ax_send),
        (six, v.ay_send), (v.rest.at[0, pl.ds(0, 2)], v.odd_send), (quarter, v.af_send), (xs.at[every, pl.ds(0, DC)], v.ac_send),
        (part.at[every, pl.ds(DC, DC)], v.rc_send), (part.at[pl.ds(1, last), pl.ds(0, 3)], v.rs_send),
        (v.from_z, v.rz_send), (v.from_pair, v.rp_send), (part.at[0, 0], v.rq_send),
    ):
        all_of(ref, sem).wait_send()

    @pl.when((z > 0) & (z < last))
    def _():
        for n in range(4):
            haul_x(0, n).wait_send()

    for i in range(1, depth):

        @pl.when((i - 1 <= z) & (z < depth - 1))
        def _():
            upward(i, whole).wait_send()

        @pl.when((z + i <= depth) & (z > 0))
        def _():
            downward(i, whole).wait_send()


def layer(
    conv_input, gate_branch, conv_taps, narrow_maps, wide_maps, decay, decay_shift, mixer_out,
    stream, gain, routes, shares, expert_gate, expert_up, expert_down,
):
    count = lax.axis_size("sp")
    depth = count // 2
    rows, channels = conv_input.shape
    kept, width = stream.shape
    half = kept // 2
    pieces = 4
    bulk = kept * 3 // 4
    lines = -(-count // SUBLANES) * SUBLANES
    single, kind = (jnp.float32, jnp.bfloat16)
    dma = pltpu.SemaphoreType.DMA
    inputs = dict(
        conv=conv_input, gate=gate_branch, taps=conv_taps, narrow=narrow_maps, wide=wide_maps,
        decay=decay, shift=decay_shift, mixer=mixer_out, stream=stream, gain=gain, routes=routes,
        shares=shares, gate_w=expert_gate, up_w=expert_up, down_w=expert_down,
    )
    scratch = {
        name: pltpu.VMEM(one.shape[1:] if name.endswith("_w") else one.shape, one.dtype)
        for name, one in inputs.items()
    }
    flat = pltpu.VMEM((rows, channels), single)
    scratch.update(
        soft=pltpu.VMEM(decay.shape, single),
        gelu=flat,
        halo=pltpu.VMEM((2 * SUBLANES, channels), kind),
        factor=flat,
        state=flat,
        padded=pltpu.VMEM((rows + SUBLANES, channels), single),
        log_keep=flat,
        drive_keep=flat,
        ends=pltpu.VMEM((count, 2 * channels // LANES, LANES), single),
        weigh_out=pltpu.VMEM((count, lines, rows), single),
        weigh_in=pltpu.VMEM((count, lines, rows), single),
        weigh=pltpu.VMEM((rows, LANES), single),
        gated=pltpu.VMEM((rows, channels), kind),
        give=pltpu.VMEM((2, kept, width), kind),
        got=pltpu.VMEM((2, kept, width), kind),
        keep=pltpu.VMEM((2, kept, width), single),
        over=pltpu.VMEM((kept, width), kind),
        came=pltpu.VMEM((kept, width), kind),
        hidden=pltpu.VMEM((kept, width), kind),
        xs=pltpu.VMEM((depth, 2 * DC, kept, width), kind),
        act=pltpu.VMEM((DC * kept, expert_gate.shape[2]), kind),
        own_act=pltpu.VMEM((DC * kept, expert_gate.shape[2]), kind),
        part=pltpu.VMEM((depth, 2 * DC, kept, width), kind),
        from_core=pltpu.VMEM((depth, DC, kept, width), kind),
        first=pltpu.VMEM((depth, 2, half, width), kind),
        rest=pltpu.VMEM((depth, 4, half, width), kind),
        from_z=pltpu.VMEM((2, kept, width), kind),
        from_pair=pltpu.VMEM((DC, bulk, width), kind),
        from_1=pltpu.VMEM((kept - bulk, width), kind),
        from_2=pltpu.VMEM((2, kept - bulk, width), kind),
        from_3=pltpu.VMEM((kept - bulk, width), kind),
        load_sem=dma((len(inputs),)),
        halo_send=dma,
        halo_recv=dma,
    )
    sent = ("weigh", "end", "pair", "cross", "ax", "ay", "af", "ac", "rc", "rs", "rz", "rp", "rq")
    scratch.update({name + "_send": dma for name in sent})
    landing = dict(
        weigh=(), end=(), pair=(2,), cross=(4,), ax=(depth, 2), ay=(depth, 2), af=(depth,),
        ac=(depth,), rc=(depth,), rs=(depth, 3), rz=(3,), rp=(), rq=(3,), az=(depth,), rt=(2, 3),
    )
    scratch.update({name + "_recv": dma(shape) if shape else dma for name, shape in landing.items()})
    scratch.update(
        up_send=dma((depth,)), dn_send=dma((depth,)), haul_send=dma((4,)), odd_send=dma
    )
    names = [name + "_hbm" for name in inputs] + ["out"] + list(scratch)
    return pl.pallas_call(
        functools.partial(layer_kernel, count, names),
        out_shape=pltpu.VMEM((kept, width), kind),
        in_specs=[pl.BlockSpec(memory_space=pl.ANY)] * len(inputs),
        out_specs=pl.BlockSpec(memory_space=pltpu.VMEM),
        scratch_shapes=list(scratch.values()),
        compiler_params=pltpu.CompilerParams(
            collective_id=1, has_side_effects=True, vmem_limit_bytes=60 * 1024 * 1024
        ),
    )(*inputs.values())


def shards(
    conv_input,
    gate_branch,
    conv_taps,
    narrow_maps,
    wide_maps,
    decay_param,
    decay_shift,
    mixer_out,
    stream,
    norm_gain,
    routes,
    route_weights,
    expert_gate,
    expert_up,
    expert_down,
):
    seq_rows, channels = conv_input.shape
    tap_count = conv_taps.shape[0]
    tp_count = lax.axis_size("tp")
    tok_local = seq_rows // tp_count
    top_count = routes.shape[1]
    expert_total = expert_gate.shape[0] * lax.axis_size("sp")
    capacity = max(2, 2 * tok_local * top_count // expert_total)
    whole_rows = capacity >= tok_local and expert_gate.shape[0] == 1
    if whole_rows and tp_count == 4 and lax.axis_size("sp") == 8:
        return layer(
            conv_input, gate_branch, conv_taps, narrow_maps, wide_maps, decay_param[None, :],
            decay_shift, mixer_out, stream, norm_gain[None, :], routes.T, route_weights.T,
            expert_gate, expert_up, expert_down,
        )
    own_index = lax.axis_index("tp")
    own_rows = lax.dynamic_slice_in_dim(routes, own_index * tok_local, tok_local, 0)
    own_weights = lax.dynamic_slice_in_dim(route_weights, own_index * tok_local, tok_local, 0)
    soft = jax.nn.softplus(-decay_param)[None, :]
    earlier = shifted(conv_input[seq_rows - tap_count + 1 :], "sp", 1)
    head = jnp.zeros((SUBLANES, channels), jnp.float32)
    head = head.at[SUBLANES - tap_count + 1 :].set(earlier.astype(jnp.float32))
    factors, local_state = mix_local(
        head, conv_input, conv_taps, narrow_maps, wide_maps, soft, decay_shift
    )
    ends = lax.all_gather(jnp.stack([factors[-1], local_state[-1]]), "sp")
    mine = lax.axis_index("sp")
    state = jnp.zeros((channels,), jnp.float32)
    for position in range(lax.axis_size("sp") - 1):
        longer = ends[position, 0] * state + ends[position, 1]
        state = jnp.where(position < mine, longer, state)
    carried = (None, state)
    recurrent = local_state + factors * carried[1]
    gated_rows = (recurrent * jax.nn.gelu(gate_branch.astype(jnp.float32))).astype(jnp.bfloat16)
    mixer_sum = lax.psum_scatter(
        jnp.dot(gated_rows, mixer_out, preferred_element_type=jnp.float32).astype(jnp.bfloat16),
        "tp",
        scatter_dimension=0,
        tiled=True,
    ).astype(jnp.float32)
    hidden_f = stream.astype(jnp.float32) + mixer_sum
    hidden = hidden_f.astype(jnp.bfloat16)
    hidden_f = hidden.astype(jnp.float32)
    normed = (
        hidden_f
        * lax.rsqrt(jnp.mean(hidden_f * hidden_f, axis=-1, keepdims=True) + NORM_EPSILON)
        * norm_gain
    ).astype(jnp.bfloat16)
    model_width = normed.shape[1]
    assignments = tok_local * top_count
    own_routes = own_rows.reshape(assignments)
    own_ranks = slot_ranks(own_routes[None, :], expert_total)[0]
    source = jnp.arange(assignments, dtype=jnp.int32) // top_count
    slot_source = (
        jnp.full((expert_total * capacity,), -1, jnp.int32)
        .at[own_routes * capacity + own_ranks]
        .set(source)
    )
    outgoing = take_rows(normed, slot_source).reshape(expert_total, 1, capacity, model_width)
    partial_value = expert_work(
        lax.all_gather(
            lax.all_to_all(outgoing, "sp", split_axis=0, concat_axis=0, tiled=True),
            "tp",
            axis=1,
            tiled=True,
        ),
        expert_gate,
        expert_up,
        expert_down,
    )
    summed = lax.psum_scatter(
        partial_value.astype(jnp.bfloat16), "tp", scatter_dimension=1, tiled=True
    )
    returned = lax.all_to_all(summed, "sp", split_axis=0, concat_axis=0, tiled=True)
    own_slots = own_routes * capacity + own_ranks
    picked = returned.reshape(expert_total * capacity, model_width)[own_slots]
    combined = jnp.sum(
        picked.reshape(tok_local, top_count, model_width).astype(jnp.float32)
        * own_weights[:, :, None],
        axis=1,
    )
    return (hidden_f + combined).astype(jnp.bfloat16)


def solution(mesh):
    placed = (
        P("sp", "tp"),
        P("sp", "tp"),
        P(None, "tp"),
        P(None, "tp", None, None),
        P(None, "tp", None, None),
        P("tp"),
        P("sp", "tp"),
        P("tp", None),
        P(("sp", "tp"), None),
        P(),
        P("sp", None),
        P("sp", None),
        P("sp", None, "tp"),
        P("sp", None, "tp"),
        P("sp", "tp", None),
    )
    return jax.shard_map(
        shards, mesh=mesh, in_specs=placed, out_specs=P(("sp", "tp"), None), check_vma=False
    )
```
